256 devices in a mesh: kv: 32 (over z, x), tp: 8 (over y, core).
Axes of the slice: x: 4, y: 4, z: 8, core: 2. Of those that a mesh axis runs over, the one named last changes fastest.
Arguments:
- layer_input: bfloat16 [1024, 4096], P('tp', 'kv'), may hold values from -6 to 6
- seq_lengths: int32 [256], P('kv'), may hold values from 1 to 4, 448 in all
- delta_state: float32 [256, 16, 128, 128], P('kv', 'tp'), may hold values from -0.4 to 0.4
- attn_gain: bfloat16 [4096], replicated, may hold values from 0.099609375 to 1.8984375
- w_query: bfloat16 [4096, 2048], P('kv', 'tp'), may hold values from -0.09375 to 0.09375
- w_key: bfloat16 [4096, 2048], P('kv', 'tp'), may hold values from -0.09375 to 0.09375
- w_value: bfloat16 [4096, 2048], P('kv', 'tp'), may hold values from -0.09375 to 0.09375
- w_outgate: bfloat16 [4096, 2048], P('kv', 'tp'), may hold values from -0.09375 to 0.09375
- w_write: bfloat16 [4096, 16], P('kv', 'tp'), may hold values from -0.09375 to 0.09375
- w_forget: bfloat16 [4096, 16], P('kv', 'tp'), may hold values from -0.09375 to 0.09375
- forget_rate: float32 [16], P('tp'), may hold values from 0.02 to 2
- head_gain: float32 [128], replicated, may hold values from 0.1 to 1.9
- w_out: bfloat16 [2048, 4096], P('tp', 'kv'), may hold values from -0.125 to 0.125
- mixer_gain: bfloat16 [4096], replicated, may hold values from 0.099609375 to 1.8984375
- w_gate: bfloat16 [4096, 11264], P('kv', 'tp'), may hold values from -0.09375 to 0.09375
- w_up: bfloat16 [4096, 11264], P('kv', 'tp'), may hold values from -0.09375 to 0.09375
- w_down: bfloat16 [11264, 4096], P('tp', 'kv'), may hold values from -0.0546875 to 0.0546875
Outputs:
- layer_output: bfloat16 [1024, 4096], P('tp', 'kv')
- next_state: float32 [256, 16, 128, 128], P('kv', 'tp')
The draws below stay inside these ranges and needn't reach their ends.
Inputs may be any that keep to these rules, and one draw needn't show every extreme that they name: `seq_lengths`: the lengths add up to 448.
All inputs are finite; a program needn't handle non-finite values. No bound on the sum of `seq_lengths` on one device may be relied on, other than what follows from the above.
Results may differ from the reference program's by a relative error of at most 0.024.
Values may be sent and summed in bfloat16 or wider, within the bound.
A program may use at most 64 MiB of HBM per device.

```python
import math
import jax
import jax.numpy as jnp
import numpy as np
from jax import lax

D = 4096
H = 16
DK = 128
FF = 11264
NEW = 4
SEQS = 256
ROWS = 1024
HW = 2048
N_TP = 8


def steps_of(stream_key, dims, split, low, largest):
    def one(axis_at, blocks):
        steps = jax.random.uniform(jax.random.fold_in(jax.random.fold_in(stream_key, 6), axis_at), (blocks,), jnp.float32, low / len(split), largest / len(split))
        return jnp.repeat(jnp.exp(steps), dims[axis_at] // blocks).reshape((-1,) + (1,) * (len(dims) - axis_at - 1))

    loudness = one(*split[0])
    for cut in split[1:]:
        loudness = loudness * one(*cut)
    return loudness


def length_profile(count, total, bound, slope):
    weights = [(1 << 20) // math.isqrt(rank ** slope) + 1 for rank in range(2, count + 1)]
    surplus, counts = total - bound - (count - 1), [1] * (count - 1)
    while surplus > 0:
        candidates = [i for i in range(count - 1) if counts[i] < bound]
        whole, remaining = sum([weights[i] for i in candidates]), surplus
        for i in candidates:
            extra = min(bound - counts[i], max(1, remaining * weights[i] // whole), surplus)
            counts[i] = counts[i] + extra
            surplus = surplus - extra
    return np.array([bound] + counts)


def ragged(rng, amount, total, bound, lean):
    if amount == 2:
        one = jax.random.randint(rng, (), max(1, total - bound), min(bound, total - 1) + 1)
        return jnp.stack([one, total - one])
    sizes = jnp.asarray(length_profile(amount, total, bound, lean), jnp.int32)
    twos = (amount - 1) // 2
    source_of, taker = sizes[1:1 + 2 * twos:2], sizes[2:2 + 2 * twos:2]
    room = jnp.minimum(source_of - 1, bound - taker)
    moved = jax.random.randint(jax.random.fold_in(rng, 1), (twos,), 0, 1 << 20) % (room + 1)
    sizes = sizes.at[1:1 + 2 * twos:2].set(source_of - moved).at[2:2 + 2 * twos:2].set(taker + moved)
    return sizes[jax.random.permutation(jax.random.fold_in(rng, 2), amount)]


def bell_draw(rng, extent, spread, most, pieces=(), held_as=jnp.bfloat16):
    level = steps_of(rng, extent, pieces, -0.22, 0.18) if pieces else 1.0
    array = jax.random.normal(rng, extent, jnp.float32) * spread * level
    return jnp.minimum(jnp.maximum(array, -most), most).astype(held_as)


def setup_inputs(seed: int = 0) -> dict:
    key_of = jax.random.split(jax.random.key(seed), 18)
    layer_input = bell_draw(key_of[0], (ROWS, D), 1.0, 6.0, ((0, 8), (1, 32)))
    seq_lengths = ragged(key_of[1], SEQS, SEQS + 3 * SEQS // 4, NEW, 2).astype(jnp.int32)
    delta_state = bell_draw(key_of[2], (SEQS, H, DK, DK), 0.05, 0.4, ((0, 32), (1, 8)), jnp.float32)
    attn_gain = jnp.clip(1.0 + 0.18 * jax.random.normal(key_of[3], (D,), jnp.float32), 0.099609375, 1.8984375).astype(jnp.bfloat16)
    w_query = bell_draw(key_of[4], (D, HW), D ** -0.5, 0.09375, ((0, 32), (1, 8)))
    w_key = bell_draw(key_of[5], (D, HW), D ** -0.5, 0.09375, ((0, 32), (1, 8)))
    w_value = bell_draw(key_of[6], (D, HW), D ** -0.5, 0.09375, ((0, 32), (1, 8)))
    w_outgate = bell_draw(key_of[7], (D, HW), D ** -0.5, 0.09375, ((0, 32), (1, 8)))
    w_write = bell_draw(key_of[8], (D, H), D ** -0.5, 0.09375, ((0, 32), (1, 8)))
    w_forget = bell_draw(key_of[9], (D, H), D ** -0.5, 0.09375, ((0, 32), (1, 8)))
    forget_rate = jnp.clip(jnp.exp(math.log(2.0) - 4.6051702 * jax.random.uniform(key_of[10], (H,), jnp.float32) ** steps_of(key_of[10], (H,), ((0, 8),), -0.2, 0.2)), 0.02, 2.0)
    head_gain = jnp.clip(1.0 + 0.18 * jax.random.normal(key_of[11], (DK,), jnp.float32), 0.1, 1.9)
    w_out = bell_draw(key_of[12], (HW, D), HW ** -0.5, 0.125, ((0, 8), (1, 32)))
    mixer_gain = jnp.clip(1.0 + 0.18 * jax.random.normal(key_of[13], (D,), jnp.float32), 0.099609375, 1.8984375).astype(jnp.bfloat16)
    w_gate = bell_draw(key_of[14], (D, FF), D ** -0.5, 0.09375, ((0, 32), (1, 8)))
    w_up = bell_draw(key_of[15], (D, FF), D ** -0.5, 0.09375, ((0, 32), (1, 8)))
    w_down = bell_draw(key_of[16], (FF, D), FF ** -0.5, 0.0546875, ((0, 8), (1, 32)))
    return dict(layer_input=layer_input, seq_lengths=seq_lengths, delta_state=delta_state, attn_gain=attn_gain, w_query=w_query, w_key=w_key, w_value=w_value, w_outgate=w_outgate, w_write=w_write, w_forget=w_forget, forget_rate=forget_rate, head_gain=head_gain, w_out=w_out, mixer_gain=mixer_gain, w_gate=w_gate, w_up=w_up, w_down=w_down)


EPS = 1e-06

def unit_norm(vectors):
    return vectors * lax.rsqrt(lax.optimization_barrier(jnp.sum(vectors * vectors, axis=-1, keepdims=True)) + EPS)

def run_delta(carried, query_unit, key_unit, value_act, write_rate, log_keep, live):
    readings = []
    for position in range(query_unit.shape[1]):
        active = live[:, position][:, None]
        beta = write_rate[:, position] * active
        keep = jnp.exp(log_keep[:, position] * active)
        key_now = key_unit[:, position]
        recalled = jnp.einsum('shk,shkv->shv', key_now, carried, precision=lax.Precision.HIGHEST)
        update = beta[:, :, None] * (value_act[:, position] - keep[:, :, None] * recalled)
        carried = keep[:, :, None, None] * carried + key_now[:, :, :, None] * update[:, :, None, :]
        reading = jnp.einsum('shk,shkv->shv', query_unit[:, position], carried, precision=lax.Precision.HIGHEST)
        readings.append(reading * active[:, :, None])
    return (carried, jnp.stack(readings, axis=1))

def reference(layer_input, seq_lengths, delta_state, attn_gain, w_query, w_key, w_value, w_outgate, w_write, w_forget, forget_rate, head_gain, w_out, mixer_gain, w_gate, w_up, w_down):
    rows_wide = layer_input.astype(jnp.float32)
    first_scale = lax.rsqrt(lax.optimization_barrier(jnp.mean(rows_wide * rows_wide, axis=1, keepdims=True)) + EPS)
    normed_in = (rows_wide * attn_gain.astype(jnp.float32)).astype(jnp.bfloat16)

    def project(weight):
        return first_scale * jnp.dot(normed_in, weight, preferred_element_type=jnp.float32)

    def split_heads(block):
        return block.reshape(SEQS, NEW, H, DK)
    query_unit = unit_norm(jax.nn.silu(split_heads(project(w_query)))) * DK ** (-0.5)
    key_unit = unit_norm(jax.nn.silu(split_heads(project(w_key))))
    value_act = jax.nn.silu(split_heads(project(w_value)))
    outgate = split_heads(project(w_outgate))
    write_rate = jax.nn.sigmoid(project(w_write).reshape(SEQS, NEW, H))
    log_keep = -forget_rate * jax.nn.softplus(project(w_forget).reshape(SEQS, NEW, H))
    positions = jnp.arange(NEW, dtype=jnp.int32)
    live = (positions[None, :] < seq_lengths[:, None]).astype(jnp.float32)
    carried, readings = run_delta(delta_state, query_unit, key_unit, value_act, write_rate, log_keep, live)
    normed = readings * lax.rsqrt(lax.optimization_barrier(jnp.mean(readings * readings, axis=-1, keepdims=True)) + EPS)
    normed = normed * head_gain * jax.nn.silu(outgate)
    mixed = normed.reshape(ROWS, HW).astype(jnp.bfloat16)
    grouped = mixed.reshape(ROWS, N_TP, HW // N_TP).astype(jnp.float32)
    out_groups = w_out.reshape(N_TP, HW // N_TP, D).astype(jnp.float32)
    group_terms = jnp.einsum('rgc,gcd->grd', grouped, out_groups)
    attended = lax.optimization_barrier(jnp.sum(group_terms.astype(jnp.bfloat16).astype(jnp.float32), axis=0))
    hidden_state = (rows_wide + attended).astype(jnp.bfloat16)
    hidden_wide = hidden_state.astype(jnp.float32)
    mixer_scale = lax.rsqrt(lax.optimization_barrier(jnp.mean(hidden_wide * hidden_wide, axis=1, keepdims=True)) + EPS)
    normed_mid = (hidden_wide * mixer_gain.astype(jnp.float32)).astype(jnp.bfloat16)
    gate_pre = mixer_scale * jnp.dot(normed_mid, w_gate, preferred_element_type=jnp.float32)
    up_pre = mixer_scale * jnp.dot(normed_mid, w_up, preferred_element_type=jnp.float32)
    activated = (jax.nn.silu(gate_pre) * up_pre).astype(jnp.bfloat16)
    mixer_out = jnp.dot(activated, w_down, preferred_element_type=jnp.float32)
    layer_output = (hidden_wide + mixer_out).astype(jnp.bfloat16)
    return (layer_output, carried)
```

```python
import functools

import jax
import jax.numpy as jnp
from jax import lax
from jax.experimental import pallas as pl
from jax.experimental.pallas import tpu as pltpu
from jax.sharding import Mesh
from jax.sharding import PartitionSpec as P

D = 4096
NEW = 4
EPS = 1e-06
NZ, NX, NY, NC = 8, 4, 4, 2
NTP = NY * NC
R = 128
F = 128
WIN = 384
MESH = pl.DeviceIdType.MESH
BF = jnp.bfloat16
F32 = jnp.float32
PLANE = [(dx, dy) for dx in range(NX) for dy in range(NY) if dx or dy]
NSEM = 224


def silu(a):
    return a * jax.nn.sigmoid(a)


def rows_of(k):
    return pl.ds(pl.multiple_of(k * R, R), R)


def dot_t(a, b):
    return lax.dot_general(a, b, (((1,), (1,)), ((), ())), preferred_element_type=F32)


class Links:
    def __init__(self, send, recv):
        self.send, self.recv, self.n, self.all = send, recv, 0, []
        self.z, self.x = lax.axis_index("z"), lax.axis_index("x")
        self.y, self.c = lax.axis_index("y"), lax.axis_index("c")

    def copy(self, src, dst, dz=0, dx=0, dy=0, dc=0):
        to = (
            lax.rem(self.z + dz, NZ),
            lax.rem(self.x + dx, NX),
            lax.rem(self.y + dy, NY),
            lax.rem(self.c + dc, NC),
        )
        return self.copy_to(src, dst, to)

    def copy_to(self, src, dst, to):
        made = pltpu.make_async_remote_copy(
            src_ref=src,
            dst_ref=dst,
            send_sem=self.send.at[self.n],
            recv_sem=self.recv.at[self.n],
            device_id=to,
            device_id_type=MESH,
        )
        self.n += 1
        self.all.append(made)
        made.start()
        return made

    def drain(self):
        for made in self.all:
            made.wait_send()


def enter(links):
    z, x, y, c = links.z, links.x, links.y, links.c
    barrier = pltpu.get_barrier_semaphore()
    to = [(dz, 0, 0, 0) for dz in range(1, NZ)]
    to += [(0, dx, dy, 0) for dx, dy in PLANE]
    to += [(0, 0, dy, 1) for dy in range(NY)]
    for dz, dx, dy, dc in to:
        pl.semaphore_signal(
            barrier,
            inc=1,
            device_id=(lax.rem(z + dz, NZ), lax.rem(x + dx, NX), lax.rem(y + dy, NY), lax.rem(c + dc, NC)),
            device_id_type=MESH,
        )
    pl.semaphore_wait(barrier, len(to))


def plane_gather_start(links, src, buf):
    tp = links.y * NC + links.c
    here = buf.at[links.x, rows_of(tp)]
    straight = [links.copy(src, here, dx=dx, dy=dy) for dx, dy in PLANE]
    forward = [links.copy(src, here, dc=1)]
    return straight, forward


def plane_gather_finish(links, buf, straight, forward):
    for (dx, dy), made in zip(PLANE, straight):
        made.wait_recv()
        xs, ys = lax.rem(links.x - dx + NX, NX), lax.rem(links.y - dy + NY, NY)
        block = buf.at[xs, rows_of(ys * NC + links.c)]
        forward.append(links.copy(block, block, dc=1))
    for made in forward:
        made.wait_recv()


def ring_sum(links, block, sendbuf, recvbuf, width):
    half = width // 2
    made = {}

    def send(way, step, side):
        offset = 4 - step if way == 0 else 4 + step
        lanes = pl.ds(side * half, half)
        value = block(offset)[:, side * half : (side + 1) * half]
        before = made.get((way, step - 1, side))
        if before is not None:
            before.wait_recv()
            value = value + recvbuf[way, step - 1, side].astype(F32)
        sendbuf[way, step, side] = value.astype(BF)
        made[way, step, side] = links.copy(
            sendbuf.at[way, step, side], recvbuf.at[way, step, side], dz=1 if way == 0 else NZ - 1
        )

    for way, step, side in [(0, 0, 0), (1, 0, 1), (0, 1, 1), (1, 1, 0), (0, 1, 0), (1, 1, 1)]:
        send(way, step, side)
    for step in (2, 3):
        for side in (1, 0):
            send(0, step, side)
            send(1, step, 1 - side)
    own = block(0)
    total = []
    for side in (0, 1):
        for way in (0, 1):
            made[way, 3, side].wait_recv()
        total.append(
            own[:, side * half : (side + 1) * half]
            + recvbuf[0, 3, side].astype(F32)
            + recvbuf[1, 3, side].astype(F32)
        )
    return jnp.concatenate(total, axis=1)


def normalize(buf, gain, out, stats, rates):
    sub = lax.broadcasted_iota(jnp.int32, (8, R), 0)
    ones = jnp.ones((16, F), BF)

    def one(b, _):
        at = rows_of(b)
        squares = jnp.zeros((R, F), F32)
        for k in range(NX):
            wide = buf[k, at, :].astype(F32)
            squares = squares + wide * wide
            out[at, k * F : (k + 1) * F] = (wide * gain[:, k * F : (k + 1) * F]).astype(BF)
        high = squares.astype(BF)
        low = (squares - high.astype(F32)).astype(BF)
        row = (dot_t(ones, high) + dot_t(ones, low))[:8]
        stat = jnp.where(sub == 4, row, 0.0)
        if rates is not None:
            for k in range(NX):
                stat = stat + dot_t(rates[k], out[at, k * F : (k + 1) * F])[:8]
        stats[b] = stat
        return 0

    lax.fori_loop(0, NTP, one, 0)


def stats_exchange(links, stats, got):
    made = []
    for dz in range(1, NZ):
        made.append(links.copy(stats.at[lax.rem(links.z + dz, NZ)], got.at[dz], dz=dz))
    return made


def stats_total(links, stats, got, made):
    total = stats[links.z]
    for dz, one in enumerate(made, 1):
        one.wait_recv()
        total = total + got[dz]
    wide = jnp.concatenate([total, jnp.zeros((R - 8, R), F32)], axis=0)
    return wide.T


def body(
    x_ref, len_ref, state_ref, gain1_ref, wq, wk, wv, wo, rate_w_ref, rate_ref, head_gain_ref, w_out_ref, gain2_ref,
    w_gate, w_up, w_down,
    out_ref, next_ref,
    xbuf, nbuf, w4, wr, rw, p1, s1, r1, stats1, got1, pre, mine, cols, readings, mixed_own, mbuf, obuf, orecv,
    hown, hbuf, stats2, got2, wg, wu, wd, p2, s2, r2, act_own, abuf, part, psend, precv, fsend, frecv,
    local, send, recv,
):
    links = Links(send, recv)
    z, x, y, c = links.z, links.x, links.y, links.c
    tp = y * NC + c
    kv = z * NX + x

    locals_ = [pltpu.make_async_copy(w, w4.at[i], local.at[i]) for i, w in enumerate((wq, wk, wv, wo))]

    def window(at):
        return pl.ds(pl.multiple_of((at * 3 - at // (NX - 1)) * F, F), WIN)

    feats = pl.ds(pl.multiple_of(x * F, F), F)
    own_copies = [
        pltpu.make_async_copy(x_ref, xbuf.at[x, rows_of(tp)], local.at[4]),
        pltpu.make_async_copy(rate_w_ref, rw.at[x], local.at[5]),
        pltpu.make_async_copy(w_gate.at[:, window(x)], wg.at[feats], local.at[6]),
        pltpu.make_async_copy(w_up.at[:, window(x)], wu.at[feats], local.at[7]),
        pltpu.make_async_copy(w_down.at[window(x)], wd.at[x], local.at[8]),
    ]
    for one in locals_ + own_copies:
        one.start()
    enter(links)

    straight, forward = plane_gather_start(links, x_ref, xbuf)
    for one in locals_:
        one.wait()
    own_w = pltpu.make_async_copy(w4.at[x], wr.at[feats], local.at[9])
    own_w.start()
    early, late = [], []
    for dx in range(1, NX):
        to = lax.rem(x + dx, NX)
        early.append(links.copy(w4.at[to], wr.at[feats], dx=dx))
        early.append(links.copy(rate_w_ref, rw.at[x], dx=dx))
    for dx in range(1, NX):
        to = lax.rem(x + dx, NX)
        late.append(links.copy(w_gate.at[:, window(to)], wg.at[feats], dx=dx))
        late.append(links.copy(w_up.at[:, window(to)], wu.at[feats], dx=dx))
    for dx in range(1, NX):
        to = lax.rem(x + dx, NX)
        late.append(links.copy(w_down.at[window(to)], wd.at[x], dx=dx))
    for one in own_copies[:2] + [own_w]:
        one.wait()
    plane_gather_finish(links, xbuf, straight, forward)
    for one in early:
        one.wait_recv()

    eighth = lax.broadcasted_iota(jnp.int32, (8, NX * F), 0) == z
    gain1 = jnp.sum(jnp.where(eighth, gain1_ref[...].astype(F32), 0.0), axis=0, keepdims=True)
    gain2 = jnp.sum(jnp.where(eighth, gain2_ref[...].astype(F32), 0.0), axis=0, keepdims=True)
    normalize(xbuf, gain1, nbuf, stats1, rw)
    made = stats_exchange(links, stats1, got1)

    ready = set()

    def projected(offset):
        if offset not in ready:
            ready.add(offset)
            p1[offset] = jnp.dot(
                nbuf[rows_of(lax.rem(z + offset, NZ)), :], wr[...], preferred_element_type=F32
            )
        return p1[offset]

    mine[...] = ring_sum(links, projected, s1, r1, 256).astype(BF)
    quarter = pl.ds(pl.multiple_of(x * 32, 32), 32)
    own_pre = pltpu.make_async_copy(mine.at[quarter], pre.at[x], local.at[10])
    own_pre.start()
    parts = []
    for dx in range(1, NX):
        to = lax.rem(x + dx, NX)
        parts.append(links.copy(mine.at[pl.ds(pl.multiple_of(to * 32, 32), 32)], pre.at[x], dx=dx))
    cols[...] = stats_total(links, stats1, got1, made)
    stat = cols[quarter, :]
    scale = lax.rsqrt(stat[:, 4:5] / D + EPS)
    lane = lax.broadcasted_iota(jnp.int32, (32, R), 1)
    row = lax.broadcasted_iota(jnp.int32, (32, R), 0)
    live = jnp.zeros((32, R), F32)
    for s in range(8):
        inside = (row // NEW == s) & (lax.rem(row, NEW) < len_ref[s])
        live = live + jnp.where(inside, 1.0, 0.0)
    rated = stat * scale
    beta = jax.nn.sigmoid(rated) * live
    rate = jnp.where(lane == 2, rate_ref[0], jnp.where(lane == 3, rate_ref[1], 0.0))
    softplus = jnp.maximum(rated, 0.0) + jnp.log1p(jnp.exp(-jnp.abs(rated)))
    keep = jnp.exp(-rate * softplus * live)
    own_pre.wait()
    for one in parts:
        one.wait_recv()
    query, key, value = (silu(pre[i].astype(F32) * scale) for i in range(3))
    gate = silu(pre[3].astype(F32) * scale)

    def unit(a):
        return a * lax.rsqrt(jnp.sum(a * a, axis=1, keepdims=True) + EPS)

    stacked = []
    for h in range(2):
        at = slice(h * F, (h + 1) * F)
        stacked += [unit(query[:, at]) * F ** (-0.5), unit(key[:, at])]
    turned = jnp.concatenate(stacked, axis=0).T
    for s in range(8):
        for h in range(2):
            state = state_ref[s, h]
            for t in range(NEW):
                r = s * NEW + t
                q_col = turned[:, h * 64 + r : h * 64 + r + 1]
                k_col = turned[:, h * 64 + 32 + r : h * 64 + 33 + r]
                hold = keep[r : r + 1, 2 + h : 3 + h]
                recalled = jnp.sum(k_col * state, axis=0, keepdims=True)
                update = beta[r : r + 1, h : h + 1] * (value[r : r + 1, h * F : (h + 1) * F] - hold * recalled)
                state = hold * state + k_col * update
                readings[r : r + 1, h * F : (h + 1) * F] = jnp.sum(q_col * state, axis=0, keepdims=True)
            next_ref[s, h] = state
    for h in range(2):
        at = slice(h * F, (h + 1) * F)
        read = readings[:, at] * live
        normed = read * lax.rsqrt(jnp.mean(read * read, axis=1, keepdims=True) + EPS)
        mixed_own[:, at] = (normed * head_gain_ref[...] * gate[:, at]).astype(BF)

    def slot(at):
        return mbuf.at[x, pl.ds(pl.multiple_of(at * 32, 32), 32)]

    own_mixed = pltpu.make_async_copy(mixed_own, slot(z), local.at[11])
    own_mixed.start()
    along_z = [links.copy(mixed_own, slot(z), dz=dz) for dz in range(1, NZ)]
    along_x = [links.copy(mixed_own, slot(z), dx=dx) for dx in range(1, NX)]
    for dz in (1, 7, 2, 6, 3, 5, 4):
        along_z[dz - 1].wait_recv()
        block = slot(lax.rem(z - dz + NZ, NZ))
        along_x += [links.copy(block, block, dx=dx) for dx in range(1, NX)]
    own_mixed.wait()
    for one in along_x:
        one.wait_recv()
    for k in range(NX):
        terms = jnp.dot(mbuf[k], w_out_ref[...], preferred_element_type=F32).astype(BF)
        for b in range(NTP):
            obuf[b, k * 32 : (k + 1) * 32, :] = terms[b * 32 : (b + 1) * 32]
    made = []
    for k in range(1, NTP):
        to = lax.rem(tp + k, NTP)
        made.append(links.copy_to(obuf.at[to], orecv.at[k], (z, x, to // NC, lax.rem(to, NC))))
    attended = obuf[tp].astype(F32)
    for k, one in enumerate(made, 1):
        one.wait_recv()
        attended = attended + orecv[k].astype(F32)
    hidden = (x_ref[...].astype(F32) + attended).astype(BF)
    hown[...] = hidden

    own_hidden = pltpu.make_async_copy(hown, hbuf.at[x, rows_of(tp)], local.at[12])
    own_hidden.start()
    straight, forward = plane_gather_start(links, hown, hbuf)
    own_hidden.wait()
    plane_gather_finish(links, hbuf, straight, forward)
    normalize(hbuf, gain2, nbuf, stats2, None)
    made = stats_exchange(links, stats2, got2)
    for one in own_copies[2:]:
        one.wait()
    for one in late:
        one.wait_recv()

    ready2 = set()

    def mixer(offset):
        if offset not in ready2:
            ready2.add(offset)
            rows = nbuf[rows_of(lax.rem(z + offset, NZ)), :]
            p2[offset, :, :WIN] = jnp.dot(rows, wg[...], preferred_element_type=F32)
            p2[offset, :, WIN:] = jnp.dot(rows, wu[...], preferred_element_type=F32)
        return p2[offset]

    total = ring_sum(links, mixer, s2, r2, 2 * WIN)
    scale2 = lax.rsqrt(stats_total(links, stats2, got2, made)[:, 4:5] / D + EPS)
    activated = silu(scale2 * total[:, :WIN]) * (scale2 * total[:, WIN:])
    again = (lax.broadcasted_iota(jnp.int32, (R, WIN), 1) < F) & (x == NX - 1)
    act_own[...] = jnp.where(again, 0.0, activated).astype(BF)

    def piece(at, side):
        return abuf.at[at, pl.ds(side * 64, 64)]

    own_act = pltpu.make_async_copy(act_own, abuf.at[z], local.at[13])
    own_act.start()
    going = {}
    for side in (0, 1):
        for way in (0, 1):
            going[way, 0, side] = links.copy(
                act_own.at[pl.ds(side * 64, 64)], piece(z, side), dz=1 if way == 0 else NZ - 1
            )
    for step in (1, 2, 3):
        for side in (0, 1):
            for way in (0, 1):
                if step == 3 and side != way:
                    continue
                going[way, step - 1, side].wait_recv()
                block = piece(lax.rem(z + (NZ - step if way == 0 else step), NZ), side)
                going[way, step, side] = links.copy(block, block, dz=1 if way == 0 else NZ - 1)
    own_act.wait()
    for one in ((0, 2, 1), (1, 2, 0), (0, 3, 0), (1, 3, 1)):
        going[one].wait_recv()
    for b in range(NZ):
        for k in range(NX):
            part[b, :, k * F : (k + 1) * F] = jnp.dot(abuf[b], wd[k], preferred_element_type=F32)
    over = []
    for k in range(NY):
        psend[k] = part[k * NC + 1 - c].astype(BF)
        over.append(links.copy(psend.at[k], precv.at[k], dc=1))
    for k in range(NY):
        over[k].wait_recv()
        both = (part[k * NC + c] + precv[k].astype(F32)).astype(BF)
        for j in range(NX):
            fsend[k, j] = both[:, j * F : (j + 1) * F]
    last = []
    for i, (dx, dy) in enumerate(PLANE):
        last.append(
            links.copy(fsend.at[lax.rem(y + dy, NY), lax.rem(x + dx, NX)], frecv.at[i], dx=dx, dy=dy)
        )
    result = hown[...].astype(F32) + fsend[y, x].astype(F32)
    for i, one in enumerate(last):
        one.wait_recv()
        result = result + frecv[i].astype(F32)
    out_ref[...] = result.astype(BF)
    links.drain()
    assert links.n <= NSEM, links.n


def local(
    layer_input, seq_lengths, delta_state, attn_gain, w_query, w_key, w_value, w_outgate, w_write, w_forget,
    forget_rate, head_gain, w_out, mixer_gain, w_gate, w_up, w_down,
):
    rate_w = jnp.concatenate([w_write.T, w_forget.T, jnp.zeros((12, F), BF)], axis=0)
    vmem = pl.BlockSpec(memory_space=pltpu.VMEM)
    smem = pl.BlockSpec(memory_space=pltpu.SMEM)
    hbm = pl.BlockSpec(memory_space=pl.ANY)
    scratch = [
        ((NX, NTP * R, F), BF),
        ((NTP * R, NX * F), BF),
        ((4, F, 256), BF),
        ((NX * F, 256), BF),
        ((NX, 16, F), BF),
        ((NZ, R, 256), F32),
        ((2, 4, 2, R, 128), BF),
        ((2, 4, 2, R, 128), BF),
        ((NZ, 8, R), F32),
        ((NZ, 8, R), F32),
        ((NX, 32, 256), BF),
        ((R, 256), BF),
        ((R, R), F32),
        ((32, 256), F32),
        ((32, 256), BF),
        ((NX, NZ * 32, 256), BF),
        ((NTP, R, F), BF),
        ((NTP, R, F), BF),
        ((R, F), BF),
        ((NX, NTP * R, F), BF),
        ((NZ, 8, R), F32),
        ((NZ, 8, R), F32),
        ((NX * F, WIN), BF),
        ((NX * F, WIN), BF),
        ((NX, WIN, F), BF),
        ((NZ, R, 2 * WIN), F32),
        ((2, 4, 2, R, WIN), BF),
        ((2, 4, 2, R, WIN), BF),
        ((R, WIN), BF),
        ((NZ, R, WIN), BF),
        ((NZ, R, NX * F), F32),
        ((NY, R, NX * F), BF),
        ((NY, R, NX * F), BF),
        ((NY, NX, R, F), BF),
        ((NX * NY, R, F), BF),
    ]
    return pl.pallas_call(
        body,
        out_shape=(
            jax.ShapeDtypeStruct((R, F), BF),
            jax.ShapeDtypeStruct(delta_state.shape, F32),
        ),
        in_specs=[
            vmem, smem, vmem, vmem, hbm, hbm, hbm, hbm, vmem, smem, vmem, vmem, vmem, hbm, hbm, hbm,
        ],
        out_specs=(vmem, vmem),
        scratch_shapes=[pltpu.VMEM(shape, dtype) for shape, dtype in scratch]
        + [
            pltpu.SemaphoreType.DMA((14,)),
            pltpu.SemaphoreType.DMA((NSEM,)),
            pltpu.SemaphoreType.DMA((NSEM,)),
        ],
        compiler_params=pltpu.CompilerParams(
            collective_id=0, has_side_effects=True, vmem_limit_bytes=56 * 1024 * 1024
        ),
    )(
        layer_input, seq_lengths, delta_state, attn_gain.reshape(8, NX * F), w_query, w_key, w_value, w_outgate,
        rate_w, forget_rate, head_gain.reshape(1, F), w_out, mixer_gain.reshape(8, NX * F), w_gate, w_up, w_down,
    )


def solution(mesh):
    split = Mesh(mesh.devices.reshape(NZ, NX, NY, NC), ("z", "x", "y", "c"))
    kv, tp = ("z", "x"), ("y", "c")
    in_specs = (
        P(tp, kv), P(kv), P(kv, tp, None, None), P(), P(kv, tp), P(kv, tp), P(kv, tp), P(kv, tp), P(kv, tp),
        P(kv, tp), P(tp), P(), P(tp, kv), P(), P(kv, tp), P(kv, tp), P(tp, kv),
    )
    out_specs = (P(tp, kv), P(kv, tp, None, None))
    return jax.shard_map(local, mesh=split, in_specs=in_specs, out_specs=out_specs, check_vma=False)
```

```python
import functools

import jax
import jax.numpy as jnp
from jax import lax
from jax.experimental import pallas as pl
from jax.experimental.pallas import tpu as pltpu
from jax.sharding import Mesh
from jax.sharding import PartitionSpec as P

D = 4096
NEW = 4
EPS = 1e-06
NZ, NX, NY, NC = 8, 4, 4, 2
NTP = NY * NC
R = 128
F = 128
WIN = 384
MESH = pl.DeviceIdType.MESH
BF = jnp.bfloat16
F32 = jnp.float32
PLANE = [(dx, dy) for dx in range(NX) for dy in range(NY) if dx or dy]
NSEM = 260
VMEM_LIMIT = 58 * 1024 * 1024


def silu(a):
    return a * jax.nn.sigmoid(a)


def rows_of(k):
    return pl.ds(pl.multiple_of(k * R, R), R)


def dot_t(a, b):
    return lax.dot_general(a, b, (((1,), (1,)), ((), ())), preferred_element_type=F32)


class Links:
    def __init__(self, send, recv):
        self.send, self.recv, self.n, self.all = send, recv, 0, []
        self.z, self.x = lax.axis_index("z"), lax.axis_index("x")
        self.y, self.c = lax.axis_index("y"), lax.axis_index("c")

    def copy(self, src, dst, dz=0, dx=0, dy=0, dc=0):
        to = (
            lax.rem(self.z + dz, NZ),
            lax.rem(self.x + dx, NX),
            lax.rem(self.y + dy, NY),
            lax.rem(self.c + dc, NC),
        )
        return self.copy_to(src, dst, to)

    def copy_to(self, src, dst, to):
        made = pltpu.make_async_remote_copy(
            src_ref=src,
            dst_ref=dst,
            send_sem=self.send.at[self.n],
            recv_sem=self.recv.at[self.n],
            device_id=to,
            device_id_type=MESH,
        )
        self.n += 1
        self.all.append(made)
        made.start()
        return made

    def drain(self):
        for made in self.all:
            made.wait_send()


def enter(links):
    z, x, y, c = links.z, links.x, links.y, links.c
    barrier = pltpu.get_barrier_semaphore()
    to = [(dz, 0, 0, 0) for dz in range(1, NZ)]
    to += [(0, dx, dy, 0) for dx, dy in PLANE]
    to += [(0, 0, dy, 1) for dy in range(NY)]
    for dz, dx, dy, dc in to:
        pl.semaphore_signal(
            barrier,
            inc=1,
            device_id=(lax.rem(z + dz, NZ), lax.rem(x + dx, NX), lax.rem(y + dy, NY), lax.rem(c + dc, NC)),
            device_id_type=MESH,
        )
    pl.semaphore_wait(barrier, len(to))


def gather_x_first(links, src, buf):
    z, x, y, c = links.z, links.x, links.y, links.c
    along_x = {dx: links.copy(src, buf.at[x, rows_of(y * NC + c)], dx=dx) for dx in (1, 3, 2)}
    along_y = {}
    for dy in (1, 3, 2):
        along_y[0, dy] = links.copy(src, buf.at[x, rows_of(y * NC + c)], dy=dy)
    forward = [links.copy(src, buf.at[x, rows_of(y * NC + c)], dc=1)]

    def finish():
        def block(dx, dy):
            return buf.at[lax.rem(x - dx + NX, NX), rows_of(lax.rem(y - dy + NY, NY) * NC + c)]

        for dx in (1, 3, 2):
            along_x[dx].wait_recv()
            for dy in (1, 3, 2):
                along_y[dx, dy] = links.copy(block(dx, 0), block(dx, 0), dy=dy)
            forward.append(links.copy(block(dx, 0), block(dx, 0), dc=1))
        for dx in (0, 1, 3, 2):
            for dy in (1, 3, 2):
                along_y[dx, dy].wait_recv()
                forward.append(links.copy(block(dx, dy), block(dx, dy), dc=1))
        for made in forward:
            made.wait_recv()

    return finish


def gather_straight(links, src, buf, rows):
    x, y, c = links.x, links.y, links.c

    def block(xs, ys):
        return buf.at[ys * NC + c, pl.ds(pl.multiple_of(xs * rows, rows), rows)]

    straight = [links.copy(src, block(x, y), dx=dx, dy=dy) for dx, dy in PLANE]
    forward = [links.copy(src, block(x, y), dc=1)]

    def finish():
        for (dx, dy), made in zip(PLANE, straight):
            made.wait_recv()
            came = block(lax.rem(x - dx + NX, NX), lax.rem(y - dy + NY, NY))
            forward.append(links.copy(came, came, dc=1))
        for made in forward:
            made.wait_recv()

    return finish


class RingSum:
    FIRST = ((0, 0, 0), (1, 0, 1), (0, 1, 1), (1, 1, 0))
    LATER = (
        ((0, 1, 0), (1, 1, 1)),
        ((0, 2, 1), (1, 2, 0)),
        ((0, 2, 0), (1, 2, 1)),
        ((0, 3, 1), (1, 3, 0)),
        ((0, 3, 0), (1, 3, 1)),
    )

    def __init__(self, links, block, sendbuf, recvbuf, width):
        self.links, self.block, self.sendbuf, self.recvbuf = links, block, sendbuf, recvbuf
        self.half, self.made = width // 2, {}

    def send(self, way, step, side):
        value = self.block(4 - step if way == 0 else 4 + step)[:, side * self.half : (side + 1) * self.half]
        before = self.made.get((way, step - 1, side))
        if before is not None:
            before.wait_recv()
            value = value + self.recvbuf[way, step - 1, side].astype(F32)
        self.sendbuf[way, step, side] = value.astype(BF)
        self.made[way, step, side] = self.links.copy(
            self.sendbuf.at[way, step, side], self.recvbuf.at[way, step, side], dz=1 if way == 0 else NZ - 1
        )

    def first(self):
        for one in self.FIRST:
            self.send(*one)

    def later(self, number):
        for one in self.LATER[number]:
            self.send(*one)

    def total(self):
        own = self.block(0)
        total = []
        for side in (1, 0):
            for way in (0, 1):
                self.made[way, 3, side].wait_recv()
            total.insert(
                0,
                own[:, side * self.half : (side + 1) * self.half]
                + self.recvbuf[0, 3, side].astype(F32)
                + self.recvbuf[1, 3, side].astype(F32),
            )
        return jnp.concatenate(total, axis=1)


class RingGather:
    def __init__(self, links, buf, rows):
        self.links, self.buf, self.rows, self.going = links, buf, rows // 2, {}

    def piece(self, at, side):
        return self.buf.at[at, pl.ds(side * self.rows, self.rows)]

    def send(self, way, step, side):
        if step:
            self.going[way, step - 1, side].wait_recv()
        block = self.piece(lax.rem(self.links.z + (NZ - step if way == 0 else step), NZ), side)
        self.going[way, step, side] = self.links.copy(block, block, dz=1 if way == 0 else NZ - 1)

    def step(self, step):
        for side in (0, 1):
            for way in (0, 1):
                if step < 3 or side == way:
                    self.send(way, step, side)
        if step == 3:
            for way in (0, 1):
                self.going[way, 2, 1 - way].wait_recv()

    def finish(self):
        for way in (0, 1):
            self.going[way, 3, way].wait_recv()


def square_rows(wide):
    squares = wide * wide
    squares = squares[:, :F] + squares[:, F : 2 * F] + squares[:, 2 * F : 3 * F] + squares[:, 3 * F :]
    if wide.shape[0] < R:
        squares = jnp.concatenate([squares, jnp.zeros((R - wide.shape[0], F), F32)], axis=0)
    ones = jnp.ones((16, F), BF)
    high = squares.astype(BF)
    low = (squares - high.astype(F32)).astype(BF)
    return (dot_t(ones, high) + dot_t(ones, low))[:8]


def stats_total(own, got, made):
    total = own
    for offset in range(1, NZ):
        made[offset].wait_recv()
        total = total + got[offset]
    return jnp.concatenate([total, jnp.zeros((R - 8, R), F32)], axis=0).T


def body(
    x_hbm, len_hbm, state_hbm, gain1_hbm, wq, wk, wv, wo, write_hbm, forget_hbm, rate_hbm, head_gain_hbm, w_out,
    gain2_hbm, w_gate, w_up, w_down,
    out_ref, next_ref,
    xbuf, w4, wr, rate_w, rw, p1, s1, r1, stats1, got1, pre, mine, cols, readings, mixed_own, wz, mz, obuf, orecv,
    hown, hb, stats2, got2, wg, wu, wd, p2, s2, r2, abuf, part, psend, precv, fsend, frecv,
    x_ref, len_ref, state_ref, gain1_ref, write_ref, forget_ref, rate_ref, head_gain_ref, gain2_ref,
    local, send, recv, over_send, over_recv,
):
    links = Links(send, recv)
    z, x, y, c = links.z, links.x, links.y, links.c
    tp = y * NC + c

    locals_ = [pltpu.make_async_copy(w, w4.at[i], local.at[i]) for i, w in enumerate((wq, wk, wv, wo))]

    def window(at):
        return pl.ds(pl.multiple_of((at * 3 - at // (NX - 1)) * F, F), WIN)

    feats = pl.ds(pl.multiple_of(x * F, F), F)
    given = [
        pltpu.make_async_copy(far, near, local.at[11 + i])
        for i, (far, near) in enumerate(
            (
                (x_hbm, x_ref), (write_hbm, write_ref), (forget_hbm, forget_ref), (gain1_hbm, gain1_ref),
                (gain2_hbm, gain2_ref), (len_hbm, len_ref), (rate_hbm, rate_ref), (head_gain_hbm, head_gain_ref),
                (state_hbm, state_ref),
            )
        )
    ]
    for one in given:
        one.start()
    own_x = pltpu.make_async_copy(x_hbm, xbuf.at[x, rows_of(tp)], local.at[4])
    own_out = pltpu.make_async_copy(w_out, wz.at[x], local.at[5])
    own_late = [
        pltpu.make_async_copy(w_gate.at[:, window(x)], wg.at[feats], local.at[6]),
        pltpu.make_async_copy(w_up.at[:, window(x)], wu.at[feats], local.at[7]),
        pltpu.make_async_copy(w_down.at[window(x)], wd.at[x], local.at[8]),
    ]
    for one in locals_ + [own_x, own_out] + own_late:
        one.start()
    for one in given[:8]:
        one.wait()
    small = [write_ref[...].astype(F32), forget_ref[...].astype(F32), jnp.zeros((12, F), F32)]
    rate_w[...] = jnp.concatenate(small, axis=0).astype(BF)
    rw[x] = rate_w[...]
    enter(links)

    finish = gather_x_first(links, x_ref, xbuf)
    for one in locals_:
        one.wait()
    own_w = pltpu.make_async_copy(w4.at[x], wr.at[feats], local.at[9])
    own_w.start()
    early, late, outs = [], [], []
    for dx in (1, 3, 2):
        to = lax.rem(x + dx, NX)
        early.append(links.copy(w4.at[to], wr.at[feats], dx=dx))
        early.append(links.copy(rate_w, rw.at[x], dx=dx))
    for dx in (1, 3, 2):
        outs.append(links.copy(w_out, wz.at[x], dx=dx))
    for dx in (1, 3, 2):
        to = lax.rem(x + dx, NX)
        late.append(links.copy(w_gate.at[:, window(to)], wg.at[feats], dx=dx))
        late.append(links.copy(w_up.at[:, window(to)], wu.at[feats], dx=dx))
    for dx in (1, 3, 2):
        to = lax.rem(x + dx, NX)
        late.append(links.copy(w_down.at[window(to)], wd.at[x], dx=dx))

    which = lax.broadcasted_iota(jnp.int32, (32, F), 0)

    def gain_of(ref):
        wide = ref[...].astype(F32)
        return jnp.concatenate(
            [jnp.sum(jnp.where(which == z * NX + k, wide, 0.0), axis=0, keepdims=True) for k in range(NX)], axis=1
        )

    gain1, gain2 = gain_of(gain1_ref), gain_of(gain2_ref)
    own_x.wait()
    own_w.wait()
    finish()
    for one in early:
        one.wait_recv()

    sub = lax.broadcasted_iota(jnp.int32, (8, R), 0)
    made1, ready = {}, {}

    def projected(offset):
        if offset not in ready:
            ready[offset] = True
            at = rows_of(lax.rem(z + offset, NZ))
            wide = jnp.concatenate([xbuf[k, at, :] for k in range(NX)], axis=1).astype(F32)
            normed = (wide * gain1).astype(BF)
            p1[offset] = jnp.dot(normed, wr[...], preferred_element_type=F32)
            stat = jnp.where(sub == 4, square_rows(wide), 0.0)
            for k in range(NX):
                stat = stat + dot_t(rw[k], normed[:, k * F : (k + 1) * F])[:8]
            stats1[offset] = stat
            if offset:
                made1[offset] = links.copy(stats1.at[offset], got1.at[offset], dz=offset)
        return p1[offset]

    ring = RingSum(links, projected, s1, r1, 256)
    ring.first()
    for number in range(5):
        ring.later(number)
    mine[...] = ring.total().astype(BF)
    quarter = pl.ds(pl.multiple_of(x * 32, 32), 32)
    own_pre = pltpu.make_async_copy(mine.at[quarter], pre.at[x], local.at[10])
    own_pre.start()
    parts = []
    for dx in (2, 1, 3):
        to = lax.rem(x + dx, NX)
        parts.append(links.copy(mine.at[pl.ds(pl.multiple_of(to * 32, 32), 32)], pre.at[x], dx=dx))
    cols[...] = stats_total(stats1[0], got1, made1)
    stat = cols[quarter, :]
    scale = lax.rsqrt(stat[:, 4:5] / D + EPS)
    lane = lax.broadcasted_iota(jnp.int32, (32, R), 1)
    row = lax.broadcasted_iota(jnp.int32, (32, R), 0)
    live = jnp.zeros((32, R), F32)
    for s in range(8):
        inside = (row // NEW == s) & (lax.rem(row, NEW) < len_ref[s])
        live = live + jnp.where(inside, 1.0, 0.0)
    rated = stat * scale
    beta = jax.nn.sigmoid(rated) * live
    rate = jnp.where(lane == 2, rate_ref[0], jnp.where(lane == 3, rate_ref[1], 0.0))
    softplus = jnp.maximum(rated, 0.0) + jnp.log1p(jnp.exp(-jnp.abs(rated)))
    keep = jnp.exp(-rate * softplus * live)
    own_pre.wait()
    for one in parts:
        one.wait_recv()
    given[8].wait()
    query, key, value = (silu(pre[i].astype(F32) * scale) for i in range(3))
    gate = silu(pre[3].astype(F32) * scale)

    def unit(a):
        return a * lax.rsqrt(jnp.sum(a * a, axis=1, keepdims=True) + EPS)

    stacked = []
    for h in range(2):
        at = slice(h * F, (h + 1) * F)
        stacked += [unit(query[:, at]) * F ** (-0.5), unit(key[:, at])]
    turned = jnp.concatenate(stacked, axis=0).T
    for s in range(8):
        for h in range(2):
            state = state_ref[s, h]
            for t in range(NEW):
                r = s * NEW + t
                q_col = turned[:, h * 64 + r : h * 64 + r + 1]
                k_col = turned[:, h * 64 + 32 + r : h * 64 + 33 + r]
                hold = keep[r : r + 1, 2 + h : 3 + h]
                recalled = jnp.sum(k_col * state, axis=0, keepdims=True)
                update = beta[r : r + 1, h : h + 1] * (value[r : r + 1, h * F : (h + 1) * F] - hold * recalled)
                state = hold * state + k_col * update
                readings[r : r + 1, h * F : (h + 1) * F] = jnp.sum(q_col * state, axis=0, keepdims=True)
            next_ref[s, h] = state
    for h in range(2):
        at = slice(h * F, (h + 1) * F)
        read = readings[:, at] * live
        normed = read * lax.rsqrt(jnp.mean(read * read, axis=1, keepdims=True) + EPS)
        mixed_own[:, at] = (normed * head_gain_ref[...] * gate[:, at]).astype(BF)

    along_z = {dz: links.copy(mixed_own, mz.at[z], dz=dz) for dz in (4, 3, 5, 2, 6, 1, 7)}
    mz[z] = mixed_own[...]
    own_out.wait()
    for one in outs:
        one.wait_recv()
    for dz in (1, 7, 2, 6, 3, 5, 4):
        along_z[dz].wait_recv()
    heads = jnp.concatenate([mz[k] for k in range(NZ)], axis=0)
    for k in range(NX):
        terms = jnp.dot(heads, wz[k], preferred_element_type=F32).astype(BF)
        for h in range(2):
            for b in range(NTP):
                obuf[h, b, :, k * F : (k + 1) * F] = terms[b * 32 + h * 16 : b * 32 + h * 16 + 16]
    made = {}
    for h in range(2):
        for k in (4, 3, 5, 2, 6, 1, 7):
            to = lax.rem(tp + k, NTP)
            made[h, k] = links.copy_to(obuf.at[h, to], orecv.at[h, k], (z, x, to // NC, lax.rem(to, NC)))

    finish = []
    for h in range(2):
        attended = obuf[h, tp].astype(F32)
        for k in range(1, NTP):
            made[h, k].wait_recv()
            attended = attended + orecv[h, k].astype(F32)
        at = pl.ds(pl.multiple_of(tp * R + x * 32 + h * 16, 16), 16)
        given = jnp.concatenate([xbuf[k, at, :] for k in range(NX)], axis=1).astype(F32)
        hown[h] = (given + attended).astype(BF)
        hb[h, tp, pl.ds(pl.multiple_of(x * 16, 16), 16), :] = hown[h]
        finish.append(gather_straight(links, hown.at[h], hb.at[h], 16))

    made2, ready2 = ({}, {}), ({}, {})

    def mixer(h):
        def block(offset):
            if offset not in ready2[h]:
                ready2[h][offset] = True
                wide = hb[h, lax.rem(z + offset, NZ)].astype(F32)
                normed = (wide * gain2).astype(BF)
                p2[h, offset, :, :WIN] = jnp.dot(normed, wg[...], preferred_element_type=F32)
                p2[h, offset, :, WIN:] = jnp.dot(normed, wu[...], preferred_element_type=F32)
                stats2[h, offset] = square_rows(wide)
                if offset:
                    made2[h][offset] = links.copy(stats2.at[h, offset], got2.at[h, offset], dz=offset)
            return p2[h, offset]

        return RingSum(links, block, s2.at[h], r2.at[h], 2 * WIN)

    sums = [mixer(h) for h in range(2)]
    gathers = [RingGather(links, abuf.at[h], 64) for h in range(2)]
    odd = lax.rem(z + c, 2)
    partner = (z, x, y, 1 - c)

    def activate(h):
        total = sums[h].total()
        scale2 = lax.rsqrt(stats_total(stats2[h, 0], got2.at[h], made2[h])[:64, 0:1] / D + EPS)
        activated = silu(scale2 * total[:, :WIN]) * (scale2 * total[:, WIN:])
        again = (lax.broadcasted_iota(jnp.int32, (64, WIN), 1) < F) & (x == NX - 1)
        abuf[h, z] = jnp.where(again, 0.0, activated).astype(BF)
        gathers[h].step(0)
        down(h, 0)

    def down(h, offset):
        block = abuf[h, lax.rem(z + offset, NZ)]
        for k in range(NX):
            part[h, offset, :, k * F : (k + 1) * F] = jnp.dot(block, wd[k], preferred_element_type=F32)

    def over(h, base, other):
        at = base + other
        return at, pltpu.make_async_remote_copy(
            src_ref=psend.at[h, at],
            dst_ref=precv.at[h, at],
            send_sem=over_send.at[h, at],
            recv_sem=over_recv.at[h, at],
            device_id=partner,
            device_id_type=MESH,
        )

    def give(h, base):
        at, one = over(h, base, 1 - odd)
        psend[h, at] = part[h, at].astype(BF)
        one.start()

    def gather_step(h, step):
        gathers[h].step(step) if step < 4 else gathers[h].finish()
        if step < 4:
            down(h, NZ - step)
            down(h, step)
        else:
            down(h, 4)
        give(h, (None, 0, 6, 2, 4)[step])

    last = {}

    def spread(h):
        for base in (0, 6, 2, 4):
            at, one = over(h, base, odd)
            one.wait_recv()
            both = (part[h, at] + precv[h, at].astype(F32)).astype(BF)
            to = lax.rem(z + at, NZ) // NC
            for k in range(NX):
                fsend[h, to, k] = both[:, k * F : (k + 1) * F]
        for i, (dx, dy) in enumerate(PLANE):
            last[h, i] = links.copy(
                fsend.at[h, lax.rem(y + dy, NY), lax.rem(x + dx, NX)], frecv.at[h, i], dx=dx, dy=dy
            )

    def put(h):
        result = hb[h, tp, :, feats].astype(F32) + fsend[h, y, x].astype(F32)
        for i in range(len(PLANE)):
            last[h, i].wait_recv()
            result = result + frecv[h, i].astype(F32)
        result = result.astype(BF)
        for k in range(NX):
            out_ref[k * 32 + h * 16 : k * 32 + h * 16 + 16, :] = result[k * 16 : (k + 1) * 16]

    finish[0]()
    for one in own_late:
        one.wait()
    for one in late:
        one.wait_recv()
    sums[0].first()
    finish[1]()
    sums[0].later(0)
    sums[1].first()
    sums[0].later(1)
    sums[0].later(2)
    sums[1].later(0)
    sums[1].later(1)
    sums[0].later(3)
    sums[0].later(4)
    sums[1].later(2)
    sums[1].later(3)
    sums[1].later(4)
    activate(0)
    activate(1)
    gather_step(0, 1)
    gather_step(1, 1)
    gather_step(0, 2)
    gather_step(1, 2)
    gather_step(0, 3)
    gather_step(1, 3)
    gather_step(0, 4)
    spread(0)
    gather_step(1, 4)
    spread(1)
    put(0)
    put(1)
    links.drain()
    for h in range(2):
        for base in (0, 6, 2, 4):
            over(h, base, 1 - odd)[1].wait_send()
    assert links.n <= NSEM, links.n


def local(
    layer_input, seq_lengths, delta_state, attn_gain, w_query, w_key, w_value, w_outgate, w_write, w_forget,
    forget_rate, head_gain, w_out, mixer_gain, w_gate, w_up, w_down,
):
    vmem = pl.BlockSpec(memory_space=pltpu.VMEM)
    hbm = pl.BlockSpec(memory_space=pltpu.HBM)
    scratch = [
        ((NX, NTP * R, F), BF),
        ((4, F, 256), BF),
        ((NX * F, 256), BF),
        ((16, F), BF),
        ((NX, 16, F), BF),
        ((NZ, R, 256), F32),
        ((2, 4, 2, R, 128), BF),
        ((2, 4, 2, R, 128), BF),
        ((NZ, 8, R), F32),
        ((NZ, 8, R), F32),
        ((NX, 32, 256), BF),
        ((R, 256), BF),
        ((R, R), F32),
        ((32, 256), F32),
        ((32, 256), BF),
        ((NX, 256, F), BF),
        ((NZ, 32, 256), BF),
        ((2, NTP, 16, NX * F), BF),
        ((2, NTP, 16, NX * F), BF),
        ((2, 16, NX * F), BF),
        ((2, NTP, 64, NX * F), BF),
        ((2, NZ, 8, R), F32),
        ((2, NZ, 8, R), F32),
        ((NX * F, WIN), BF),
        ((NX * F, WIN), BF),
        ((NX, WIN, F), BF),
        ((2, NZ, 64, 2 * WIN), F32),
        ((2, 2, 4, 2, 64, WIN), BF),
        ((2, 2, 4, 2, 64, WIN), BF),
        ((2, NZ, 64, WIN), BF),
        ((2, NZ, 64, NX * F), F32),
        ((2, NZ, 64, NX * F), BF),
        ((2, NZ, 64, NX * F), BF),
        ((2, NY, NX, 64, F), BF),
        ((2, NX * NY, 64, F), BF),
    ]
    held = [
        pltpu.VMEM((R, F), BF),
        pltpu.SMEM((8,), jnp.int32),
        pltpu.VMEM(delta_state.shape, F32),
        pltpu.VMEM((32, F), BF),
        pltpu.VMEM((2, F), BF),
        pltpu.VMEM((2, F), BF),
        pltpu.SMEM((2,), F32),
        pltpu.VMEM((1, F), F32),
        pltpu.VMEM((32, F), BF),
    ]
    return pl.pallas_call(
        body,
        out_shape=(
            jax.ShapeDtypeStruct((R, F), BF),
            jax.ShapeDtypeStruct(delta_state.shape, F32),
        ),
        in_specs=[
            hbm, hbm, hbm, hbm, hbm, hbm, hbm, hbm, hbm, hbm, hbm, hbm, hbm, hbm, hbm, hbm, hbm,
        ],
        out_specs=(vmem, vmem),
        scratch_shapes=[pltpu.VMEM(shape, dtype) for shape, dtype in scratch]
        + held
        + [
            pltpu.SemaphoreType.DMA((20,)),
            pltpu.SemaphoreType.DMA((NSEM,)),
            pltpu.SemaphoreType.DMA((NSEM,)),
            pltpu.SemaphoreType.DMA((2, NZ)),
            pltpu.SemaphoreType.DMA((2, NZ)),
        ],
        compiler_params=pltpu.CompilerParams(
            collective_id=0, has_side_effects=True, vmem_limit_bytes=VMEM_LIMIT
        ),
    )(
        layer_input, seq_lengths, delta_state, attn_gain.reshape(32, F), w_query, w_key, w_value, w_outgate,
        w_write.T, w_forget.T, forget_rate, head_gain.reshape(1, F), w_out, mixer_gain.reshape(32, F), w_gate, w_up,
        w_down,
    )


def solution(mesh):
    split = Mesh(mesh.devices.reshape(NZ, NX, NY, NC), ("z", "x", "y", "c"))
    kv, tp = ("z", "x"), ("y", "c")
    in_specs = (
        P(tp, kv), P(kv), P(kv, tp, None, None), P(), P(kv, tp), P(kv, tp), P(kv, tp), P(kv, tp), P(kv, tp),
        P(kv, tp), P(tp), P(), P(tp, kv), P(), P(kv, tp), P(kv, tp), P(tp, kv),
    )
    out_specs = (P(tp, kv), P(kv, tp, None, None))
    return jax.shard_map(local, mesh=split, in_specs=in_specs, out_specs=out_specs, check_vma=False)
```

```python
import math

import jax
import jax.numpy as jnp
from jax import lax
from jax.experimental import pallas as pl
from jax.experimental.pallas import tpu as pltpu
from jax.sharding import Mesh
from jax.sharding import PartitionSpec as P

D = 4096
NEW = 4
EPS = 1e-06
NZ, NX, NY, NC = 8, 4, 4, 2
NTP = NY * NC
R = 128
F = 128
WIN = 384
MESH = pl.DeviceIdType.MESH
BF = jnp.bfloat16
F32 = jnp.float32
PLANE = [(dx, dy) for dx in range(NX) for dy in range(NY) if dx or dy]
NRECV = 135
NSEND = 11
VMEM_LIMIT = 58 * 1024 * 1024


def silu(a):
    return a * jax.nn.sigmoid(a)


def rows_of(k):
    return pl.ds(pl.multiple_of(k * R, R), R)


def dot_t(a, b):
    return lax.dot_general(a, b, (((1,), (1,)), ((), ())), preferred_element_type=F32)


class Gate:
    def __init__(self, links):
        self.links, self.index, self.size = links, links.fresh(), 0

    def wait(self):
        self.links.wait_bytes(self.links.recv.at[self.index], self.size)


class Links:
    def __init__(self, send, recv, ruler):
        self.send, self.recv, self.ruler, self.n, self.sent = send, recv, ruler, 0, []
        self.z, self.x = lax.axis_index("z"), lax.axis_index("x")
        self.y, self.c = lax.axis_index("y"), lax.axis_index("c")

    def fresh(self):
        self.n += 1
        return self.n - 1

    def phase(self):
        self.sent.append(0)

    def copy(self, src, dst, dz=0, dx=0, dy=0, dc=0, gate=None):
        to = (
            lax.rem(self.z + dz, NZ),
            lax.rem(self.x + dx, NX),
            lax.rem(self.y + dy, NY),
            lax.rem(self.c + dc, NC),
        )
        return self.copy_to(src, dst, to, gate)

    def copy_to(self, src, dst, to, gate=None, index=None):
        size = math.prod(src.shape) * jnp.dtype(src.dtype).itemsize
        self.sent[-1] += size
        if gate is not None:
            gate.size += size
            index = gate.index
        elif index is None:
            index = self.fresh()
        made = pltpu.make_async_remote_copy(
            src_ref=src,
            dst_ref=dst,
            send_sem=self.send.at[len(self.sent) - 1],
            recv_sem=self.recv.at[index],
            device_id=to,
            device_id_type=MESH,
        )
        made.start()
        return made

    def wait_bytes(self, sem, size):
        part = self.ruler.at[pl.ds(0, size // (2 * F))]
        pltpu.make_async_copy(part, part, sem).wait()

    def drain(self):
        for i, size in enumerate(self.sent):
            self.wait_bytes(self.send.at[i], size)
        assert self.n <= NRECV and len(self.sent) <= NSEND, (self.n, len(self.sent))


def greet(links):
    z, x, y, c = links.z, links.x, links.y, links.c
    barrier = pltpu.get_barrier_semaphore()
    to = [(dz, dx, 0, 0) for dz in (0, 1, NZ - 1) for dx in range(NX) if dz or dx]
    to += [(dz, 0, 0, 0) for dz in range(2, NZ - 1)]
    to += [(0, dx, dy, 0) for dx in range(NX) for dy in range(1, NY)]
    to += [(0, 0, dy, 1) for dy in range(NY)]
    for dz, dx, dy, dc in to:
        pl.semaphore_signal(
            barrier,
            inc=1,
            device_id=(lax.rem(z + dz, NZ), lax.rem(x + dx, NX), lax.rem(y + dy, NY), lax.rem(c + dc, NC)),
            device_id_type=MESH,
        )
    return lambda: pl.semaphore_wait(barrier, len(to))


def gather_x_first(links, src, buf):
    z, x, y, c = links.z, links.x, links.y, links.c
    along_x = {dx: links.copy(src, buf.at[x, rows_of(y * NC + c)], dx=dx) for dx in (1, 3, 2)}
    along_y = {}
    for dy in (1, 3, 2):
        along_y[0, dy] = links.copy(src, buf.at[x, rows_of(y * NC + c)], dy=dy)
    forward = Gate(links)
    links.copy(src, buf.at[x, rows_of(y * NC + c)], dc=1, gate=forward)

    def finish():
        def block(dx, dy):
            return buf.at[lax.rem(x - dx + NX, NX), rows_of(lax.rem(y - dy + NY, NY) * NC + c)]

        for dx in (1, 3, 2):
            along_x[dx].wait_recv()
            for dy in (1, 3, 2):
                along_y[dx, dy] = links.copy(block(dx, 0), block(dx, 0), dy=dy)
            links.copy(block(dx, 0), block(dx, 0), dc=1, gate=forward)
        for dx in (0, 1, 3, 2):
            for dy in (1, 3, 2):
                along_y[dx, dy].wait_recv()
                links.copy(block(dx, dy), block(dx, dy), dc=1, gate=forward)
        forward.wait()

    return finish


def gather_straight(links, src, buf, rows):
    x, y, c = links.x, links.y, links.c

    def block(xs, ys):
        return buf.at[ys * NC + c, pl.ds(pl.multiple_of(xs * rows, rows), rows)]

    straight = [links.copy(src, block(x, y), dx=dx, dy=dy) for dx, dy in PLANE]
    forward = Gate(links)
    links.copy(src, block(x, y), dc=1, gate=forward)

    def finish():
        for (dx, dy), made in zip(PLANE, straight):
            made.wait_recv()
            came = block(lax.rem(x - dx + NX, NX), lax.rem(y - dy + NY, NY))
            links.copy(came, came, dc=1, gate=forward)
        forward.wait()

    return finish


FAR, THREE, TWO, ONE = range(4)


class RingSum:
    FIRST = ((0, FAR, 0), (1, FAR, 1), (0, THREE, 1), (1, THREE, 0), (0, THREE, 0), (1, THREE, 1))
    LATER = (((0, TWO, 1), (1, TWO, 0)), ((0, TWO, 0), (1, TWO, 1)), ((0, ONE, 1), (1, ONE, 0)), ((0, ONE, 0), (1, ONE, 1)))

    def __init__(self, links, block, sendbuf, recvbuf, width):
        self.links, self.block, self.sendbuf, self.recvbuf = links, block, sendbuf, recvbuf
        self.half, self.made = width // 2, {}

    def value(self, way, kind, side):
        value = self.block(4 - kind if way == 0 else 4 + kind)[:, side * self.half : (side + 1) * self.half]
        before = [(way, kind - 1, side)] if kind > THREE else []
        if kind == TWO and side == way:
            before.append((way, FAR, side))
        for one in before:
            self.made[one].wait_recv()
            value = value + self.recvbuf[one].astype(F32)
        return value

    def send(self, way, kind, side):
        at = (way, kind, side)
        self.sendbuf[at] = self.value(*at).astype(BF)
        hops = 2 if kind == FAR else 1
        self.made[at] = self.links.copy(
            self.sendbuf.at[at], self.recvbuf.at[at], dz=hops if way == 0 else NZ - hops
        )

    def first(self):
        for one in self.FIRST:
            self.send(*one)

    def later(self, number):
        for one in self.LATER[number]:
            self.send(*one)

    def total(self):
        own = self.block(0)
        total = []
        for side in (0, 1):
            value = own[:, side * self.half : (side + 1) * self.half]
            for way in (0, 1):
                self.made[way, ONE, side].wait_recv()
                value = value + self.recvbuf[way, ONE, side].astype(F32)
            total.append(value)
        return jnp.concatenate(total, axis=1)


class RingSumWhole:
    def __init__(self, links, block, sendbuf, recvbuf, width):
        self.links, self.block, self.sendbuf, self.recvbuf = links, block, sendbuf, recvbuf
        self.half, self.made = width // 2, {}

    def lanes(self, side):
        return slice(None) if side is None else slice(side * self.half, (side + 1) * self.half)

    def send(self, way, kind, side=None):
        lanes = self.lanes(side)
        value = self.block(4 - kind if way == 0 else 4 + kind)[:, lanes]
        if kind == THREE and side == way:
            self.made[way, FAR, side].wait_recv()
            value = value + self.recvbuf[way, FAR, :, lanes].astype(F32)
        elif kind > THREE:
            for before in ((way, THREE, 1 - way), (way, THREE, way)) if kind == TWO else ((way, TWO, None),):
                self.made[before].wait_recv()
            value = value + self.recvbuf[way, kind - 1].astype(F32)
        self.sendbuf[way, kind, :, lanes] = value.astype(BF)
        at = (way, kind) if side is None else (way, kind, slice(None), pl.ds(side * self.half, self.half))
        self.made[way, kind, side] = self.links.copy(
            self.sendbuf.at[at], self.recvbuf.at[at], dz=1 if way == 0 else NZ - 1
        )

    def first(self):
        for way in (0, 1):
            self.send(way, FAR, way)
        for way in (0, 1):
            self.send(way, THREE, 1 - way)

    def later(self, number):
        for way in (0, 1):
            self.send(way, *((THREE, way), (TWO, None), (ONE, None))[number])

    def total(self):
        value = self.block(0)
        for way in (0, 1):
            self.made[way, ONE, None].wait_recv()
            value = value + self.recvbuf[way, ONE].astype(F32)
        return value


class RingGather:
    def __init__(self, links, buf, rows):
        self.links, self.buf, self.rows, self.going = links, buf, rows // 2, {}

    def step(self, step):
        for way in (0, 1):
            if step:
                self.going[way, step].wait_recv()
            at = lax.rem(self.links.z + (NZ - step if way == 0 else step), NZ)
            if step == 2:
                half = self.buf.at[at, pl.ds(way * self.rows, self.rows)]
                self.going[way, 4] = self.links.copy(half, half, dz=2 if way == 0 else NZ - 2)
            if step < 3:
                self.going[way, step + 1] = self.links.copy(
                    self.buf.at[at], self.buf.at[at], dz=1 if way == 0 else NZ - 1
                )

    def finish(self):
        for way in (0, 1):
            self.going[way, 4].wait_recv()


def square_rows(wide):
    squares = wide * wide
    squares = squares[:, :F] + squares[:, F : 2 * F] + squares[:, 2 * F : 3 * F] + squares[:, 3 * F :]
    if wide.shape[0] < R:
        squares = jnp.concatenate([squares, jnp.zeros((R - wide.shape[0], F), F32)], axis=0)
    ones = jnp.ones((16, F), BF)
    high = squares.astype(BF)
    low = (squares - high.astype(F32)).astype(BF)
    return (dot_t(ones, high) + dot_t(ones, low))[:8]


def stats_total(own, got, gate):
    gate.wait()
    total = own
    for offset in range(1, NZ):
        total = total + got[offset]
    return jnp.concatenate([total, jnp.zeros((R - 8, R), F32)], axis=0).T


def body(
    x_hbm, len_hbm, state_hbm, gain1_hbm, wq, wk, wv, wo, write_hbm, forget_hbm, rate_hbm, head_gain_hbm, w_out,
    gain2_hbm, w_gate, w_up, w_down,
    out_ref, next_hbm,
    xbuf, w4, wr, rate_w, rw, p1, s1, r1, stats1, got1, pre, last1, cols, readings, mixed_own, wz, mz, obuf, orecv,
    hown, hb, stats2, got2, wg, wu, wd, p2, s2, r2, abuf, part, psend, precv, fsend, frecv,
    x_ref, len_ref, state_ref, gain1_ref, write_ref, forget_ref, rate_ref, head_gain_ref, gain2_ref,
    ruler, local, send, recv,
):
    links = Links(send, recv, ruler)
    links.phase()
    arrive = greet(links)
    z, x, y, c = links.z, links.x, links.y, links.c
    tp = y * NC + c

    locals_ = [pltpu.make_async_copy(w, w4.at[i], local.at[i]) for i, w in enumerate((wq, wk, wv, wo))]

    def window(at):
        return pl.ds(pl.multiple_of((at * 3 - at // (NX - 1)) * F, F), WIN)

    feats = pl.ds(pl.multiple_of(x * F, F), F)
    given = [
        pltpu.make_async_copy(far, near, local.at[11 + i])
        for i, (far, near) in enumerate(
            (
                (x_hbm, x_ref), (write_hbm, write_ref), (forget_hbm, forget_ref), (gain1_hbm, gain1_ref),
                (gain2_hbm, gain2_ref), (len_hbm, len_ref), (rate_hbm, rate_ref), (head_gain_hbm, head_gain_ref),
                (state_hbm, state_ref),
            )
        )
    ]
    for one in given:
        one.start()
    own_x = pltpu.make_async_copy(x_hbm, xbuf.at[x, rows_of(tp)], local.at[4])
    own_out = pltpu.make_async_copy(w_out, wz.at[x], local.at[5])
    own_late = [
        pltpu.make_async_copy(w_gate.at[:, window(x)], wg.at[feats], local.at[6]),
        pltpu.make_async_copy(w_up.at[:, window(x)], wu.at[feats], local.at[7]),
        pltpu.make_async_copy(w_down.at[window(x)], wd.at[x], local.at[8]),
    ]
    for one in locals_ + [own_x, own_out] + own_late:
        one.start()
    for one in given[:8]:
        one.wait()
    small = [write_ref[...].astype(F32), forget_ref[...].astype(F32), jnp.zeros((12, F), F32)]
    rate_w[...] = jnp.concatenate(small, axis=0).astype(BF)
    rw[x] = rate_w[...]
    arrive()

    finish = gather_x_first(links, x_ref, xbuf)
    for one in locals_:
        one.wait()
    own_w = pltpu.make_async_copy(w4.at[x], wr.at[feats], local.at[9])
    own_w.start()
    early, early_rates, late, outs = Gate(links), Gate(links), Gate(links), Gate(links)
    for dx in (1, 3, 2):
        to = lax.rem(x + dx, NX)
        links.copy(w4.at[to], wr.at[feats], dx=dx, gate=early)
        links.copy(rate_w, rw.at[x], dx=dx, gate=early_rates)
    links.phase()
    for dx in (1, 3, 2):
        links.copy(w_out, wz.at[x], dx=dx, gate=outs)
    for dx in (1, 3, 2):
        to = lax.rem(x + dx, NX)
        links.copy(w_gate.at[:, window(to)], wg.at[feats], dx=dx, gate=late)
        links.copy(w_up.at[:, window(to)], wu.at[feats], dx=dx, gate=late)
    for dx in (1, 3, 2):
        to = lax.rem(x + dx, NX)
        links.copy(w_down.at[window(to)], wd.at[x], dx=dx, gate=late)
    links.phase()

    which = lax.broadcasted_iota(jnp.int32, (32, F), 0)

    def gain_of(ref):
        wide = ref[...].astype(F32)
        return jnp.concatenate(
            [jnp.sum(jnp.where(which == z * NX + k, wide, 0.0), axis=0, keepdims=True) for k in range(NX)], axis=1
        )

    gain1, gain2 = gain_of(gain1_ref), gain_of(gain2_ref)
    own_x.wait()
    own_w.wait()
    finish()
    early.wait()
    early_rates.wait()
    links.phase()

    sub = lax.broadcasted_iota(jnp.int32, (8, R), 0)
    stats_gate, ready = Gate(links), {}

    def projected(offset):
        if offset not in ready:
            ready[offset] = True
            at = rows_of(lax.rem(z + offset, NZ))
            wide = jnp.concatenate([xbuf[k, at, :] for k in range(NX)], axis=1).astype(F32)
            normed = (wide * gain1).astype(BF)
            p1[offset] = jnp.dot(normed, wr[...], preferred_element_type=F32)
            stat = jnp.where(sub == 4, square_rows(wide), 0.0)
            for k in range(NX):
                stat = stat + dot_t(rw[k], normed[:, k * F : (k + 1) * F])[:8]
            stats1[offset] = stat
            if offset:
                links.copy(stats1.at[offset], got1.at[offset], dz=offset, gate=stats_gate)
        return p1[offset]

    def part_of(at):
        return pl.ds(pl.multiple_of(at * 32, 32), 32)

    ring = RingSum(links, projected, s1, r1, 256)
    ring.first()
    ring.later(0)
    ring.later(1)
    pre_gate = Gate(links)
    last1[2] = projected(0).astype(BF)
    for dx in range(1, NX):
        links.copy(last1.at[2, part_of(lax.rem(x + dx, NX))], pre.at[x, 2], dx=dx, gate=pre_gate)
    for way in (0, 1):
        for side in (1 - way, way):
            last1[way, :, side * F : (side + 1) * F] = ring.value(way, ONE, side).astype(BF)
        for dx in (2, 1, 3, 0):
            links.copy(
                last1.at[way, part_of(lax.rem(x + dx, NX))], pre.at[x, way], dz=1 if way == 0 else NZ - 1, dx=dx,
                gate=pre_gate,
            )
    quarter = part_of(x)
    pre[x, 2] = last1[2, quarter, :]
    cols[...] = stats_total(stats1[0], got1, stats_gate)
    stat = cols[quarter, :]
    scale = lax.rsqrt(stat[:, 4:5] / D + EPS)
    lane = lax.broadcasted_iota(jnp.int32, (32, R), 1)
    row = lax.broadcasted_iota(jnp.int32, (32, R), 0)
    live = jnp.zeros((32, R), F32)
    for s in range(8):
        inside = (row // NEW == s) & (lax.rem(row, NEW) < len_ref[s])
        live = live + jnp.where(inside, 1.0, 0.0)
    rated = stat * scale
    beta = jax.nn.sigmoid(rated) * live
    rate = jnp.where(lane == 2, rate_ref[0], jnp.where(lane == 3, rate_ref[1], 0.0))
    softplus = jnp.maximum(rated, 0.0) + jnp.log1p(jnp.exp(-jnp.abs(rated)))
    keep = jnp.exp(-rate * softplus * live)
    pre_gate.wait()
    links.phase()

    def summed(i):
        return (pre[i, 0].astype(F32) + pre[i, 1].astype(F32) + pre[i, 2].astype(F32)) * scale

    given[8].wait()
    query, key, value, gate = (silu(summed(i)) for i in range(4))

    def unit(a):
        return a * lax.rsqrt(jnp.sum(a * a, axis=1, keepdims=True) + EPS)

    stacked = []
    for h in range(2):
        at = slice(h * F, (h + 1) * F)
        stacked += [unit(query[:, at]) * F ** (-0.5), unit(key[:, at])]
    turned = jnp.concatenate(stacked, axis=0).T
    for s in range(8):
        for h in range(2):
            state = state_ref[s, h]
            for t in range(NEW):
                r = s * NEW + t
                q_col = turned[:, h * 64 + r : h * 64 + r + 1]
                k_col = turned[:, h * 64 + 32 + r : h * 64 + 33 + r]
                hold = keep[r : r + 1, 2 + h : 3 + h]
                recalled = jnp.sum(k_col * state, axis=0, keepdims=True)
                update = beta[r : r + 1, h : h + 1] * (value[r : r + 1, h * F : (h + 1) * F] - hold * recalled)
                state = hold * state + k_col * update
                readings[r : r + 1, h * F : (h + 1) * F] = jnp.sum(q_col * state, axis=0, keepdims=True)
            state_ref[s, h] = state
    for h in range(2):
        at = slice(h * F, (h + 1) * F)
        read = readings[:, at] * live
        normed = read * lax.rsqrt(jnp.mean(read * read, axis=1, keepdims=True) + EPS)
        mixed_own[:, at] = (normed * head_gain_ref[...] * gate[:, at]).astype(BF)

    out_state = pltpu.make_async_copy(state_ref, next_hbm, local.at[10])
    mixed_gate = Gate(links)
    for dz in (4, 3, 5, 2, 6, 1, 7):
        links.copy(mixed_own, mz.at[z], dz=dz, gate=mixed_gate)
    out_state.start()
    mz[z] = mixed_own[...]
    own_out.wait()
    outs.wait()
    mixed_gate.wait()
    heads = jnp.concatenate([mz[k] for k in range(NZ)], axis=0)
    for k in range(NX):
        terms = jnp.dot(heads, wz[k], preferred_element_type=F32).astype(BF)
        for h in range(2):
            for b in range(NTP):
                obuf[h, b, :, k * F : (k + 1) * F] = terms[b * 32 + h * 16 : b * 32 + h * 16 + 16]
    tp_gates = [Gate(links), Gate(links)]
    for h in range(2):
        for k in (4, 3, 5, 2, 6, 1, 7):
            to = lax.rem(tp + k, NTP)
            links.copy_to(obuf.at[h, to], orecv.at[h, k], (z, x, to // NC, lax.rem(to, NC)), tp_gates[h])

    finish = []
    for h in range(2):
        attended = obuf[h, tp].astype(F32)
        links.phase()
        tp_gates[h].wait()
        for k in range(1, NTP):
            attended = attended + orecv[h, k].astype(F32)
        at = pl.ds(pl.multiple_of(tp * R + x * 32 + h * 16, 16), 16)
        given = jnp.concatenate([xbuf[k, at, :] for k in range(NX)], axis=1).astype(F32)
        hown[h] = (given + attended).astype(BF)
        hb[h, tp, pl.ds(pl.multiple_of(x * 16, 16), 16), :] = hown[h]
        finish.append(gather_straight(links, hown.at[h], hb.at[h], 16))

    stats_gates, ready2 = (Gate(links), Gate(links)), ({}, {})

    def mixer(h):
        def block(offset):
            if offset not in ready2[h]:
                ready2[h][offset] = True
                wide = hb[h, lax.rem(z + offset, NZ)].astype(F32)
                normed = (wide * gain2).astype(BF)
                p2[h, offset, :, :WIN] = jnp.dot(normed, wg[...], preferred_element_type=F32)
                p2[h, offset, :, WIN:] = jnp.dot(normed, wu[...], preferred_element_type=F32)
                stats2[h, offset] = square_rows(wide)
                if offset:
                    links.copy(stats2.at[h, offset], got2.at[h, offset], dz=offset, gate=stats_gates[h])
            return p2[h, offset]

        return RingSumWhole(links, block, s2.at[h], r2.at[h], 2 * WIN)

    sums = [mixer(h) for h in range(2)]
    gathers = [RingGather(links, abuf.at[h], 64) for h in range(2)]
    odd = lax.rem(z + c, 2)
    partner = (z, x, y, 1 - c)

    def activate(h):
        total = sums[h].total()
        scale2 = lax.rsqrt(stats_total(stats2[h, 0], got2.at[h], stats_gates[h])[:64, 0:1] / D + EPS)
        activated = silu(scale2 * total[:, :WIN]) * (scale2 * total[:, WIN:])
        again = (lax.broadcasted_iota(jnp.int32, (64, WIN), 1) < F) & (x == NX - 1)
        abuf[h, z] = jnp.where(again, 0.0, activated).astype(BF)
        gathers[h].step(0)
        down(h, 0)

    def down(h, offset):
        block = abuf[h, lax.rem(z + offset, NZ)]
        for k in range(NX):
            part[h, offset, :, k * F : (k + 1) * F] = jnp.dot(block, wd[k], preferred_element_type=F32)

    turns = (0, 6, 2, 4)
    over = {(h, base): links.fresh() for h in range(2) for base in turns}

    def give(h, base):
        at = base + 1 - odd
        psend[h, at] = part[h, at].astype(BF)
        over_made[h, base] = links.copy_to(psend.at[h, at], precv.at[h, at], partner, index=over[h, base])

    over_made = {}

    def gather_step(h, step):
        gathers[h].step(step) if step < 4 else gathers[h].finish()
        if step < 4:
            down(h, NZ - step)
            down(h, step)
        else:
            down(h, 4)
        give(h, turns[step - 1])

    last_gates = [Gate(links), Gate(links)]

    def spread(h):
        links.phase()
        for base in turns:
            at = base + odd
            over_made[h, base].wait_recv()
            both = (part[h, at] + precv[h, at].astype(F32)).astype(BF)
            to = lax.rem(z + at, NZ) // NC
            for k in range(NX):
                fsend[h, to, k] = both[:, k * F : (k + 1) * F]
        for i, (dx, dy) in enumerate(PLANE):
            links.copy(
                fsend.at[h, lax.rem(y + dy, NY), lax.rem(x + dx, NX)], frecv.at[h, i], dx=dx, dy=dy, gate=last_gates[h]
            )

    def put(h):
        result = hb[h, tp, :, feats].astype(F32) + fsend[h, y, x].astype(F32)
        last_gates[h].wait()
        for i in range(len(PLANE)):
            result = result + frecv[h, i].astype(F32)
        result = result.astype(BF)
        for k in range(NX):
            out_ref[k * 32 + h * 16 : k * 32 + h * 16 + 16, :] = result[k * 16 : (k + 1) * 16]

    finish[0]()
    for one in own_late:
        one.wait()
    late.wait()
    links.phase()
    sums[0].first()
    finish[1]()
    sums[1].first()
    sums[0].later(0)
    sums[1].later(0)
    sums[0].later(1)
    sums[1].later(1)
    sums[0].later(2)
    sums[1].later(2)
    links.phase()
    activate(0)
    activate(1)
    gather_step(0, 1)
    gather_step(1, 1)
    gather_step(0, 2)
    gather_step(1, 2)
    gather_step(0, 3)
    gather_step(1, 3)
    gather_step(0, 4)
    spread(0)
    gather_step(1, 4)
    spread(1)
    put(0)
    put(1)
    out_state.wait()
    links.drain()


def hand_over(out_tmp, state_tmp, out_ref, state_out, held_out, held_state, came, went):
    pieces = [(out_tmp, held_out, out_ref)]
    pieces += [(state_tmp.at[i], held_state.at[i], state_out.at[i]) for i in range(8)]
    coming = [pltpu.make_async_copy(a, b, came.at[i]) for i, (a, b, _) in enumerate(pieces)]
    going = [pltpu.make_async_copy(b, c, went.at[i]) for i, (_, b, c) in enumerate(pieces)]
    for one in coming:
        one.start()
    for one, two in zip(coming, going):
        one.wait()
        two.start()
    for two in going:
        two.wait()


def local(
    layer_input, seq_lengths, delta_state, attn_gain, w_query, w_key, w_value, w_outgate, w_write, w_forget,
    forget_rate, head_gain, w_out, mixer_gain, w_gate, w_up, w_down,
):
    vmem = pl.BlockSpec(memory_space=pltpu.VMEM)
    hbm = pl.BlockSpec(memory_space=pltpu.HBM)
    scratch = [
        ((NX, NTP * R, F), BF),
        ((4, F, 256), BF),
        ((NX * F, 256), BF),
        ((16, F), BF),
        ((NX, 16, F), BF),
        ((NZ, R, 256), F32),
        ((2, 4, 2, R, 128), BF),
        ((2, 4, 2, R, 128), BF),
        ((NZ, 8, R), F32),
        ((NZ, 8, R), F32),
        ((NX, 3, 32, 256), BF),
        ((3, R, 256), BF),
        ((R, R), F32),
        ((32, 256), F32),
        ((32, 256), BF),
        ((NX, 256, F), BF),
        ((NZ, 32, 256), BF),
        ((2, NTP, 16, NX * F), BF),
        ((2, NTP, 16, NX * F), BF),
        ((2, 16, NX * F), BF),
        ((2, NTP, 64, NX * F), BF),
        ((2, NZ, 8, R), F32),
        ((2, NZ, 8, R), F32),
        ((NX * F, WIN), BF),
        ((NX * F, WIN), BF),
        ((NX, WIN, F), BF),
        ((2, NZ, 64, 2 * WIN), F32),
        ((2, 2, 4, 64, 2 * WIN), BF),
        ((2, 2, 4, 64, 2 * WIN), BF),
        ((2, NZ, 64, WIN), BF),
        ((2, NZ, 64, NX * F), F32),
        ((2, NZ, 64, NX * F), BF),
        ((2, NZ, 64, NX * F), BF),
        ((2, NY, NX, 64, F), BF),
        ((2, NX * NY, 64, F), BF),
    ]
    held = [
        pltpu.VMEM((R, F), BF),
        pltpu.SMEM((8,), jnp.int32),
        pltpu.VMEM(delta_state.shape, F32),
        pltpu.VMEM((32, F), BF),
        pltpu.VMEM((2, F), BF),
        pltpu.VMEM((2, F), BF),
        pltpu.SMEM((2,), F32),
        pltpu.VMEM((1, F), F32),
        pltpu.VMEM((32, F), BF),
    ]
    out_tmp, state_tmp = pl.pallas_call(
        body,
        out_shape=(
            jax.ShapeDtypeStruct((R, F), BF),
            jax.ShapeDtypeStruct(delta_state.shape, F32),
        ),
        in_specs=[
            hbm, hbm, hbm, hbm, hbm, hbm, hbm, hbm, hbm, hbm, hbm, hbm, hbm, hbm, hbm, hbm, hbm,
        ],
        out_specs=(vmem, hbm),
        scratch_shapes=[pltpu.VMEM(shape, dtype) for shape, dtype in scratch]
        + held
        + [
            pltpu.VMEM((16384, F), BF),
            pltpu.SemaphoreType.DMA((20,)),
            pltpu.SemaphoreType.DMA((NSEND,)),
            pltpu.SemaphoreType.DMA((NRECV,)),
        ],
        compiler_params=pltpu.CompilerParams(
            collective_id=0, has_side_effects=True, vmem_limit_bytes=VMEM_LIMIT
        ),
    )(
        layer_input, seq_lengths, delta_state, attn_gain.reshape(32, F), w_query, w_key, w_value, w_outgate,
        w_write.T, w_forget.T, forget_rate, head_gain.reshape(1, F), w_out, mixer_gain.reshape(32, F), w_gate, w_up,
        w_down,
    )
    return pl.pallas_call(
        hand_over,
        out_shape=(
            jax.ShapeDtypeStruct((R, F), BF),
            jax.ShapeDtypeStruct(delta_state.shape, F32),
        ),
        in_specs=[hbm, hbm],
        out_specs=(hbm, hbm),
        scratch_shapes=[
            pltpu.VMEM((R, F), BF),
            pltpu.VMEM(delta_state.shape, F32),
            pltpu.SemaphoreType.DMA((9,)),
            pltpu.SemaphoreType.DMA((9,)),
        ],
        compiler_params=pltpu.CompilerParams(vmem_limit_bytes=VMEM_LIMIT),
    )(out_tmp, state_tmp)


def solution(mesh):
    split = Mesh(mesh.devices.reshape(NZ, NX, NY, NC), ("z", "x", "y", "c"))
    kv, tp = ("z", "x"), ("y", "c")
    in_specs = (
        P(tp, kv), P(kv), P(kv, tp, None, None), P(), P(kv, tp), P(kv, tp), P(kv, tp), P(kv, tp), P(kv, tp),
        P(kv, tp), P(tp), P(), P(tp, kv), P(), P(kv, tp), P(kv, tp), P(tp, kv),
    )
    out_specs = (P(tp, kv), P(kv, tp, None, None))
    return jax.shard_map(local, mesh=split, in_specs=in_specs, out_specs=out_specs, check_vma=False)
```

```python
import math

import jax
import jax.numpy as jnp
from jax import lax
from jax.experimental import pallas as pl
from jax.experimental.pallas import tpu as pltpu
from jax.sharding import Mesh
from jax.sharding import PartitionSpec as P

D = 4096
NEW = 4
EPS = 1e-06
NZ, NX, NY, NC = 8, 4, 4, 2
NTP = NY * NC
R = 128
F = 128
WIN = 384
MESH = pl.DeviceIdType.MESH
BF = jnp.bfloat16
F32 = jnp.float32
PLANE = [(dx, dy) for dx in range(NX) for dy in range(NY) if dx or dy]
NRECV = 109
NSEND = 11
VMEM_LIMIT = 58 * 1024 * 1024


def silu(a):
    return a * jax.nn.sigmoid(a)


def rows_of(k):
    return pl.ds(pl.multiple_of(k * R, R), R)


def dot_t(a, b):
    return lax.dot_general(a, b, (((1,), (1,)), ((), ())), preferred_element_type=F32)


class Gate:
    def __init__(self, links):
        self.links, self.index, self.size = links, links.fresh(), 0

    def wait(self):
        self.links.wait_bytes(self.links.recv.at[self.index], self.size)


class Links:
    def __init__(self, send, recv, ruler):
        self.send, self.recv, self.ruler, self.n, self.sent = send, recv, ruler, 0, []
        self.z, self.x = lax.axis_index("z"), lax.axis_index("x")
        self.y, self.c = lax.axis_index("y"), lax.axis_index("c")

    def fresh(self):
        self.n += 1
        return self.n - 1

    def phase(self):
        self.sent.append(0)

    def copy(self, src, dst, dz=0, dx=0, dy=0, dc=0, gate=None):
        to = (
            lax.rem(self.z + dz, NZ),
            lax.rem(self.x + dx, NX),
            lax.rem(self.y + dy, NY),
            lax.rem(self.c + dc, NC),
        )
        return self.copy_to(src, dst, to, gate)

    def copy_to(self, src, dst, to, gate=None, index=None):
        size = math.prod(src.shape) * jnp.dtype(src.dtype).itemsize
        self.sent[-1] += size
        if gate is not None:
            gate.size += size
            index = gate.index
        elif index is None:
            index = self.fresh()
        made = pltpu.make_async_remote_copy(
            src_ref=src,
            dst_ref=dst,
            send_sem=self.send.at[len(self.sent) - 1],
            recv_sem=self.recv.at[index],
            device_id=to,
            device_id_type=MESH,
        )
        made.start()
        return made

    def wait_bytes(self, sem, size):
        part = self.ruler.at[pl.ds(0, size // (2 * F))]
        pltpu.make_async_copy(part, part, sem).wait()

    def drain(self):
        for i, size in enumerate(self.sent):
            self.wait_bytes(self.send.at[i], size)
        assert self.n == NRECV and len(self.sent) == NSEND, (self.n, len(self.sent))


def greet(links):
    z, x, y, c = links.z, links.x, links.y, links.c
    barrier = pltpu.get_barrier_semaphore()
    to = [(dz, dx, 0, 0) for dz in (0, 1, 2, NZ - 2, NZ - 1) for dx in range(NX) if dz or dx]
    to += [(dz, 0, 0, 0) for dz in range(3, NZ - 2)]
    to += [(0, dx, dy, 0) for dx in range(NX) for dy in range(1, NY)]
    to += [(0, 0, dy, 1) for dy in range(NY)]
    for dz, dx, dy, dc in to:
        pl.semaphore_signal(
            barrier,
            inc=1,
            device_id=(lax.rem(z + dz, NZ), lax.rem(x + dx, NX), lax.rem(y + dy, NY), lax.rem(c + dc, NC)),
            device_id_type=MESH,
        )
    return lambda: pl.semaphore_wait(barrier, len(to))


def gather_x_first(links, src, buf):
    z, x, y, c = links.z, links.x, links.y, links.c
    along_x = {dx: links.copy(src, buf.at[x, rows_of(y * NC + c)], dx=dx) for dx in (1, 3, 2)}
    along_y = {}
    for dy in (1, 3, 2):
        along_y[0, dy] = links.copy(src, buf.at[x, rows_of(y * NC + c)], dy=dy)
    forward = Gate(links)
    links.copy(src, buf.at[x, rows_of(y * NC + c)], dc=1, gate=forward)

    def finish():
        def block(dx, dy):
            return buf.at[lax.rem(x - dx + NX, NX), rows_of(lax.rem(y - dy + NY, NY) * NC + c)]

        for dx in (1, 3, 2):
            along_x[dx].wait_recv()
            for dy in (1, 3, 2):
                along_y[dx, dy] = links.copy(block(dx, 0), block(dx, 0), dy=dy)
            links.copy(block(dx, 0), block(dx, 0), dc=1, gate=forward)
        for dx in (0, 1, 3, 2):
            for dy in (1, 3, 2):
                along_y[dx, dy].wait_recv()
                links.copy(block(dx, dy), block(dx, dy), dc=1, gate=forward)
        forward.wait()

    return finish


def gather_straight(links, src, buf, rows):
    x, y, c = links.x, links.y, links.c

    def block(xs, ys):
        return buf.at[ys * NC + c, pl.ds(pl.multiple_of(xs * rows, rows), rows)]

    straight = [links.copy(src, block(x, y), dx=dx, dy=dy) for dx, dy in PLANE]
    forward = Gate(links)
    links.copy(src, block(x, y), dc=1, gate=forward)

    def finish():
        for (dx, dy), made in zip(PLANE, straight):
            made.wait_recv()
            came = block(lax.rem(x - dx + NX, NX), lax.rem(y - dy + NY, NY))
            links.copy(came, came, dc=1, gate=forward)
        forward.wait()

    return finish


FAR, THREE, TWO, ONE = range(4)


class RingSumWhole:
    def __init__(self, links, block, sendbuf, recvbuf, width):
        self.links, self.block, self.sendbuf, self.recvbuf = links, block, sendbuf, recvbuf
        self.half, self.made = width // 2, {}

    def lanes(self, side):
        return slice(None) if side is None else slice(side * self.half, (side + 1) * self.half)

    def send(self, way, kind, side=None):
        lanes = self.lanes(side)
        value = self.block(4 - kind if way == 0 else 4 + kind)[:, lanes]
        if kind == THREE and side == way:
            self.made[way, FAR, side].wait_recv()
            value = value + self.recvbuf[way, FAR, :, lanes].astype(F32)
        elif kind > THREE:
            for before in ((way, THREE, 1 - way), (way, THREE, way)) if kind == TWO else ((way, TWO, None),):
                self.made[before].wait_recv()
            value = value + self.recvbuf[way, kind - 1].astype(F32)
        self.sendbuf[way, kind, :, lanes] = value.astype(BF)
        at = (way, kind) if side is None else (way, kind, slice(None), pl.ds(side * self.half, self.half))
        self.made[way, kind, side] = self.links.copy(
            self.sendbuf.at[at], self.recvbuf.at[at], dz=1 if way == 0 else NZ - 1
        )

    def first(self):
        for way in (0, 1):
            self.send(way, FAR, way)
        for way in (0, 1):
            self.send(way, THREE, 1 - way)

    def later(self, number):
        for way in (0, 1):
            self.send(way, *((THREE, way), (TWO, None), (ONE, None))[number])

    def total(self):
        value = self.block(0)
        for way in (0, 1):
            self.made[way, ONE, None].wait_recv()
            value = value + self.recvbuf[way, ONE].astype(F32)
        return value


class RingGather:
    def __init__(self, links, buf, rows):
        self.links, self.buf, self.rows, self.going = links, buf, rows // 2, {}

    def step(self, step):
        for way in (0, 1):
            if step:
                self.going[way, step].wait_recv()
            at = lax.rem(self.links.z + (NZ - step if way == 0 else step), NZ)
            if step == 2:
                half = self.buf.at[at, pl.ds(way * self.rows, self.rows)]
                self.going[way, 4] = self.links.copy(half, half, dz=2 if way == 0 else NZ - 2)
            if step < 3:
                self.going[way, step + 1] = self.links.copy(
                    self.buf.at[at], self.buf.at[at], dz=1 if way == 0 else NZ - 1
                )

    def finish(self):
        for way in (0, 1):
            self.going[way, 4].wait_recv()


def square_rows(wide):
    squares = wide * wide
    squares = squares[:, :F] + squares[:, F : 2 * F] + squares[:, 2 * F : 3 * F] + squares[:, 3 * F :]
    if wide.shape[0] < R:
        squares = jnp.concatenate([squares, jnp.zeros((R - wide.shape[0], F), F32)], axis=0)
    ones = jnp.ones((16, F), BF)
    high = squares.astype(BF)
    low = (squares - high.astype(F32)).astype(BF)
    return (dot_t(ones, high) + dot_t(ones, low))[:8]


def stats_total(own, got, gate):
    gate.wait()
    total = own
    for offset in range(1, NZ):
        total = total + got[offset]
    return jnp.concatenate([total, jnp.zeros((R - 8, R), F32)], axis=0).T


def body(
    x_hbm, len_hbm, state_hbm, gain1_hbm, wq, wk, wv, wo, write_hbm, forget_hbm, rate_hbm, head_gain_hbm, w_out,
    gain2_hbm, w_gate, w_up, w_down,
    out_ref, next_hbm,
    xbuf, w4, wr, rate_w, rw, p1, s1, r1, stats1, got1, pre, last1, cols, on_first, updates, decays, readings, mixed_own, wz, mz, obuf, orecv,
    hown, hb, stats2, got2, wg, wu, wd, p2, s2, r2, abuf, part, psend, precv, fsend, frecv,
    x_ref, len_ref, state_ref, gain1_ref, write_ref, forget_ref, rate_ref, head_gain_ref, gain2_ref,
    ruler, local, send, recv,
):
    links = Links(send, recv, ruler)
    links.phase()
    arrive = greet(links)
    z, x, y, c = links.z, links.x, links.y, links.c
    tp = y * NC + c

    locals_ = [pltpu.make_async_copy(w, w4.at[i], local.at[i]) for i, w in enumerate((wq, wk, wv, wo))]

    def window(at):
        return pl.ds(pl.multiple_of((at * 3 - at // (NX - 1)) * F, F), WIN)

    feats = pl.ds(pl.multiple_of(x * F, F), F)
    given = [
        pltpu.make_async_copy(far, near, local.at[11 + i])
        for i, (far, near) in enumerate(
            (
                (x_hbm, x_ref), (write_hbm, write_ref), (forget_hbm, forget_ref), (gain1_hbm, gain1_ref),
                (gain2_hbm, gain2_ref), (len_hbm, len_ref), (rate_hbm, rate_ref), (head_gain_hbm, head_gain_ref),
                (state_hbm, state_ref),
            )
        )
    ]
    for one in given:
        one.start()
    own_x = pltpu.make_async_copy(x_hbm, xbuf.at[x, rows_of(tp)], local.at[4])
    own_out = pltpu.make_async_copy(w_out, wz.at[x], local.at[5])
    own_late = [
        pltpu.make_async_copy(w_gate.at[:, window(x)], wg.at[feats], local.at[6]),
        pltpu.make_async_copy(w_up.at[:, window(x)], wu.at[feats], local.at[7]),
        pltpu.make_async_copy(w_down.at[window(x)], wd.at[x], local.at[8]),
    ]
    for one in locals_ + [own_x, own_out] + own_late:
        one.start()
    for one in given[:8]:
        one.wait()
    small = [write_ref[...].astype(F32), forget_ref[...].astype(F32), jnp.zeros((12, F), F32)]
    rate_w[...] = jnp.concatenate(small, axis=0).astype(BF)
    rw[x] = rate_w[...]
    arrive()

    finish = gather_x_first(links, x_ref, xbuf)
    for one in locals_:
        one.wait()
    own_w = pltpu.make_async_copy(w4.at[x], wr.at[feats], local.at[9])
    own_w.start()
    early, early_rates, late, outs = Gate(links), Gate(links), Gate(links), Gate(links)
    for dx in (1, 3, 2):
        to = lax.rem(x + dx, NX)
        links.copy(w4.at[to], wr.at[feats], dx=dx, gate=early)
        links.copy(rate_w, rw.at[x], dx=dx, gate=early_rates)
    links.phase()
    for dx in (1, 3, 2):
        links.copy(w_out, wz.at[x], dx=dx, gate=outs)
    for dx in (1, 3, 2):
        to = lax.rem(x + dx, NX)
        links.copy(w_gate.at[:, window(to)], wg.at[feats], dx=dx, gate=late)
        links.copy(w_up.at[:, window(to)], wu.at[feats], dx=dx, gate=late)
    links.phase()

    which = lax.broadcasted_iota(jnp.int32, (32, F), 0)

    def gain_of(ref):
        wide = ref[...].astype(F32)
        return jnp.concatenate(
            [jnp.sum(jnp.where(which == z * NX + k, wide, 0.0), axis=0, keepdims=True) for k in range(NX)], axis=1
        )

    gain1, gain2 = gain_of(gain1_ref), gain_of(gain2_ref)
    own_x.wait()
    own_w.wait()
    finish()
    early.wait()
    early_rates.wait()
    links.phase()

    sub = lax.broadcasted_iota(jnp.int32, (8, R), 0)
    stats_gate, ready = Gate(links), {}

    def projected(offset):
        if offset not in ready:
            ready[offset] = True
            at = rows_of(lax.rem(z + offset, NZ))
            wide = jnp.concatenate([xbuf[k, at, :] for k in range(NX)], axis=1).astype(F32)
            normed = (wide * gain1).astype(BF)
            p1[offset] = jnp.dot(normed, wr[...], preferred_element_type=F32)
            stat = jnp.where(sub == 4, square_rows(wide), 0.0)
            for k in range(NX):
                stat = stat + dot_t(rw[k], normed[:, k * F : (k + 1) * F])[:8]
            stats1[offset] = stat
            if offset:
                links.copy(stats1.at[offset], got1.at[offset], dz=offset, gate=stats_gate)
        return p1[offset]

    def part_of(at):
        return pl.ds(pl.multiple_of(at * 32, 32), 32)

    near = {}
    for way in (0, 1):
        side = pl.ds(way * F, F)
        s1[way, 0, :, way * F : (way + 1) * F] = projected(4)[:, way * F : (way + 1) * F].astype(BF)
        near[way, 0] = links.copy(s1.at[way, 0, :, side], r1.at[way, 0, :, side], dz=2 if way == 0 else NZ - 2)
    for way in (0, 1):
        s1[way, 1] = projected(3 if way == 0 else 5).astype(BF)
        near[way, 1] = links.copy(s1.at[way, 1], r1.at[way, 1], dz=1 if way == 0 else NZ - 1)
    pre_gate = Gate(links)

    def to_owners(slot, value, dz):
        last1[slot] = value.astype(BF)
        for dx in (2, 1, 3, 0):
            if dx or dz:
                links.copy(last1.at[slot, part_of(lax.rem(x + dx, NX))], pre.at[x, slot], dz=dz, dx=dx, gate=pre_gate)

    to_owners(1, projected(1), 1)
    to_owners(2, projected(7), NZ - 1)
    to_owners(0, projected(0), 0)
    for way in (0, 1):
        value = projected(2 if way == 0 else 6)
        near[way, 0].wait_recv()
        near[way, 1].wait_recv()
        half = value[:, way * F : (way + 1) * F] + r1[way, 0, :, way * F : (way + 1) * F].astype(F32)
        halves = [half, value[:, F:]] if way == 0 else [value[:, :F], half]
        to_owners(3 + way, jnp.concatenate(halves, axis=1) + r1[way, 1].astype(F32), 2 if way == 0 else NZ - 2)
    quarter = part_of(x)
    pre[x, 0] = last1[0, quarter, :]
    cols[...] = stats_total(stats1[0], got1, stats_gate)
    stat = cols[quarter, :]
    scale = lax.rsqrt(stat[:, 4:5] / D + EPS)
    lane = lax.broadcasted_iota(jnp.int32, (32, R), 1)
    row = lax.broadcasted_iota(jnp.int32, (32, R), 0)
    live = jnp.zeros((32, R), F32)
    for s in range(8):
        inside = (row // NEW == s) & (lax.rem(row, NEW) < len_ref[s])
        live = live + jnp.where(inside, 1.0, 0.0)
    rated = stat * scale
    beta = jax.nn.sigmoid(rated) * live
    rate = jnp.where(lane == 2, rate_ref[0], jnp.where(lane == 3, rate_ref[1], 0.0))
    softplus = jnp.maximum(rated, 0.0) + jnp.log1p(jnp.exp(-jnp.abs(rated)))
    keep = jnp.exp(-rate * softplus * live)
    pre_gate.wait()
    links.phase()

    def summed(i):
        return sum(pre[i, k].astype(F32) for k in range(5)) * scale

    given[8].wait()
    for dx in (1, 3, 2):
        to = lax.rem(x + dx, NX)
        links.copy(w_down.at[window(to)], wd.at[x], dx=dx, gate=late)
    query, key, value, gate = (silu(summed(i)) for i in range(4))

    def unit(a):
        return a * lax.rsqrt(jnp.sum(a * a, axis=1, keepdims=True) + EPS)

    stacked = []
    for h in range(2):
        at = slice(h * F, (h + 1) * F)
        stacked += [unit(query[:, at]) * F ** (-0.5), unit(key[:, at])]
    upper = lax.broadcasted_iota(jnp.int32, (8, F), 0) < NEW
    for pair in range(4):
        near8 = slice(pair * 8, pair * 8 + 8)
        for h in range(2):
            both = jnp.concatenate([stacked[2 * h][near8], stacked[2 * h + 1][near8]], axis=0)
            one, two = (
                jnp.dot(both, state_ref[2 * pair + i, h], precision=lax.Precision.HIGHEST, preferred_element_type=F32)
                for i in range(2)
            )
            for k in range(2):
                half = slice(k * 8, k * 8 + 8)
                on_first[k, near8, h * F : (h + 1) * F] = jnp.where(upper, one[half], two[half])
    position = lax.rem(row, NEW)

    def later_by(a, n):
        return jnp.concatenate([a[32 - n :], a[: 32 - n]], axis=0)

    def sooner_by(a, n):
        return jnp.concatenate([a[n:], a[:n]], axis=0)

    for h in range(2):
        at = slice(h * F, (h + 1) * F)
        q_now, k_now, v_now = stacked[2 * h], stacked[2 * h + 1], value[:, at]
        write = jnp.broadcast_to(beta[:, h : h + 1], (32, F))
        hold = jnp.broadcast_to(keep[:, 2 + h : 3 + h], (32, F))
        over1 = hold
        over2 = over1 * later_by(hold, 1)
        over3 = over2 * later_by(hold, 2)
        over4 = over3 * later_by(hold, 3)
        whole = jnp.where(position == 0, over1, jnp.where(position == 1, over2, jnp.where(position == 2, over3, over4)))
        alone = write * (v_now - whole * on_first[1, :, at])
        among_k, among_q = [], [jnp.sum(q_now * k_now, axis=1, keepdims=True)]
        for n, over_n in ((1, over1), (2, over2), (3, over3)):
            k_then = later_by(k_now, n)
            inside = jnp.where(position >= n, over_n, 0.0)
            among_k.append(write * inside * jnp.sum(k_now * k_then, axis=1, keepdims=True))
            among_q.append(inside * jnp.sum(q_now * k_then, axis=1, keepdims=True))
        update = alone
        for _ in range(NEW - 1):
            update = alone - sum(among_k[n - 1] * later_by(update, n) for n in (1, 2, 3))
        reading = whole * on_first[0, :, at] + among_q[0] * update
        for n in (1, 2, 3):
            reading = reading + among_q[n] * later_by(update, n)
        readings[:, at] = reading
        ahead1 = sooner_by(hold, 1)
        ahead2 = ahead1 * sooner_by(hold, 2)
        ahead3 = ahead2 * sooner_by(hold, 3)
        rest = jnp.where(position == 3, 1.0, jnp.where(position == 2, ahead1, jnp.where(position == 1, ahead2, ahead3)))
        updates[:, at] = rest * update
        decays[:, at] = whole
    for h in range(2):
        at = slice(h * F, (h + 1) * F)
        read = readings[:, at] * live
        normed = read * lax.rsqrt(jnp.mean(read * read, axis=1, keepdims=True) + EPS)
        mixed_own[:, at] = (normed * head_gain_ref[...] * gate[:, at]).astype(BF)

    mixed_gate = Gate(links)
    for dz in (4, 3, 5, 2, 6, 1, 7):
        links.copy(mixed_own, mz.at[z], dz=dz, gate=mixed_gate)
    mz[z] = mixed_own[...]
    turned = jnp.concatenate(stacked, axis=0).T
    for s in range(8):
        for h in range(2):
            at = slice(h * F, (h + 1) * F)
            state = decays[s * NEW + NEW - 1 : (s + 1) * NEW, at] * state_ref[s, h]
            for r in range(s * NEW, (s + 1) * NEW):
                state = state + turned[:, h * 64 + 32 + r : h * 64 + 33 + r] * updates[r : r + 1, at]
            state_ref[s, h] = state
    out_state = pltpu.make_async_copy(state_ref, next_hbm, local.at[10])
    out_state.start()
    own_out.wait()
    outs.wait()
    mixed_gate.wait()
    heads = jnp.concatenate([mz[k] for k in range(NZ)], axis=0)
    for k in range(NX):
        terms = jnp.dot(heads, wz[k], preferred_element_type=F32).astype(BF)
        for h in range(2):
            for b in range(NTP):
                obuf[h, b, :, k * F : (k + 1) * F] = terms[b * 32 + h * 16 : b * 32 + h * 16 + 16]
    tp_gates = [Gate(links), Gate(links)]
    for h in range(2):
        for k in (4, 3, 5, 2, 6, 1, 7):
            to = lax.rem(tp + k, NTP)
            links.copy_to(obuf.at[h, to], orecv.at[h, k], (z, x, to // NC, lax.rem(to, NC)), tp_gates[h])

    finish = []
    for h in range(2):
        attended = obuf[h, tp].astype(F32)
        links.phase()
        tp_gates[h].wait()
        for k in range(1, NTP):
            attended = attended + orecv[h, k].astype(F32)
        at = pl.ds(pl.multiple_of(tp * R + x * 32 + h * 16, 16), 16)
        given = jnp.concatenate([xbuf[k, at, :] for k in range(NX)], axis=1).astype(F32)
        hown[h] = (given + attended).astype(BF)
        hb[h, tp, pl.ds(pl.multiple_of(x * 16, 16), 16), :] = hown[h]
        finish.append(gather_straight(links, hown.at[h], hb.at[h], 16))

    stats_gates, ready2 = (Gate(links), Gate(links)), ({}, {})

    def mixer(h):
        def block(offset):
            if offset not in ready2[h]:
                ready2[h][offset] = True
                wide = hb[h, lax.rem(z + offset, NZ)].astype(F32)
                normed = (wide * gain2).astype(BF)
                p2[h, offset, :, :WIN] = jnp.dot(normed, wg[...], preferred_element_type=F32)
                p2[h, offset, :, WIN:] = jnp.dot(normed, wu[...], preferred_element_type=F32)
                stats2[h, offset] = square_rows(wide)
                if offset:
                    links.copy(stats2.at[h, offset], got2.at[h, offset], dz=offset, gate=stats_gates[h])
            return p2[h, offset]

        return RingSumWhole(links, block, s2.at[h], r2.at[h], 2 * WIN)

    sums = [mixer(h) for h in range(2)]
    gathers = [RingGather(links, abuf.at[h], 64) for h in range(2)]
    odd = lax.rem(z + c, 2)
    partner = (z, x, y, 1 - c)

    def activate(h):
        total = sums[h].total()
        scale2 = lax.rsqrt(stats_total(stats2[h, 0], got2.at[h], stats_gates[h])[:64, 0:1] / D + EPS)
        activated = silu(scale2 * total[:, :WIN]) * (scale2 * total[:, WIN:])
        again = (lax.broadcasted_iota(jnp.int32, (64, WIN), 1) < F) & (x == NX - 1)
        abuf[h, z] = jnp.where(again, 0.0, activated).astype(BF)
        gathers[h].step(0)
        down(h, 0)

    def down(h, offset):
        block = abuf[h, lax.rem(z + offset, NZ)]
        for k in range(NX):
            part[h, offset, :, k * F : (k + 1) * F] = jnp.dot(block, wd[k], preferred_element_type=F32)

    turns = (0, 6, 2, 4)
    over = {(h, base): links.fresh() for h in range(2) for base in turns}

    def give(h, base):
        at = base + 1 - odd
        psend[h, at] = part[h, at].astype(BF)
        over_made[h, base] = links.copy_to(psend.at[h, at], precv.at[h, at], partner, index=over[h, base])

    over_made = {}

    def gather_step(h, step):
        gathers[h].step(step) if step < 4 else gathers[h].finish()
        if step < 4:
            down(h, NZ - step)
            down(h, step)
        else:
            down(h, 4)
        give(h, turns[step - 1])

    last_gates = [Gate(links), Gate(links)]

    def spread(h):
        links.phase()
        for base in turns:
            at = base + odd
            over_made[h, base].wait_recv()
            both = (part[h, at] + precv[h, at].astype(F32)).astype(BF)
            to = lax.rem(z + at, NZ) // NC
            for k in range(NX):
                fsend[h, to, k] = both[:, k * F : (k + 1) * F]
        for i, (dx, dy) in enumerate(PLANE):
            links.copy(
                fsend.at[h, lax.rem(y + dy, NY), lax.rem(x + dx, NX)], frecv.at[h, i], dx=dx, dy=dy, gate=last_gates[h]
            )

    def put(h):
        result = hb[h, tp, :, feats].astype(F32) + fsend[h, y, x].astype(F32)
        last_gates[h].wait()
        for i in range(len(PLANE)):
            result = result + frecv[h, i].astype(F32)
        result = result.astype(BF)
        for k in range(NX):
            out_ref[k * 32 + h * 16 : k * 32 + h * 16 + 16, :] = result[k * 16 : (k + 1) * 16]

    finish[0]()
    for one in own_late:
        one.wait()
    late.wait()
    links.phase()
    sums[0].first()
    finish[1]()
    sums[1].first()
    sums[0].later(0)
    sums[1].later(0)
    sums[0].later(1)
    sums[1].later(1)
    sums[0].later(2)
    sums[1].later(2)
    links.phase()
    activate(0)
    activate(1)
    gather_step(0, 1)
    gather_step(1, 1)
    gather_step(0, 2)
    gather_step(1, 2)
    gather_step(0, 3)
    gather_step(1, 3)
    gather_step(0, 4)
    spread(0)
    gather_step(1, 4)
    spread(1)
    put(0)
    put(1)
    out_state.wait()
    links.drain()


def hand_over(out_tmp, state_tmp, out_ref, state_out, held_out, held_state, came, went):
    pieces = [(out_tmp, held_out, out_ref)]
    pieces += [(state_tmp.at[i], held_state.at[i], state_out.at[i]) for i in range(8)]
    coming = [pltpu.make_async_copy(a, b, came.at[i]) for i, (a, b, _) in enumerate(pieces)]
    going = [pltpu.make_async_copy(b, c, went.at[i]) for i, (_, b, c) in enumerate(pieces)]
    for one in coming:
        one.start()
    for one, two in zip(coming, going):
        one.wait()
        two.start()
    for two in going:
        two.wait()


def local(
    layer_input, seq_lengths, delta_state, attn_gain, w_query, w_key, w_value, w_outgate, w_write, w_forget,
    forget_rate, head_gain, w_out, mixer_gain, w_gate, w_up, w_down,
):
    vmem = pl.BlockSpec(memory_space=pltpu.VMEM)
    hbm = pl.BlockSpec(memory_space=pltpu.HBM)
    scratch = [
        ((NX, NTP * R, F), BF),
        ((4, F, 256), BF),
        ((NX * F, 256), BF),
        ((16, F), BF),
        ((NX, 16, F), BF),
        ((NZ, R, 256), F32),
        ((2, 2, R, 256), BF),
        ((2, 2, R, 256), BF),
        ((NZ, 8, R), F32),
        ((NZ, 8, R), F32),
        ((NX, 5, 32, 256), BF),
        ((5, R, 256), BF),
        ((R, R), F32),
        ((2, 32, 256), F32),
        ((32, 256), F32),
        ((32, 256), F32),
        ((32, 256), F32),
        ((32, 256), BF),
        ((NX, 256, F), BF),
        ((NZ, 32, 256), BF),
        ((2, NTP, 16, NX * F), BF),
        ((2, NTP, 16, NX * F), BF),
        ((2, 16, NX * F), BF),
        ((2, NTP, 64, NX * F), BF),
        ((2, NZ, 8, R), F32),
        ((2, NZ, 8, R), F32),
        ((NX * F, WIN), BF),
        ((NX * F, WIN), BF),
        ((NX, WIN, F), BF),
        ((2, NZ, 64, 2 * WIN), F32),
        ((2, 2, 4, 64, 2 * WIN), BF),
        ((2, 2, 4, 64, 2 * WIN), BF),
        ((2, NZ, 64, WIN), BF),
        ((2, NZ, 64, NX * F), F32),
        ((2, NZ, 64, NX * F), BF),
        ((2, NZ, 64, NX * F), BF),
        ((2, NY, NX, 64, F), BF),
        ((2, NX * NY, 64, F), BF),
    ]
    held = [
        pltpu.VMEM((R, F), BF),
        pltpu.SMEM((8,), jnp.int32),
        pltpu.VMEM(delta_state.shape, F32),
        pltpu.VMEM((32, F), BF),
        pltpu.VMEM((2, F), BF),
        pltpu.VMEM((2, F), BF),
        pltpu.SMEM((2,), F32),
        pltpu.VMEM((1, F), F32),
        pltpu.VMEM((32, F), BF),
    ]
    out_tmp, state_tmp = pl.pallas_call(
        body,
        out_shape=(
            jax.ShapeDtypeStruct((R, F), BF),
            jax.ShapeDtypeStruct(delta_state.shape, F32),
        ),
        in_specs=[
            hbm, hbm, hbm, hbm, hbm, hbm, hbm, hbm, hbm, hbm, hbm, hbm, hbm, hbm, hbm, hbm, hbm,
        ],
        out_specs=(vmem, hbm),
        scratch_shapes=[pltpu.VMEM(shape, dtype) for shape, dtype in scratch]
        + held
        + [
            pltpu.VMEM((16384, F), BF),
            pltpu.SemaphoreType.DMA((20,)),
            pltpu.SemaphoreType.DMA((NSEND,)),
            pltpu.SemaphoreType.DMA((NRECV,)),
        ],
        compiler_params=pltpu.CompilerParams(
            collective_id=0, has_side_effects=True, vmem_limit_bytes=VMEM_LIMIT
        ),
    )(
        layer_input, seq_lengths, delta_state, attn_gain.reshape(32, F), w_query, w_key, w_value, w_outgate,
        w_write.T, w_forget.T, forget_rate, head_gain.reshape(1, F), w_out, mixer_gain.reshape(32, F), w_gate, w_up,
        w_down,
    )
    return pl.pallas_call(
        hand_over,
        out_shape=(
            jax.ShapeDtypeStruct((R, F), BF),
            jax.ShapeDtypeStruct(delta_state.shape, F32),
        ),
        in_specs=[hbm, hbm],
        out_specs=(hbm, hbm),
        scratch_shapes=[
            pltpu.VMEM((R, F), BF),
            pltpu.VMEM(delta_state.shape, F32),
            pltpu.SemaphoreType.DMA((9,)),
            pltpu.SemaphoreType.DMA((9,)),
        ],
        compiler_params=pltpu.CompilerParams(vmem_limit_bytes=VMEM_LIMIT),
    )(out_tmp, state_tmp)


def solution(mesh):
    split = Mesh(mesh.devices.reshape(NZ, NX, NY, NC), ("z", "x", "y", "c"))
    kv, tp = ("z", "x"), ("y", "c")
    in_specs = (
        P(tp, kv), P(kv), P(kv, tp, None, None), P(), P(kv, tp), P(kv, tp), P(kv, tp), P(kv, tp), P(kv, tp),
        P(kv, tp), P(tp), P(), P(tp, kv), P(), P(kv, tp), P(kv, tp), P(tp, kv),
    )
    out_specs = (P(tp, kv), P(kv, tp, None, None))
    return jax.shard_map(local, mesh=split, in_specs=in_specs, out_specs=out_specs, check_vma=False)
```

```python
import math

import jax
import jax.numpy as jnp
from jax import lax
from jax.experimental import pallas as pl
from jax.experimental.pallas import tpu as pltpu
from jax.sharding import Mesh
from jax.sharding import PartitionSpec as P

D = 4096
NEW = 4
EPS = 1e-06
NZ, NX, NY, NC = 8, 4, 4, 2
NTP = NY * NC
R = 128
F = 128
WIN = 384
MESH = pl.DeviceIdType.MESH
BF = jnp.bfloat16
F32 = jnp.float32
PLANE = [(dx, dy) for dx in range(NX) for dy in range(NY) if dx or dy]
NRECV = 109
NSEND = 10
VMEM_LIMIT = 58 * 1024 * 1024


def silu(a):
    return a * jax.nn.sigmoid(a)


def rows_of(k):
    return pl.ds(pl.multiple_of(k * R, R), R)


def dot_t(a, b):
    return lax.dot_general(a, b, (((1,), (1,)), ((), ())), preferred_element_type=F32)


class Gate:
    def __init__(self, links):
        self.links, self.index, self.size = links, links.fresh(), 0

    def wait(self):
        self.links.wait_bytes(self.links.recv.at[self.index], self.size)


class Links:
    def __init__(self, send, recv, ruler):
        self.send, self.recv, self.ruler, self.n, self.sent = send, recv, ruler, 0, []
        self.z, self.x = lax.axis_index("z"), lax.axis_index("x")
        self.y, self.c = lax.axis_index("y"), lax.axis_index("c")

    def fresh(self):
        self.n += 1
        return self.n - 1

    def phase(self):
        self.sent.append(0)

    def copy(self, src, dst, dz=0, dx=0, dy=0, dc=0, gate=None):
        to = (
            lax.rem(self.z + dz, NZ),
            lax.rem(self.x + dx, NX),
            lax.rem(self.y + dy, NY),
            lax.rem(self.c + dc, NC),
        )
        return self.copy_to(src, dst, to, gate)

    def copy_to(self, src, dst, to, gate=None, index=None):
        size = math.prod(src.shape) * jnp.dtype(src.dtype).itemsize
        self.sent[-1] += size
        if gate is not None:
            gate.size += size
            index = gate.index
        elif index is None:
            index = self.fresh()
        made = pltpu.make_async_remote_copy(
            src_ref=src,
            dst_ref=dst,
            send_sem=self.send.at[len(self.sent) - 1],
            recv_sem=self.recv.at[index],
            device_id=to,
            device_id_type=MESH,
        )
        made.start()
        return made

    def wait_bytes(self, sem, size):
        part = self.ruler.at[pl.ds(0, size // (2 * F))]
        pltpu.make_async_copy(part, part, sem).wait()

    def drain(self):
        for i, size in enumerate(self.sent):
            self.wait_bytes(self.send.at[i], size)
        assert self.n == NRECV and len(self.sent) == NSEND, (self.n, len(self.sent))


def greet(links):
    z, x, y, c = links.z, links.x, links.y, links.c
    barrier = pltpu.get_barrier_semaphore()
    to = [(dz, dx, 0, 0) for dz in (0, 1, 2, NZ - 2, NZ - 1) for dx in range(NX) if dz or dx]
    to += [(dz, 0, 0, 0) for dz in range(3, NZ - 2)]
    to += [(0, dx, dy, 0) for dx in range(NX) for dy in range(1, NY)]
    to += [(0, 0, dy, 1) for dy in range(NY)]
    for dz, dx, dy, dc in to:
        pl.semaphore_signal(
            barrier,
            inc=1,
            device_id=(lax.rem(z + dz, NZ), lax.rem(x + dx, NX), lax.rem(y + dy, NY), lax.rem(c + dc, NC)),
            device_id_type=MESH,
        )
    return lambda: pl.semaphore_wait(barrier, len(to))


def gather_x_first(links, src, buf):
    z, x, y, c = links.z, links.x, links.y, links.c
    along_x = {dx: links.copy(src, buf.at[x, rows_of(y * NC + c)], dx=dx) for dx in (1, 3, 2)}
    along_y = {}
    for dy in (1, 3, 2):
        along_y[0, dy] = links.copy(src, buf.at[x, rows_of(y * NC + c)], dy=dy)
    forward = Gate(links)
    links.copy(src, buf.at[x, rows_of(y * NC + c)], dc=1, gate=forward)

    def finish():
        def block(dx, dy):
            return buf.at[lax.rem(x - dx + NX, NX), rows_of(lax.rem(y - dy + NY, NY) * NC + c)]

        for dx in (1, 3, 2):
            along_x[dx].wait_recv()
            for dy in (1, 3, 2):
                along_y[dx, dy] = links.copy(block(dx, 0), block(dx, 0), dy=dy)
            links.copy(block(dx, 0), block(dx, 0), dc=1, gate=forward)
        for dx in (0, 1, 3, 2):
            for dy in (1, 3, 2):
                along_y[dx, dy].wait_recv()
                links.copy(block(dx, dy), block(dx, dy), dc=1, gate=forward)
        forward.wait()

    return finish


def gather_straight(links, src, buf, rows):
    x, y, c = links.x, links.y, links.c

    def block(xs, ys):
        return buf.at[ys * NC + c, pl.ds(pl.multiple_of(xs * rows, rows), rows)]

    straight = [links.copy(src, block(x, y), dx=dx, dy=dy) for dx, dy in PLANE]
    forward = Gate(links)
    links.copy(src, block(x, y), dc=1, gate=forward)

    def finish():
        for (dx, dy), made in zip(PLANE, straight):
            made.wait_recv()
            came = block(lax.rem(x - dx + NX, NX), lax.rem(y - dy + NY, NY))
            links.copy(came, came, dc=1, gate=forward)
        forward.wait()

    return finish


FAR, THREE, TWO, ONE = range(4)


class RingSumWhole:
    def __init__(self, links, block, sendbuf, recvbuf, width):
        self.links, self.block, self.sendbuf, self.recvbuf = links, block, sendbuf, recvbuf
        self.half, self.made = width // 2, {}

    def lanes(self, side):
        return slice(None) if side is None else slice(side * self.half, (side + 1) * self.half)

    def send(self, way, kind, side=None):
        lanes = self.lanes(side)
        value = self.block(4 - kind if way == 0 else 4 + kind)[:, lanes]
        if kind == THREE and side == way:
            self.made[way, FAR, side].wait_recv()
            value = value + self.recvbuf[way, FAR, :, lanes].astype(F32)
        elif kind > THREE:
            for before in ((way, THREE, 1 - way), (way, THREE, way)) if kind == TWO else ((way, TWO, None),):
                self.made[before].wait_recv()
            value = value + self.recvbuf[way, kind - 1].astype(F32)
        self.sendbuf[way, kind, :, lanes] = value.astype(BF)
        at = (way, kind) if side is None else (way, kind, slice(None), pl.ds(side * self.half, self.half))
        self.made[way, kind, side] = self.links.copy(
            self.sendbuf.at[at], self.recvbuf.at[at], dz=1 if way == 0 else NZ - 1
        )

    def first(self):
        for way in (0, 1):
            self.send(way, FAR, way)
        for way in (0, 1):
            self.send(way, THREE, 1 - way)

    def later(self, number):
        for way in (0, 1):
            self.send(way, *((THREE, way), (TWO, None), (ONE, None))[number])

    def total(self):
        value = self.block(0)
        for way in (0, 1):
            self.made[way, ONE, None].wait_recv()
            value = value + self.recvbuf[way, ONE].astype(F32)
        return value


class RingGather:
    def __init__(self, links, buf, rows):
        self.links, self.buf, self.rows, self.going = links, buf, rows // 2, {}

    def step(self, step):
        for way in (0, 1):
            if step:
                self.going[way, step].wait_recv()
            at = lax.rem(self.links.z + (NZ - step if way == 0 else step), NZ)
            if step == 2:
                half = self.buf.at[at, pl.ds(way * self.rows, self.rows)]
                self.going[way, 4] = self.links.copy(half, half, dz=2 if way == 0 else NZ - 2)
            if step < 3:
                self.going[way, step + 1] = self.links.copy(
                    self.buf.at[at], self.buf.at[at], dz=1 if way == 0 else NZ - 1
                )

    def finish(self):
        for way in (0, 1):
            self.going[way, 4].wait_recv()


def square_rows(wide):
    squares = wide * wide
    squares = squares[:, :F] + squares[:, F : 2 * F] + squares[:, 2 * F : 3 * F] + squares[:, 3 * F :]
    if wide.shape[0] < R:
        squares = jnp.concatenate([squares, jnp.zeros((R - wide.shape[0], F), F32)], axis=0)
    ones = jnp.ones((16, F), BF)
    high = squares.astype(BF)
    low = (squares - high.astype(F32)).astype(BF)
    return (dot_t(ones, high) + dot_t(ones, low))[:8]


def stats_total(own, got, gate):
    gate.wait()
    total = own
    for offset in range(1, NZ):
        total = total + got[offset]
    return jnp.concatenate([total, jnp.zeros((R - 8, R), F32)], axis=0).T


def body(
    x_hbm, len_hbm, state_hbm, gain1_hbm, wq, wk, wv, wo, write_hbm, forget_hbm, rate_hbm, head_gain_hbm, w_out,
    gain2_hbm, w_gate, w_up, w_down,
    out_ref, next_hbm,
    xbuf, w4, wr, rate_w, rw, p1, s1, r1, stats1, got1, pre, last1, cols, on_first, updates, decays, readings, mixed_own, wz, mz, obuf, orecv,
    hown, hb, stats2, got2, wg, wu, wd, p2, s2, r2, abuf, part, psend, precv, fsend, frecv,
    x_ref, len_ref, state_ref, gain1_ref, write_ref, forget_ref, rate_ref, head_gain_ref, gain2_ref,
    ruler, local, send, recv,
):
    links = Links(send, recv, ruler)
    links.phase()
    arrive = greet(links)
    z, x, y, c = links.z, links.x, links.y, links.c
    tp = y * NC + c

    locals_ = [pltpu.make_async_copy(w, w4.at[i], local.at[i]) for i, w in enumerate((wq, wk, wv, wo))]

    def window(at):
        return pl.ds(pl.multiple_of((at * 3 - at // (NX - 1)) * F, F), WIN)

    feats = pl.ds(pl.multiple_of(x * F, F), F)
    given = [
        pltpu.make_async_copy(far, near, local.at[11 + i])
        for i, (far, near) in enumerate(
            (
                (x_hbm, x_ref), (write_hbm, write_ref), (forget_hbm, forget_ref), (gain1_hbm, gain1_ref),
                (gain2_hbm, gain2_ref), (len_hbm, len_ref), (rate_hbm, rate_ref), (head_gain_hbm, head_gain_ref),
                (state_hbm, state_ref),
            )
        )
    ]
    for one in given:
        one.start()
    own_x = pltpu.make_async_copy(x_hbm, xbuf.at[x, rows_of(tp)], local.at[4])
    own_out = pltpu.make_async_copy(w_out, wz.at[x], local.at[5])
    own_late = [
        pltpu.make_async_copy(w_gate.at[:, window(x)], wg.at[feats], local.at[6]),
        pltpu.make_async_copy(w_up.at[:, window(x)], wu.at[feats], local.at[7]),
        pltpu.make_async_copy(w_down.at[window(x)], wd.at[x], local.at[8]),
    ]
    for one in locals_ + [own_x, own_out] + own_late:
        one.start()
    for one in given[:8]:
        one.wait()
    small = [write_ref[...].astype(F32), forget_ref[...].astype(F32), jnp.zeros((12, F), F32)]
    rate_w[...] = jnp.concatenate(small, axis=0).astype(BF)
    rw[x] = rate_w[...]
    arrive()

    finish = gather_x_first(links, x_ref, xbuf)
    for one in locals_:
        one.wait()
    own_w = pltpu.make_async_copy(w4.at[x], wr.at[feats], local.at[9])
    own_w.start()
    early, early_rates, late, outs = Gate(links), Gate(links), Gate(links), Gate(links)
    for dx in (1, 3, 2):
        to = lax.rem(x + dx, NX)
        links.copy(w4.at[to], wr.at[feats], dx=dx, gate=early)
        links.copy(rate_w, rw.at[x], dx=dx, gate=early_rates)
    links.phase()
    for dx in (1, 3, 2):
        links.copy(w_out, wz.at[x], dx=dx, gate=outs)
    for dx in (1, 3, 2):
        to = lax.rem(x + dx, NX)
        links.copy(w_gate.at[:, window(to)], wg.at[feats], dx=dx, gate=late)
        links.copy(w_up.at[:, window(to)], wu.at[feats], dx=dx, gate=late)
    links.phase()

    which = lax.broadcasted_iota(jnp.int32, (32, F), 0)

    def gain_of(ref):
        wide = ref[...].astype(F32)
        return jnp.concatenate(
            [jnp.sum(jnp.where(which == z * NX + k, wide, 0.0), axis=0, keepdims=True) for k in range(NX)], axis=1
        )

    gain1, gain2 = gain_of(gain1_ref), gain_of(gain2_ref)
    own_x.wait()
    own_w.wait()
    finish()
    early.wait()
    early_rates.wait()
    links.phase()

    sub = lax.broadcasted_iota(jnp.int32, (8, R), 0)
    stats_gate, ready = Gate(links), {}

    def projected(offset):
        if offset not in ready:
            ready[offset] = True
            at = rows_of(lax.rem(z + offset, NZ))
            wide = jnp.concatenate([xbuf[k, at, :] for k in range(NX)], axis=1).astype(F32)
            normed = (wide * gain1).astype(BF)
            p1[offset] = jnp.dot(normed, wr[...], preferred_element_type=F32)
            stat = jnp.where(sub == 4, square_rows(wide), 0.0)
            for k in range(NX):
                stat = stat + dot_t(rw[k], normed[:, k * F : (k + 1) * F])[:8]
            stats1[offset] = stat
            if offset:
                links.copy(stats1.at[offset], got1.at[offset], dz=offset, gate=stats_gate)
        return p1[offset]

    def part_of(at):
        return pl.ds(pl.multiple_of(at * 32, 32), 32)

    near = {}
    for way in (0, 1):
        side = pl.ds(way * F, F)
        s1[way, 0, :, way * F : (way + 1) * F] = projected(4)[:, way * F : (way + 1) * F].astype(BF)
        near[way, 0] = links.copy(s1.at[way, 0, :, side], r1.at[way, 0, :, side], dz=2 if way == 0 else NZ - 2)
    for way in (0, 1):
        s1[way, 1] = projected(3 if way == 0 else 5).astype(BF)
        near[way, 1] = links.copy(s1.at[way, 1], r1.at[way, 1], dz=1 if way == 0 else NZ - 1)
    pre_gate = Gate(links)

    def to_owners(slot, value, dz):
        last1[slot] = value.astype(BF)
        for dx in (2, 1, 3, 0):
            if dx or dz:
                links.copy(last1.at[slot, part_of(lax.rem(x + dx, NX))], pre.at[x, slot], dz=dz, dx=dx, gate=pre_gate)

    to_owners(1, projected(1), 1)
    to_owners(2, projected(7), NZ - 1)
    to_owners(0, projected(0), 0)
    for way in (0, 1):
        value = projected(2 if way == 0 else 6)
        near[way, 0].wait_recv()
        near[way, 1].wait_recv()
        half = value[:, way * F : (way + 1) * F] + r1[way, 0, :, way * F : (way + 1) * F].astype(F32)
        halves = [half, value[:, F:]] if way == 0 else [value[:, :F], half]
        to_owners(3 + way, jnp.concatenate(halves, axis=1) + r1[way, 1].astype(F32), 2 if way == 0 else NZ - 2)
    quarter = part_of(x)
    pre[x, 0] = last1[0, quarter, :]
    cols[...] = stats_total(stats1[0], got1, stats_gate)
    stat = cols[quarter, :]
    scale = lax.rsqrt(stat[:, 4:5] / D + EPS)
    lane = lax.broadcasted_iota(jnp.int32, (32, R), 1)
    row = lax.broadcasted_iota(jnp.int32, (32, R), 0)
    live = jnp.zeros((32, R), F32)
    for s in range(8):
        inside = (row // NEW == s) & (lax.rem(row, NEW) < len_ref[s])
        live = live + jnp.where(inside, 1.0, 0.0)
    rated = stat * scale
    beta = jax.nn.sigmoid(rated) * live
    rate = jnp.where(lane == 2, rate_ref[0], jnp.where(lane == 3, rate_ref[1], 0.0))
    softplus = jnp.maximum(rated, 0.0) + jnp.log1p(jnp.exp(-jnp.abs(rated)))
    keep = jnp.exp(-rate * softplus * live)
    pre_gate.wait()
    links.phase()

    def summed(i):
        return sum(pre[i, k].astype(F32) for k in range(5)) * scale

    given[8].wait()
    for dx in (1, 3, 2):
        to = lax.rem(x + dx, NX)
        links.copy(w_down.at[window(to)], wd.at[x], dx=dx, gate=late)
    query, key, value, gate = (silu(summed(i)) for i in range(4))

    def unit(a):
        return a * lax.rsqrt(jnp.sum(a * a, axis=1, keepdims=True) + EPS)

    stacked = []
    for h in range(2):
        at = slice(h * F, (h + 1) * F)
        stacked += [unit(query[:, at]) * F ** (-0.5), unit(key[:, at])]
    upper = lax.broadcasted_iota(jnp.int32, (8, F), 0) < NEW
    for pair in range(4):
        near8 = slice(pair * 8, pair * 8 + 8)
        for h in range(2):
            both = jnp.concatenate([stacked[2 * h][near8], stacked[2 * h + 1][near8]], axis=0)
            one, two = (
                jnp.dot(both, state_ref[2 * pair + i, h], precision=lax.Precision.HIGHEST, preferred_element_type=F32)
                for i in range(2)
            )
            for k in range(2):
                half = slice(k * 8, k * 8 + 8)
                on_first[k, near8, h * F : (h + 1) * F] = jnp.where(upper, one[half], two[half])
    position = lax.rem(row, NEW)

    def later_by(a, n):
        return jnp.concatenate([a[32 - n :], a[: 32 - n]], axis=0)

    def sooner_by(a, n):
        return jnp.concatenate([a[n:], a[:n]], axis=0)

    for h in range(2):
        at = slice(h * F, (h + 1) * F)
        q_now, k_now, v_now = stacked[2 * h], stacked[2 * h + 1], value[:, at]
        write = jnp.broadcast_to(beta[:, h : h + 1], (32, F))
        hold = jnp.broadcast_to(keep[:, 2 + h : 3 + h], (32, F))
        over1 = hold
        over2 = over1 * later_by(hold, 1)
        over3 = over2 * later_by(hold, 2)
        over4 = over3 * later_by(hold, 3)
        whole = jnp.where(position == 0, over1, jnp.where(position == 1, over2, jnp.where(position == 2, over3, over4)))
        alone = write * (v_now - whole * on_first[1, :, at])
        among_k, among_q = [], [jnp.sum(q_now * k_now, axis=1, keepdims=True)]
        for n, over_n in ((1, over1), (2, over2), (3, over3)):
            k_then = later_by(k_now, n)
            inside = jnp.where(position >= n, over_n, 0.0)
            among_k.append(write * inside * jnp.sum(k_now * k_then, axis=1, keepdims=True))
            among_q.append(inside * jnp.sum(q_now * k_then, axis=1, keepdims=True))
        update = alone
        for _ in range(NEW - 1):
            update = alone - sum(among_k[n - 1] * later_by(update, n) for n in (1, 2, 3))
        reading = whole * on_first[0, :, at] + among_q[0] * update
        for n in (1, 2, 3):
            reading = reading + among_q[n] * later_by(update, n)
        readings[:, at] = reading
        ahead1 = sooner_by(hold, 1)
        ahead2 = ahead1 * sooner_by(hold, 2)
        ahead3 = ahead2 * sooner_by(hold, 3)
        rest = jnp.where(position == 3, 1.0, jnp.where(position == 2, ahead1, jnp.where(position == 1, ahead2, ahead3)))
        updates[:, at] = rest * update
        decays[:, at] = whole
    for h in range(2):
        at = slice(h * F, (h + 1) * F)
        read = readings[:, at] * live
        normed = read * lax.rsqrt(jnp.mean(read * read, axis=1, keepdims=True) + EPS)
        mixed_own[:, at] = (normed * head_gain_ref[...] * gate[:, at]).astype(BF)

    mixed_gate = Gate(links)
    for dz in (4, 3, 5, 2, 6, 1, 7):
        links.copy(mixed_own, mz.at[z], dz=dz, gate=mixed_gate)
    mz[z] = mixed_own[...]
    turned = jnp.concatenate(stacked, axis=0).T
    for s in range(8):
        for h in range(2):
            at = slice(h * F, (h + 1) * F)
            state = decays[s * NEW + NEW - 1 : (s + 1) * NEW, at] * state_ref[s, h]
            for r in range(s * NEW, (s + 1) * NEW):
                state = state + turned[:, h * 64 + 32 + r : h * 64 + 33 + r] * updates[r : r + 1, at]
            state_ref[s, h] = state
    out_state = pltpu.make_async_copy(state_ref, next_hbm, local.at[10])
    out_state.start()
    own_out.wait()
    outs.wait()
    mixed_gate.wait()
    heads = jnp.concatenate([mz[k] for k in range(NZ)], axis=0)
    for k in range(NX):
        terms = jnp.dot(heads, wz[k], preferred_element_type=F32).astype(BF)
        for h in range(2):
            for b in range(NTP):
                obuf[h, b, :, k * F : (k + 1) * F] = terms[b * 32 + h * 16 : b * 32 + h * 16 + 16]
    tp_gates = [Gate(links), Gate(links)]
    for h in range(2):
        for k in (4, 3, 5, 2, 6, 1, 7):
            to = lax.rem(tp + k, NTP)
            links.copy_to(obuf.at[h, to], orecv.at[h, k], (z, x, to // NC, lax.rem(to, NC)), tp_gates[h])

    finish = []
    for h in range(2):
        attended = obuf[h, tp].astype(F32)
        links.phase()
        tp_gates[h].wait()
        for k in range(1, NTP):
            attended = attended + orecv[h, k].astype(F32)
        at = pl.ds(pl.multiple_of(tp * R + x * 32 + h * 16, 16), 16)
        given = jnp.concatenate([xbuf[k, at, :] for k in range(NX)], axis=1).astype(F32)
        hown[h] = (given + attended).astype(BF)
        hb[h, tp, pl.ds(pl.multiple_of(x * 16, 16), 16), :] = hown[h]
        finish.append(gather_straight(links, hown.at[h], hb.at[h], 16))

    stats_gates, ready2 = (Gate(links), Gate(links)), ({}, {})

    def mixer(h):
        def block(offset):
            if offset not in ready2[h]:
                ready2[h][offset] = True
                wide = hb[h, lax.rem(z + offset, NZ)].astype(F32)
                normed = (wide * gain2).astype(BF)
                p2[h, offset, :, :WIN] = jnp.dot(normed, wg[...], preferred_element_type=F32)
                p2[h, offset, :, WIN:] = jnp.dot(normed, wu[...], preferred_element_type=F32)
                stats2[h, offset] = square_rows(wide)
                if offset:
                    links.copy(stats2.at[h, offset], got2.at[h, offset], dz=offset, gate=stats_gates[h])
            return p2[h, offset]

        return RingSumWhole(links, block, s2.at[h], r2.at[h], 2 * WIN)

    sums = [mixer(h) for h in range(2)]
    gathers = [RingGather(links, abuf.at[h], 64) for h in range(2)]
    odd = lax.rem(z + c, 2)
    partner = (z, x, y, 1 - c)

    def activate(h):
        total = sums[h].total()
        scale2 = lax.rsqrt(stats_total(stats2[h, 0], got2.at[h], stats_gates[h])[:64, 0:1] / D + EPS)
        activated = silu(scale2 * total[:, :WIN]) * (scale2 * total[:, WIN:])
        again = (lax.broadcasted_iota(jnp.int32, (64, WIN), 1) < F) & (x == NX - 1)
        abuf[h, z] = jnp.where(again, 0.0, activated).astype(BF)
        gathers[h].step(0)
        down(h, 0)

    def down(h, offset):
        block = abuf[h, lax.rem(z + offset, NZ)]
        for k in range(NX):
            part[h, offset, :, k * F : (k + 1) * F] = jnp.dot(block, wd[k], preferred_element_type=F32)

    turns = (0, 6, 2, 4)
    over = {(h, base): links.fresh() for h in range(2) for base in turns}

    def give(h, base):
        at = base + 1 - odd
        psend[h, at] = part[h, at].astype(BF)
        over_made[h, base] = links.copy_to(psend.at[h, at], precv.at[h, at], partner, index=over[h, base])

    over_made = {}

    def gather_step(h, step):
        gathers[h].step(step) if step < 4 else gathers[h].finish()
        if step < 4:
            down(h, NZ - step)
            down(h, step)
        else:
            down(h, 4)
        give(h, turns[step - 1])

    last_gates = [Gate(links), Gate(links)]

    def spread(h, turn):
        at = turns[turn] + odd
        over_made[h, turns[turn]].wait_recv()
        both = (part[h, at] + precv[h, at].astype(F32)).astype(BF)
        for k in range(NX):
            fsend[h, turn, k] = both[:, k * F : (k + 1) * F]
        to = lax.rem(z + at, NZ) // NC
        for dx in (2, 1, 3):
            xd = lax.rem(x + dx, NX)
            links.copy_to(fsend.at[h, turn, xd], frecv.at[h, y * NX + x], (z, xd, to, c), last_gates[h])

        @pl.when(to != y)
        def _():
            links.copy_to(fsend.at[h, turn, x], frecv.at[h, y * NX + x], (z, x, to, c), last_gates[h])

        @pl.when(to == y)
        def _():
            frecv[h, y * NX + x] = fsend[h, turn, x]

        if turn == 3:
            links.sent[-1] -= 2 * 64 * F
            last_gates[h].size -= 2 * 64 * F

    def put(h):
        result = hb[h, tp, :, feats].astype(F32)
        last_gates[h].wait()
        for i in range(NX * NY):
            result = result + frecv[h, i].astype(F32)
        result = result.astype(BF)
        for k in range(NX):
            out_ref[k * 32 + h * 16 : k * 32 + h * 16 + 16, :] = result[k * 16 : (k + 1) * 16]

    finish[0]()
    for one in own_late:
        one.wait()
    late.wait()
    links.phase()
    sums[0].first()
    finish[1]()
    sums[1].first()
    sums[0].later(0)
    sums[1].later(0)
    sums[0].later(1)
    sums[1].later(1)
    sums[0].later(2)
    sums[1].later(2)
    links.phase()
    activate(0)
    activate(1)
    links.phase()
    gather_step(0, 1)
    gather_step(1, 1)
    gather_step(0, 2)
    spread(0, 0)
    gather_step(1, 2)
    spread(1, 0)
    gather_step(0, 3)
    spread(0, 1)
    gather_step(1, 3)
    spread(1, 1)
    gather_step(0, 4)
    spread(0, 2)
    gather_step(1, 4)
    spread(1, 2)
    spread(0, 3)
    spread(1, 3)
    put(0)
    put(1)
    out_state.wait()
    links.drain()


def hand_over(out_tmp, state_tmp, out_ref, state_out, held_out, held_state, came, went):
    pieces = [(out_tmp, held_out, out_ref)]
    pieces += [(state_tmp.at[i], held_state.at[i], state_out.at[i]) for i in range(8)]
    coming = [pltpu.make_async_copy(a, b, came.at[i]) for i, (a, b, _) in enumerate(pieces)]
    going = [pltpu.make_async_copy(b, c, went.at[i]) for i, (_, b, c) in enumerate(pieces)]
    for one in coming:
        one.start()
    for one, two in zip(coming, going):
        one.wait()
        two.start()
    for two in going:
        two.wait()


def local(
    layer_input, seq_lengths, delta_state, attn_gain, w_query, w_key, w_value, w_outgate, w_write, w_forget,
    forget_rate, head_gain, w_out, mixer_gain, w_gate, w_up, w_down,
):
    vmem = pl.BlockSpec(memory_space=pltpu.VMEM)
    hbm = pl.BlockSpec(memory_space=pltpu.HBM)
    scratch = [
        ((NX, NTP * R, F), BF),
        ((4, F, 256), BF),
        ((NX * F, 256), BF),
        ((16, F), BF),
        ((NX, 16, F), BF),
        ((NZ, R, 256), F32),
        ((2, 2, R, 256), BF),
        ((2, 2, R, 256), BF),
        ((NZ, 8, R), F32),
        ((NZ, 8, R), F32),
        ((NX, 5, 32, 256), BF),
        ((5, R, 256), BF),
        ((R, R), F32),
        ((2, 32, 256), F32),
        ((32, 256), F32),
        ((32, 256), F32),
        ((32, 256), F32),
        ((32, 256), BF),
        ((NX, 256, F), BF),
        ((NZ, 32, 256), BF),
        ((2, NTP, 16, NX * F), BF),
        ((2, NTP, 16, NX * F), BF),
        ((2, 16, NX * F), BF),
        ((2, NTP, 64, NX * F), BF),
        ((2, NZ, 8, R), F32),
        ((2, NZ, 8, R), F32),
        ((NX * F, WIN), BF),
        ((NX * F, WIN), BF),
        ((NX, WIN, F), BF),
        ((2, NZ, 64, 2 * WIN), F32),
        ((2, 2, 4, 64, 2 * WIN), BF),
        ((2, 2, 4, 64, 2 * WIN), BF),
        ((2, NZ, 64, WIN), BF),
        ((2, NZ, 64, NX * F), F32),
        ((2, NZ, 64, NX * F), BF),
        ((2, NZ, 64, NX * F), BF),
        ((2, NY, NX, 64, F), BF),
        ((2, NX * NY, 64, F), BF),
    ]
    held = [
        pltpu.VMEM((R, F), BF),
        pltpu.SMEM((8,), jnp.int32),
        pltpu.VMEM(delta_state.shape, F32),
        pltpu.VMEM((32, F), BF),
        pltpu.VMEM((2, F), BF),
        pltpu.VMEM((2, F), BF),
        pltpu.SMEM((2,), F32),
        pltpu.VMEM((1, F), F32),
        pltpu.VMEM((32, F), BF),
    ]
    out_tmp, state_tmp = pl.pallas_call(
        body,
        out_shape=(
            jax.ShapeDtypeStruct((R, F), BF),
            jax.ShapeDtypeStruct(delta_state.shape, F32),
        ),
        in_specs=[
            hbm, hbm, hbm, hbm, hbm, hbm, hbm, hbm, hbm, hbm, hbm, hbm, hbm, hbm, hbm, hbm, hbm,
        ],
        out_specs=(vmem, hbm),
        scratch_shapes=[pltpu.VMEM(shape, dtype) for shape, dtype in scratch]
        + held
        + [
            pltpu.VMEM((16384, F), BF),
            pltpu.SemaphoreType.DMA((20,)),
            pltpu.SemaphoreType.DMA((NSEND,)),
            pltpu.SemaphoreType.DMA((NRECV,)),
        ],
        compiler_params=pltpu.CompilerParams(
            collective_id=0, has_side_effects=True, vmem_limit_bytes=VMEM_LIMIT
        ),
    )(
        layer_input, seq_lengths, delta_state, attn_gain.reshape(32, F), w_query, w_key, w_value, w_outgate,
        w_write.T, w_forget.T, forget_rate, head_gain.reshape(1, F), w_out, mixer_gain.reshape(32, F), w_gate, w_up,
        w_down,
    )
    return pl.pallas_call(
        hand_over,
        out_shape=(
            jax.ShapeDtypeStruct((R, F), BF),
            jax.ShapeDtypeStruct(delta_state.shape, F32),
        ),
        in_specs=[hbm, hbm],
        out_specs=(hbm, hbm),
        scratch_shapes=[
            pltpu.VMEM((R, F), BF),
            pltpu.VMEM(delta_state.shape, F32),
            pltpu.SemaphoreType.DMA((9,)),
            pltpu.SemaphoreType.DMA((9,)),
        ],
        compiler_params=pltpu.CompilerParams(vmem_limit_bytes=VMEM_LIMIT),
    )(out_tmp, state_tmp)


def solution(mesh):
    split = Mesh(mesh.devices.reshape(NZ, NX, NY, NC), ("z", "x", "y", "c"))
    kv, tp = ("z", "x"), ("y", "c")
    in_specs = (
        P(tp, kv), P(kv), P(kv, tp, None, None), P(), P(kv, tp), P(kv, tp), P(kv, tp), P(kv, tp), P(kv, tp),
        P(kv, tp), P(tp), P(), P(tp, kv), P(), P(kv, tp), P(kv, tp), P(tp, kv),
    )
    out_specs = (P(tp, kv), P(kv, tp, None, None))
    return jax.shard_map(local, mesh=split, in_specs=in_specs, out_specs=out_specs, check_vma=False)
```

```python
import math

import jax
import jax.numpy as jnp
from jax import lax
from jax.experimental import pallas as pl
from jax.experimental.pallas import tpu as pltpu
from jax.sharding import Mesh
from jax.sharding import PartitionSpec as P

D = 4096
NEW = 4
EPS = 1e-06
NZ, NX, NY, NC = 8, 4, 4, 2
NTP = NY * NC
R = 128
F = 128
WIN = 384
MESH = pl.DeviceIdType.MESH
BF = jnp.bfloat16
F32 = jnp.float32
PLANE = [(dx, dy) for dx in range(NX) for dy in range(NY) if dx or dy]
STRAIGHT = (False, False)
NRECV = 110 - 2 * sum(STRAIGHT)
NSEND = 10
VMEM_LIMIT = 58 * 1024 * 1024


def silu(a):
    return a * jax.nn.sigmoid(a)


def rows_of(k):
    return pl.ds(pl.multiple_of(k * R, R), R)


def dot_t(a, b):
    return lax.dot_general(a, b, (((1,), (1,)), ((), ())), preferred_element_type=F32)


class Gate:
    def __init__(self, links):
        self.links, self.index, self.size = links, links.fresh(), 0

    def wait(self):
        self.links.wait_bytes(self.links.recv.at[self.index], self.size)


class Links:
    def __init__(self, send, recv, ruler):
        self.send, self.recv, self.ruler, self.n, self.sent = send, recv, ruler, 0, []
        self.z, self.x = lax.axis_index("z"), lax.axis_index("x")
        self.y, self.c = lax.axis_index("y"), lax.axis_index("c")

    def fresh(self):
        self.n += 1
        return self.n - 1

    def phase(self):
        self.sent.append(0)

    def copy(self, src, dst, dz=0, dx=0, dy=0, dc=0, gate=None):
        to = (
            lax.rem(self.z + dz, NZ),
            lax.rem(self.x + dx, NX),
            lax.rem(self.y + dy, NY),
            lax.rem(self.c + dc, NC),
        )
        return self.copy_to(src, dst, to, gate)

    def copy_to(self, src, dst, to, gate=None, index=None):
        size = math.prod(src.shape) * jnp.dtype(src.dtype).itemsize
        self.sent[-1] += size
        if gate is not None:
            gate.size += size
            index = gate.index
        elif index is None:
            index = self.fresh()
        made = pltpu.make_async_remote_copy(
            src_ref=src,
            dst_ref=dst,
            send_sem=self.send.at[len(self.sent) - 1],
            recv_sem=self.recv.at[index],
            device_id=to,
            device_id_type=MESH,
        )
        made.start()
        return made

    def wait_bytes(self, sem, size):
        part = self.ruler.at[pl.ds(0, size // (2 * F))]
        pltpu.make_async_copy(part, part, sem).wait()

    def drain(self):
        for i, size in enumerate(self.sent):
            self.wait_bytes(self.send.at[i], size)
        assert self.n == NRECV and len(self.sent) == NSEND, (self.n, len(self.sent))


def greet(links):
    z, x, y, c = links.z, links.x, links.y, links.c
    barrier = pltpu.get_barrier_semaphore()
    to = [(dz, 0, 0, 0) for dz in (4, 3, 5)]
    to += [(dz, dx, 0, 0) for dz in (2, NZ - 2, 1, NZ - 1, 0) for dx in range(NX) if dz or dx]
    to += [(0, dx, dy, 0) for dx in range(NX) for dy in range(1, NY)]
    to += [(0, 0, dy, 1) for dy in range(NY)]
    for dz, dx, dy, dc in to:
        pl.semaphore_signal(
            barrier,
            inc=1,
            device_id=(lax.rem(z + dz, NZ), lax.rem(x + dx, NX), lax.rem(y + dy, NY), lax.rem(c + dc, NC)),
            device_id_type=MESH,
        )
    return lambda: pl.semaphore_wait(barrier, len(to))


def gather_x_first(links, src, buf):
    z, x, y, c = links.z, links.x, links.y, links.c
    along_x = {dx: links.copy(src, buf.at[x, rows_of(y * NC + c)], dx=dx) for dx in (1, 3, 2)}
    along_y = {}
    for dy in (1, 3, 2):
        along_y[0, dy] = links.copy(src, buf.at[x, rows_of(y * NC + c)], dy=dy)
    forward = Gate(links)
    links.copy(src, buf.at[x, rows_of(y * NC + c)], dc=1, gate=forward)

    def finish():
        def block(dx, dy):
            return buf.at[lax.rem(x - dx + NX, NX), rows_of(lax.rem(y - dy + NY, NY) * NC + c)]

        for dx in (1, 3, 2):
            along_x[dx].wait_recv()
            for dy in (1, 3, 2):
                along_y[dx, dy] = links.copy(block(dx, 0), block(dx, 0), dy=dy)
            links.copy(block(dx, 0), block(dx, 0), dc=1, gate=forward)
        for dx in (0, 1, 3, 2):
            for dy in (1, 3, 2):
                along_y[dx, dy].wait_recv()
                links.copy(block(dx, dy), block(dx, dy), dc=1, gate=forward)
        forward.wait()

    return finish


def gather_straight(links, src, buf, rows):
    x, y, c = links.x, links.y, links.c

    def block(xs, ys):
        return buf.at[ys * NC + c, pl.ds(pl.multiple_of(xs * rows, rows), rows)]

    straight = [links.copy(src, block(x, y), dx=dx, dy=dy) for dx, dy in PLANE]
    forward = Gate(links)
    links.copy(src, block(x, y), dc=1, gate=forward)

    def finish():
        for (dx, dy), made in zip(PLANE, straight):
            made.wait_recv()
            came = block(lax.rem(x - dx + NX, NX), lax.rem(y - dy + NY, NY))
            links.copy(came, came, dc=1, gate=forward)
        forward.wait()

    return finish


FAR, THREE, TWO, ONE = range(4)


class RingSum:
    def __init__(self, links, block, sendbuf, recvbuf, width, straight):
        self.links, self.block, self.sendbuf, self.recvbuf = links, block, sendbuf, recvbuf
        self.half, self.made, self.straight = width // 2, {}, straight

    def lanes(self, side):
        return slice(None) if side is None else slice(side * self.half, (side + 1) * self.half)

    def add(self, value, way, kind, side, lanes):
        self.made[way, kind, side].wait_recv()
        return value + self.recvbuf[way, kind, :, lanes].astype(F32)

    def send(self, way, kind, side=None):
        lanes = self.lanes(side)
        value = self.block(4 - kind if way == 0 else 4 + kind)[:, lanes]
        if kind == THREE and side == way:
            value = self.add(value, way, FAR, side, lanes)
        elif kind == TWO and self.straight:
            parts = [value[:, : self.half], value[:, self.half :]]
            parts[way] = self.add(parts[way], way, FAR, way, self.lanes(way))
            value = self.add(jnp.concatenate(parts, axis=1), way, THREE, None, lanes)
        elif kind == TWO:
            self.made[way, THREE, 1 - way].wait_recv()
            value = self.add(value, way, THREE, way, lanes)
        elif kind == ONE:
            value = self.add(value, way, TWO, None, lanes)
        self.sendbuf[way, kind, :, lanes] = value.astype(BF)
        at = (way, kind) if side is None else (way, kind, slice(None), pl.ds(side * self.half, self.half))
        hops = 2 if kind == FAR and self.straight else 1
        self.made[way, kind, side] = self.links.copy(
            self.sendbuf.at[at], self.recvbuf.at[at], dz=hops if way == 0 else NZ - hops
        )

    def farthest(self):
        for way in (0, 1):
            self.send(way, FAR, way)

    def three(self):
        for way in (0, 1):
            self.send(way, THREE, None if self.straight else 1 - way)

    def later(self, number):
        if number or not self.straight:
            for way in (0, 1):
                self.send(way, *((THREE, way), (TWO, None), (ONE, None))[number])

    def total(self):
        value = self.block(0)
        for way in (0, 1):
            value = self.add(value, way, ONE, None, slice(None))
        return value


class RingGather:
    def __init__(self, links, buf, rows):
        self.links, self.buf, self.rows, self.going = links, buf, rows // 2, {}

    def step(self, step):
        for way in (0, 1):
            if step:
                self.going[way, step].wait_recv()
            at = lax.rem(self.links.z + (NZ - step if way == 0 else step), NZ)
            if step == 2:
                half = self.buf.at[at, pl.ds(way * self.rows, self.rows)]
                self.going[way, 4] = self.links.copy(half, half, dz=2 if way == 0 else NZ - 2)
            if step < 3:
                self.going[way, step + 1] = self.links.copy(
                    self.buf.at[at], self.buf.at[at], dz=1 if way == 0 else NZ - 1
                )

    def finish(self):
        for way in (0, 1):
            self.going[way, 4].wait_recv()


def square_rows(wide):
    squares = wide * wide
    squares = squares[:, :F] + squares[:, F : 2 * F] + squares[:, 2 * F : 3 * F] + squares[:, 3 * F :]
    if wide.shape[0] < R:
        squares = jnp.concatenate([squares, jnp.zeros((R - wide.shape[0], F), F32)], axis=0)
    ones = jnp.ones((16, F), BF)
    high = squares.astype(BF)
    low = (squares - high.astype(F32)).astype(BF)
    return (dot_t(ones, high) + dot_t(ones, low))[:8]


def stats_total(own, got, gate):
    gate.wait()
    total = own
    for offset in range(1, NZ):
        total = total + got[offset]
    return jnp.concatenate([total, jnp.zeros((R - 8, R), F32)], axis=0).T


def body(
    x_hbm, len_hbm, state_hbm, gain1_hbm, wq, wk, wv, wo, write_hbm, forget_hbm, rate_hbm, head_gain_hbm, w_out,
    gain2_hbm, w_gate, w_up, w_down,
    out_ref, next_hbm,
    xbuf, w4, wr, rate_w, rw, p1, s1, r1, stats1, got1, pre, last1, cols, on_first, updates, decays, readings, mixed_own, wz, mz, obuf, orecv,
    hown, hb, stats2, got2, wg, wu, wd, p2, s2, r2, abuf, part, psend, precv, fsend, frecv,
    x_ref, len_ref, state_ref, gain1_ref, write_ref, forget_ref, rate_ref, head_gain_ref, gain2_ref,
    ruler, local, send, recv,
):
    links = Links(send, recv, ruler)
    links.phase()
    arrive = greet(links)
    z, x, y, c = links.z, links.x, links.y, links.c
    tp = y * NC + c

    locals_ = [pltpu.make_async_copy(w, w4.at[i], local.at[i]) for i, w in enumerate((wq, wk, wv, wo))]

    def window(at):
        return pl.ds(pl.multiple_of((at * 3 - at // (NX - 1)) * F, F), WIN)

    feats = pl.ds(pl.multiple_of(x * F, F), F)
    given = [
        pltpu.make_async_copy(far, near, local.at[11 + i])
        for i, (far, near) in enumerate(
            (
                (x_hbm, x_ref), (write_hbm, write_ref), (forget_hbm, forget_ref), (gain1_hbm, gain1_ref),
                (gain2_hbm, gain2_ref), (len_hbm, len_ref), (rate_hbm, rate_ref), (head_gain_hbm, head_gain_ref),
                (state_hbm, state_ref),
            )
        )
    ]
    for one in given:
        one.start()
    own_x = pltpu.make_async_copy(x_hbm, xbuf.at[x, rows_of(tp)], local.at[4])
    own_out = pltpu.make_async_copy(w_out, wz.at[x], local.at[5])
    own_late = [
        pltpu.make_async_copy(w_gate.at[:, window(x)], wg.at[feats], local.at[6]),
        pltpu.make_async_copy(w_up.at[:, window(x)], wu.at[feats], local.at[7]),
        pltpu.make_async_copy(w_down.at[window(x)], wd.at[x], local.at[8]),
    ]
    for one in locals_ + [own_x, own_out] + own_late:
        one.start()
    arrive()

    given[0].wait()
    finish = gather_x_first(links, x_ref, xbuf)
    for one in given[1:8]:
        one.wait()
    small = [write_ref[...].astype(F32), forget_ref[...].astype(F32), jnp.zeros((12, F), F32)]
    rate_w[...] = jnp.concatenate(small, axis=0).astype(BF)
    rw[x] = rate_w[...]
    for one in locals_:
        one.wait()
    own_w = pltpu.make_async_copy(w4.at[x], wr.at[feats], local.at[9])
    own_w.start()
    early, early_rates, late, outs = Gate(links), Gate(links), Gate(links), Gate(links)
    for dx in (1, 3, 2):
        to = lax.rem(x + dx, NX)
        links.copy(w4.at[to], wr.at[feats], dx=dx, gate=early)
        links.copy(rate_w, rw.at[x], dx=dx, gate=early_rates)
    links.phase()
    for dx in (1, 3, 2):
        links.copy(w_out, wz.at[x], dx=dx, gate=outs)
    for dx in (1, 3, 2):
        to = lax.rem(x + dx, NX)
        links.copy(w_gate.at[:, window(to)], wg.at[feats], dx=dx, gate=late)
        links.copy(w_up.at[:, window(to)], wu.at[feats], dx=dx, gate=late)
    links.phase()

    which = lax.broadcasted_iota(jnp.int32, (32, F), 0)

    def gain_of(ref):
        wide = ref[...].astype(F32)
        return jnp.concatenate(
            [jnp.sum(jnp.where(which == z * NX + k, wide, 0.0), axis=0, keepdims=True) for k in range(NX)], axis=1
        )

    gain1, gain2 = gain_of(gain1_ref), gain_of(gain2_ref)
    own_x.wait()
    own_w.wait()
    finish()
    early.wait()
    early_rates.wait()
    links.phase()

    sub = lax.broadcasted_iota(jnp.int32, (8, R), 0)
    stats_gate, ready = Gate(links), {}

    def projected(offset):
        if offset not in ready:
            ready[offset] = True
            at = rows_of(lax.rem(z + offset, NZ))
            wide = jnp.concatenate([xbuf[k, at, :] for k in range(NX)], axis=1).astype(F32)
            normed = (wide * gain1).astype(BF)
            p1[offset] = jnp.dot(normed, wr[...], preferred_element_type=F32)
            stat = jnp.where(sub == 4, square_rows(wide), 0.0)
            for k in range(NX):
                stat = stat + dot_t(rw[k], normed[:, k * F : (k + 1) * F])[:8]
            stats1[offset] = stat
            if offset:
                links.copy(stats1.at[offset], got1.at[offset], dz=offset, gate=stats_gate)
        return p1[offset]

    def part_of(at):
        return pl.ds(pl.multiple_of(at * 32, 32), 32)

    near = {}
    for way in (0, 1):
        side = pl.ds(way * F, F)
        s1[way, 0, :, way * F : (way + 1) * F] = projected(4)[:, way * F : (way + 1) * F].astype(BF)
        near[way, 0] = links.copy(s1.at[way, 0, :, side], r1.at[way, 0, :, side], dz=2 if way == 0 else NZ - 2)
    for way in (0, 1):
        s1[way, 1] = projected(3 if way == 0 else 5).astype(BF)
        near[way, 1] = links.copy(s1.at[way, 1], r1.at[way, 1], dz=1 if way == 0 else NZ - 1)
    pre_gate = Gate(links)

    def to_owners(slot, value, dz):
        last1[slot] = value.astype(BF)
        for dx in (2, 1, 3, 0):
            if dx or dz:
                links.copy(last1.at[slot, part_of(lax.rem(x + dx, NX))], pre.at[x, slot], dz=dz, dx=dx, gate=pre_gate)

    to_owners(1, projected(1), 1)
    to_owners(2, projected(7), NZ - 1)
    to_owners(0, projected(0), 0)
    for way in (0, 1):
        value = projected(2 if way == 0 else 6)
        near[way, 0].wait_recv()
        near[way, 1].wait_recv()
        half = value[:, way * F : (way + 1) * F] + r1[way, 0, :, way * F : (way + 1) * F].astype(F32)
        halves = [half, value[:, F:]] if way == 0 else [value[:, :F], half]
        to_owners(3 + way, jnp.concatenate(halves, axis=1) + r1[way, 1].astype(F32), 2 if way == 0 else NZ - 2)
    quarter = part_of(x)
    pre[x, 0] = last1[0, quarter, :]
    cols[...] = stats_total(stats1[0], got1, stats_gate)
    stat = cols[quarter, :]
    scale = lax.rsqrt(stat[:, 4:5] / D + EPS)
    lane = lax.broadcasted_iota(jnp.int32, (32, R), 1)
    row = lax.broadcasted_iota(jnp.int32, (32, R), 0)
    live = jnp.zeros((32, R), F32)
    for s in range(8):
        inside = (row // NEW == s) & (lax.rem(row, NEW) < len_ref[s])
        live = live + jnp.where(inside, 1.0, 0.0)
    rated = stat * scale
    beta = jax.nn.sigmoid(rated) * live
    rate = jnp.where(lane == 2, rate_ref[0], jnp.where(lane == 3, rate_ref[1], 0.0))
    softplus = jnp.maximum(rated, 0.0) + jnp.log1p(jnp.exp(-jnp.abs(rated)))
    keep = jnp.exp(-rate * softplus * live)
    pre_gate.wait()
    links.phase()

    def summed(i):
        return sum(pre[i, k].astype(F32) for k in range(5)) * scale

    given[8].wait()
    for dx in (1, 3, 2):
        to = lax.rem(x + dx, NX)
        links.copy(w_down.at[window(to)], wd.at[x], dx=dx, gate=late)
    query, key, value, gate = (silu(summed(i)) for i in range(4))

    def unit(a):
        return a * lax.rsqrt(jnp.sum(a * a, axis=1, keepdims=True) + EPS)

    stacked = []
    for h in range(2):
        at = slice(h * F, (h + 1) * F)
        stacked += [unit(query[:, at]) * F ** (-0.5), unit(key[:, at])]
    upper = lax.broadcasted_iota(jnp.int32, (8, F), 0) < NEW
    for pair in range(4):
        near8 = slice(pair * 8, pair * 8 + 8)
        for h in range(2):
            both = jnp.concatenate([stacked[2 * h][near8], stacked[2 * h + 1][near8]], axis=0)
            one, two = (
                jnp.dot(both, state_ref[2 * pair + i, h], precision=lax.Precision.HIGHEST, preferred_element_type=F32)
                for i in range(2)
            )
            for k in range(2):
                half = slice(k * 8, k * 8 + 8)
                on_first[k, near8, h * F : (h + 1) * F] = jnp.where(upper, one[half], two[half])
    position = lax.rem(row, NEW)

    def later_by(a, n):
        return jnp.concatenate([a[32 - n :], a[: 32 - n]], axis=0)

    def sooner_by(a, n):
        return jnp.concatenate([a[n:], a[:n]], axis=0)

    for h in range(2):
        at = slice(h * F, (h + 1) * F)
        q_now, k_now, v_now = stacked[2 * h], stacked[2 * h + 1], value[:, at]
        write = jnp.broadcast_to(beta[:, h : h + 1], (32, F))
        hold = jnp.broadcast_to(keep[:, 2 + h : 3 + h], (32, F))
        over1 = hold
        over2 = over1 * later_by(hold, 1)
        over3 = over2 * later_by(hold, 2)
        over4 = over3 * later_by(hold, 3)
        whole = jnp.where(position == 0, over1, jnp.where(position == 1, over2, jnp.where(position == 2, over3, over4)))
        alone = write * (v_now - whole * on_first[1, :, at])
        among_k, among_q = [], [jnp.sum(q_now * k_now, axis=1, keepdims=True)]
        for n, over_n in ((1, over1), (2, over2), (3, over3)):
            k_then = later_by(k_now, n)
            inside = jnp.where(position >= n, over_n, 0.0)
            among_k.append(write * inside * jnp.sum(k_now * k_then, axis=1, keepdims=True))
            among_q.append(inside * jnp.sum(q_now * k_then, axis=1, keepdims=True))
        update = alone
        for _ in range(NEW - 1):
            update = alone - sum(among_k[n - 1] * later_by(update, n) for n in (1, 2, 3))
        reading = whole * on_first[0, :, at] + among_q[0] * update
        for n in (1, 2, 3):
            reading = reading + among_q[n] * later_by(update, n)
        readings[:, at] = reading
        ahead1 = sooner_by(hold, 1)
        ahead2 = ahead1 * sooner_by(hold, 2)
        ahead3 = ahead2 * sooner_by(hold, 3)
        rest = jnp.where(position == 3, 1.0, jnp.where(position == 2, ahead1, jnp.where(position == 1, ahead2, ahead3)))
        updates[:, at] = rest * update
        decays[:, at] = whole
    for h in range(2):
        at = slice(h * F, (h + 1) * F)
        read = readings[:, at] * live
        normed = read * lax.rsqrt(jnp.mean(read * read, axis=1, keepdims=True) + EPS)
        mixed_own[:, at] = (normed * head_gain_ref[...] * gate[:, at]).astype(BF)

    mixed_gates = [Gate(links), Gate(links)]
    for h in range(2):
        mz[h, z] = mixed_own[h * 16 : h * 16 + 16, :]
        for dz in (4, 3, 5, 2, 6, 1, 7):
            links.copy(mixed_own.at[pl.ds(h * 16, 16)], mz.at[h, z], dz=dz, gate=mixed_gates[h])
    turned = jnp.concatenate(stacked, axis=0).T
    for s in range(8):
        for h in range(2):
            at = slice(h * F, (h + 1) * F)
            state = decays[s * NEW + NEW - 1 : (s + 1) * NEW, at] * state_ref[s, h]
            for r in range(s * NEW, (s + 1) * NEW):
                state = state + turned[:, h * 64 + 32 + r : h * 64 + 33 + r] * updates[r : r + 1, at]
            state_ref[s, h] = state
    out_state = pltpu.make_async_copy(state_ref, next_hbm, local.at[10])
    out_state.start()
    own_out.wait()
    outs.wait()
    tp_gates = [Gate(links), Gate(links)]
    for h in range(2):
        mixed_gates[h].wait()
        heads = jnp.concatenate([mz[h, k] for k in range(NZ)], axis=0)
        for k in range(NX):
            terms = jnp.dot(heads, wz[k], preferred_element_type=F32).astype(BF)
            for b in range(NTP):
                obuf[h, b, :, k * F : (k + 1) * F] = terms[b * 16 : b * 16 + 16]
        for k in (4, 3, 5, 2, 6, 1, 7):
            to = lax.rem(tp + k, NTP)
            links.copy_to(obuf.at[h, to], orecv.at[h, k], (z, x, to // NC, lax.rem(to, NC)), tp_gates[h])

    finish = []
    for h in range(2):
        attended = obuf[h, tp].astype(F32)
        links.phase()
        tp_gates[h].wait()
        for k in range(1, NTP):
            attended = attended + orecv[h, k].astype(F32)
        at = pl.ds(pl.multiple_of(tp * R + x * 32 + h * 16, 16), 16)
        given = jnp.concatenate([xbuf[k, at, :] for k in range(NX)], axis=1).astype(F32)
        hown[h] = (given + attended).astype(BF)
        hb[h, tp, pl.ds(pl.multiple_of(x * 16, 16), 16), :] = hown[h]
        finish.append(gather_straight(links, hown.at[h], hb.at[h], 16))

    stats_gates, ready2 = (Gate(links), Gate(links)), ({}, {})

    def mixer(h):
        def block(offset):
            if offset not in ready2[h]:
                ready2[h][offset] = True
                wide = hb[h, lax.rem(z + offset, NZ)].astype(F32)
                normed = (wide * gain2).astype(BF)
                p2[h, offset, :, :WIN] = jnp.dot(normed, wg[...], preferred_element_type=F32)
                p2[h, offset, :, WIN:] = jnp.dot(normed, wu[...], preferred_element_type=F32)
                stats2[h, offset] = square_rows(wide)
                if offset:
                    links.copy(stats2.at[h, offset], got2.at[h, offset], dz=offset, gate=stats_gates[h])
            return p2[h, offset]

        return RingSum(links, block, s2.at[h], r2.at[h], 2 * WIN, STRAIGHT[h])

    sums = [mixer(h) for h in range(2)]
    gathers = [RingGather(links, abuf.at[h], 64) for h in range(2)]
    odd = lax.rem(z + c, 2)
    partner = (z, x, y, 1 - c)

    def activate(h):
        total = sums[h].total()
        scale2 = lax.rsqrt(stats_total(stats2[h, 0], got2.at[h], stats_gates[h])[:64, 0:1] / D + EPS)
        activated = silu(scale2 * total[:, :WIN]) * (scale2 * total[:, WIN:])
        again = (lax.broadcasted_iota(jnp.int32, (64, WIN), 1) < F) & (x == NX - 1)
        abuf[h, z] = jnp.where(again, 0.0, activated).astype(BF)
        gathers[h].step(0)
        down(h, 0)

    def down(h, offset):
        block = abuf[h, lax.rem(z + offset, NZ)]
        for k in range(NX):
            part[h, offset, :, k * F : (k + 1) * F] = jnp.dot(block, wd[k], preferred_element_type=F32)

    turns = (0, 6, 2, 4)
    over = {(h, base): links.fresh() for h in range(2) for base in turns}

    def give(h, base):
        at = base + 1 - odd
        psend[h, at] = part[h, at].astype(BF)
        over_made[h, base] = links.copy_to(psend.at[h, at], precv.at[h, at], partner, index=over[h, base])

    over_made = {}

    def gather_step(h, step):
        gathers[h].step(step) if step < 4 else gathers[h].finish()
        if step < 4:
            down(h, NZ - step)
            down(h, step)
        else:
            down(h, 4)
        give(h, turns[step - 1])

    last_gates = [Gate(links), Gate(links)]

    def spread(h, turn):
        at = turns[turn] + odd
        over_made[h, turns[turn]].wait_recv()
        both = (part[h, at] + precv[h, at].astype(F32)).astype(BF)
        for k in range(NX):
            fsend[h, turn, k] = both[:, k * F : (k + 1) * F]
        to = lax.rem(z + at, NZ) // NC
        for dx in (2, 1, 3):
            xd = lax.rem(x + dx, NX)
            links.copy_to(fsend.at[h, turn, xd], frecv.at[h, y * NX + x], (z, xd, to, c), last_gates[h])

        @pl.when(to != y)
        def _():
            links.copy_to(fsend.at[h, turn, x], frecv.at[h, y * NX + x], (z, x, to, c), last_gates[h])

        @pl.when(to == y)
        def _():
            frecv[h, y * NX + x] = fsend[h, turn, x]

        if turn == 3:
            links.sent[-1] -= 2 * 64 * F
            last_gates[h].size -= 2 * 64 * F

    def put(h):
        result = hb[h, tp, :, feats].astype(F32)
        last_gates[h].wait()
        for i in range(NX * NY):
            result = result + frecv[h, i].astype(F32)
        result = result.astype(BF)
        for k in range(NX):
            out_ref[k * 32 + h * 16 : k * 32 + h * 16 + 16, :] = result[k * 16 : (k + 1) * 16]

    finish[0]()
    for one in own_late:
        one.wait()
    late.wait()
    links.phase()
    sums[0].farthest()
    sums[0].three()
    finish[1]()
    sums[1].farthest()
    sums[0].later(0)
    sums[1].three()
    sums[1].later(0)
    sums[0].later(1)
    sums[1].later(1)
    sums[0].later(2)
    sums[1].later(2)
    links.phase()
    activate(0)
    activate(1)
    links.phase()
    gather_step(0, 1)
    gather_step(1, 1)
    gather_step(0, 2)
    spread(0, 0)
    gather_step(1, 2)
    spread(1, 0)
    gather_step(0, 3)
    spread(0, 1)
    gather_step(1, 3)
    spread(1, 1)
    gather_step(0, 4)
    spread(0, 2)
    gather_step(1, 4)
    spread(1, 2)
    spread(0, 3)
    spread(1, 3)
    put(0)
    put(1)
    out_state.wait()
    links.drain()


def hand_over(out_tmp, state_tmp, out_ref, state_out, held_out, held_state, came, went):
    pieces = [(out_tmp, held_out, out_ref)]
    pieces += [(state_tmp.at[i], held_state.at[i], state_out.at[i]) for i in range(8)]
    coming = [pltpu.make_async_copy(a, b, came.at[i]) for i, (a, b, _) in enumerate(pieces)]
    going = [pltpu.make_async_copy(b, c, went.at[i]) for i, (_, b, c) in enumerate(pieces)]
    for one in coming:
        one.start()
    for one, two in zip(coming, going):
        one.wait()
        two.start()
    for two in going:
        two.wait()


def local(
    layer_input, seq_lengths, delta_state, attn_gain, w_query, w_key, w_value, w_outgate, w_write, w_forget,
    forget_rate, head_gain, w_out, mixer_gain, w_gate, w_up, w_down,
):
    vmem = pl.BlockSpec(memory_space=pltpu.VMEM)
    hbm = pl.BlockSpec(memory_space=pltpu.HBM)
    scratch = [
        ((NX, NTP * R, F), BF),
        ((4, F, 256), BF),
        ((NX * F, 256), BF),
        ((16, F), BF),
        ((NX, 16, F), BF),
        ((NZ, R, 256), F32),
        ((2, 2, R, 256), BF),
        ((2, 2, R, 256), BF),
        ((NZ, 8, R), F32),
        ((NZ, 8, R), F32),
        ((NX, 5, 32, 256), BF),
        ((5, R, 256), BF),
        ((R, R), F32),
        ((2, 32, 256), F32),
        ((32, 256), F32),
        ((32, 256), F32),
        ((32, 256), F32),
        ((32, 256), BF),
        ((NX, 256, F), BF),
        ((2, NZ, 16, 256), BF),
        ((2, NTP, 16, NX * F), BF),
        ((2, NTP, 16, NX * F), BF),
        ((2, 16, NX * F), BF),
        ((2, NTP, 64, NX * F), BF),
        ((2, NZ, 8, R), F32),
        ((2, NZ, 8, R), F32),
        ((NX * F, WIN), BF),
        ((NX * F, WIN), BF),
        ((NX, WIN, F), BF),
        ((2, NZ, 64, 2 * WIN), F32),
        ((2, 2, 4, 64, 2 * WIN), BF),
        ((2, 2, 4, 64, 2 * WIN), BF),
        ((2, NZ, 64, WIN), BF),
        ((2, NZ, 64, NX * F), F32),
        ((2, NZ, 64, NX * F), BF),
        ((2, NZ, 64, NX * F), BF),
        ((2, NY, NX, 64, F), BF),
        ((2, NX * NY, 64, F), BF),
    ]
    held = [
        pltpu.VMEM((R, F), BF),
        pltpu.SMEM((8,), jnp.int32),
        pltpu.VMEM(delta_state.shape, F32),
        pltpu.VMEM((32, F), BF),
        pltpu.VMEM((2, F), BF),
        pltpu.VMEM((2, F), BF),
        pltpu.SMEM((2,), F32),
        pltpu.VMEM((1, F), F32),
        pltpu.VMEM((32, F), BF),
    ]
    out_tmp, state_tmp = pl.pallas_call(
        body,
        out_shape=(
            jax.ShapeDtypeStruct((R, F), BF),
            jax.ShapeDtypeStruct(delta_state.shape, F32),
        ),
        in_specs=[
            hbm, hbm, hbm, hbm, hbm, hbm, hbm, hbm, hbm, hbm, hbm, hbm, hbm, hbm, hbm, hbm, hbm,
        ],
        out_specs=(vmem, hbm),
        scratch_shapes=[pltpu.VMEM(shape, dtype) for shape, dtype in scratch]
        + held
        + [
            pltpu.VMEM((16384, F), BF),
            pltpu.SemaphoreType.DMA((20,)),
            pltpu.SemaphoreType.DMA((NSEND,)),
            pltpu.SemaphoreType.DMA((NRECV,)),
        ],
        compiler_params=pltpu.CompilerParams(
            collective_id=0, has_side_effects=True, vmem_limit_bytes=VMEM_LIMIT
        ),
    )(
        layer_input, seq_lengths, delta_state, attn_gain.reshape(32, F), w_query, w_key, w_value, w_outgate,
        w_write.T, w_forget.T, forget_rate, head_gain.reshape(1, F), w_out, mixer_gain.reshape(32, F), w_gate, w_up,
        w_down,
    )
    return pl.pallas_call(
        hand_over,
        out_shape=(
            jax.ShapeDtypeStruct((R, F), BF),
            jax.ShapeDtypeStruct(delta_state.shape, F32),
        ),
        in_specs=[hbm, hbm],
        out_specs=(hbm, hbm),
        scratch_shapes=[
            pltpu.VMEM((R, F), BF),
            pltpu.VMEM(delta_state.shape, F32),
            pltpu.SemaphoreType.DMA((9,)),
            pltpu.SemaphoreType.DMA((9,)),
        ],
        compiler_params=pltpu.CompilerParams(vmem_limit_bytes=VMEM_LIMIT),
    )(out_tmp, state_tmp)


def solution(mesh):
    split = Mesh(mesh.devices.reshape(NZ, NX, NY, NC), ("z", "x", "y", "c"))
    kv, tp = ("z", "x"), ("y", "c")
    in_specs = (
        P(tp, kv), P(kv), P(kv, tp, None, None), P(), P(kv, tp), P(kv, tp), P(kv, tp), P(kv, tp), P(kv, tp),
        P(kv, tp), P(tp), P(), P(tp, kv), P(), P(kv, tp), P(kv, tp), P(tp, kv),
    )
    out_specs = (P(tp, kv), P(kv, tp, None, None))
    return jax.shard_map(local, mesh=split, in_specs=in_specs, out_specs=out_specs, check_vma=False)
```

```python
import math

import jax
import jax.numpy as jnp
from jax import lax
from jax.experimental import pallas as pl
from jax.experimental.pallas import tpu as pltpu
from jax.sharding import Mesh
from jax.sharding import PartitionSpec as P

D = 4096
NEW = 4
EPS = 1e-06
NZ, NX, NY, NC = 8, 4, 4, 2
NTP = NY * NC
R = 128
F = 128
WIN = 384
MESH = pl.DeviceIdType.MESH
BF = jnp.bfloat16
F32 = jnp.float32


def hops_of(d):
    return min(d[0], NX - d[0]) + min(d[1], NY - d[1])


PLANE = sorted(((dx, dy) for dx in range(NX) for dy in range(NY) if dx or dy), key=hops_of)
STRAIGHT = (False, False)
NRECV = 88 - 2 * sum(STRAIGHT)
NSEND = 10
VMEM_LIMIT = 58 * 1024 * 1024


def silu(a):
    return a * jax.nn.sigmoid(a)


def rows_of(k):
    return pl.ds(pl.multiple_of(k * R, R), R)


def dot_t(a, b):
    return lax.dot_general(a, b, (((1,), (1,)), ((), ())), preferred_element_type=F32)


class Gate:
    def __init__(self, links):
        self.links, self.index, self.size = links, links.fresh(), 0

    def wait(self):
        self.links.wait_bytes(self.links.recv.at[self.index], self.size)


class Links:
    def __init__(self, send, recv, ruler):
        self.send, self.recv, self.ruler, self.n, self.sent = send, recv, ruler, 0, []
        self.z, self.x = lax.axis_index("z"), lax.axis_index("x")
        self.y, self.c = lax.axis_index("y"), lax.axis_index("c")

    def fresh(self):
        self.n += 1
        return self.n - 1

    def phase(self):
        self.sent.append(0)

    def copy(self, src, dst, dz=0, dx=0, dy=0, dc=0, gate=None):
        to = (
            lax.rem(self.z + dz, NZ),
            lax.rem(self.x + dx, NX),
            lax.rem(self.y + dy, NY),
            lax.rem(self.c + dc, NC),
        )
        return self.copy_to(src, dst, to, gate)

    def copy_to(self, src, dst, to, gate=None, index=None):
        size = math.prod(src.shape) * jnp.dtype(src.dtype).itemsize
        self.sent[-1] += size
        if gate is not None:
            gate.size += size
            index = gate.index
        elif index is None:
            index = self.fresh()
        made = pltpu.make_async_remote_copy(
            src_ref=src,
            dst_ref=dst,
            send_sem=self.send.at[len(self.sent) - 1],
            recv_sem=self.recv.at[index],
            device_id=to,
            device_id_type=MESH,
        )
        made.start()
        return made

    def wait_bytes(self, sem, size):
        part = self.ruler.at[pl.ds(0, size // (2 * F))]
        pltpu.make_async_copy(part, part, sem).wait()

    def drain(self):
        for i, size in enumerate(self.sent):
            self.wait_bytes(self.send.at[i], size)
        assert self.n == NRECV and len(self.sent) == NSEND, (self.n, len(self.sent))


def greet(links):
    z, x, y, c = links.z, links.x, links.y, links.c
    barrier = pltpu.get_barrier_semaphore()
    to = [(dz, 0, 0, 0) for dz in (4, 3, 5)]
    to += [(dz, dx, 0, 0) for dz in (2, NZ - 2, 1, NZ - 1, 0) for dx in range(NX) if dz or dx]
    to += [(0, dx, dy, 0) for dx in range(NX) for dy in range(1, NY)]
    to += [(0, 0, dy, 1) for dy in range(NY)]
    for dz, dx, dy, dc in to:
        pl.semaphore_signal(
            barrier,
            inc=1,
            device_id=(lax.rem(z + dz, NZ), lax.rem(x + dx, NX), lax.rem(y + dy, NY), lax.rem(c + dc, NC)),
            device_id_type=MESH,
        )
    return lambda: pl.semaphore_wait(barrier, len(to))


def gather_x_first(links, src, buf):
    z, x, y, c = links.z, links.x, links.y, links.c
    along_x = {dx: links.copy(src, buf.at[x, rows_of(y * NC + c)], dx=dx) for dx in (1, 3, 2)}
    along_y = {}
    for dy in (1, 3, 2):
        along_y[0, dy] = links.copy(src, buf.at[x, rows_of(y * NC + c)], dy=dy)
    forward = Gate(links)
    links.copy(src, buf.at[x, rows_of(y * NC + c)], dc=1, gate=forward)

    def finish():
        def block(dx, dy):
            return buf.at[lax.rem(x - dx + NX, NX), rows_of(lax.rem(y - dy + NY, NY) * NC + c)]

        for dx in (1, 3, 2):
            along_x[dx].wait_recv()
            for dy in (1, 3, 2):
                along_y[dx, dy] = links.copy(block(dx, 0), block(dx, 0), dy=dy)
            links.copy(block(dx, 0), block(dx, 0), dc=1, gate=forward)
        for dx in (0, 1, 3, 2):
            for dy in (1, 3, 2):
                along_y[dx, dy].wait_recv()
                links.copy(block(dx, dy), block(dx, dy), dc=1, gate=forward)
        forward.wait()

    return finish


def gather_straight(links, src, buf, rows):
    x, y, c = links.x, links.y, links.c

    def block(xs, ys):
        return buf.at[ys * NC + c, pl.ds(pl.multiple_of(xs * rows, rows), rows)]

    straight = {hops: Gate(links) for hops in range(1, 5)}
    for d in reversed(PLANE):
        links.copy(src, block(x, y), dx=d[0], dy=d[1], gate=straight[hops_of(d)])
    forward = Gate(links)
    links.copy(src, block(x, y), dc=1, gate=forward)

    def finish():
        for hops, gate in straight.items():
            gate.wait()
            for dx, dy in (d for d in PLANE if hops_of(d) == hops):
                came = block(lax.rem(x - dx + NX, NX), lax.rem(y - dy + NY, NY))
                links.copy(came, came, dc=1, gate=forward)
        forward.wait()

    return finish


FAR, THREE, TWO, ONE = range(4)


class RingSum:
    def __init__(self, links, block, sendbuf, recvbuf, width, straight):
        self.links, self.block, self.sendbuf, self.recvbuf = links, block, sendbuf, recvbuf
        self.half, self.made, self.straight = width // 2, {}, straight

    def lanes(self, side):
        return slice(None) if side is None else slice(side * self.half, (side + 1) * self.half)

    def add(self, value, way, kind, side, lanes):
        self.made[way, kind, side].wait_recv()
        return value + self.recvbuf[way, kind, :, lanes].astype(F32)

    def send(self, way, kind, side=None):
        lanes = self.lanes(side)
        value = self.block(4 - kind if way == 0 else 4 + kind)[:, lanes]
        if kind == THREE and side == way:
            value = self.add(value, way, FAR, side, lanes)
        elif kind == TWO and self.straight:
            parts = [value[:, : self.half], value[:, self.half :]]
            parts[way] = self.add(parts[way], way, FAR, way, self.lanes(way))
            value = self.add(jnp.concatenate(parts, axis=1), way, THREE, None, lanes)
        elif kind == TWO:
            self.made[way, THREE, 1 - way].wait_recv()
            value = self.add(value, way, THREE, way, lanes)
        elif kind == ONE:
            value = self.add(value, way, TWO, None, lanes)
        self.sendbuf[way, kind, :, lanes] = value.astype(BF)
        at = (way, kind) if side is None else (way, kind, slice(None), pl.ds(side * self.half, self.half))
        hops = 2 if kind == FAR and self.straight else 1
        self.made[way, kind, side] = self.links.copy(
            self.sendbuf.at[at], self.recvbuf.at[at], dz=hops if way == 0 else NZ - hops
        )

    def farthest(self):
        for way in (0, 1):
            self.send(way, FAR, way)

    def three(self):
        for way in (0, 1):
            self.send(way, THREE, None if self.straight else 1 - way)

    def later(self, number):
        if number or not self.straight:
            for way in (0, 1):
                self.send(way, *((THREE, way), (TWO, None), (ONE, None))[number])

    def total(self):
        value = self.block(0)
        for way in (0, 1):
            value = self.add(value, way, ONE, None, slice(None))
        return value


class RingGather:
    def __init__(self, links, buf, rows):
        self.links, self.buf, self.rows, self.going = links, buf, rows // 2, {}

    def step(self, step):
        for way in (0, 1):
            if step:
                self.going[way, step].wait_recv()
            at = lax.rem(self.links.z + (NZ - step if way == 0 else step), NZ)
            if step == 2:
                half = self.buf.at[at, pl.ds(way * self.rows, self.rows)]
                self.going[way, 4] = self.links.copy(half, half, dz=2 if way == 0 else NZ - 2)
            if step < 3:
                self.going[way, step + 1] = self.links.copy(
                    self.buf.at[at], self.buf.at[at], dz=1 if way == 0 else NZ - 1
                )

    def finish(self):
        for way in (0, 1):
            self.going[way, 4].wait_recv()


def square_rows(wide):
    squares = wide * wide
    squares = squares[:, :F] + squares[:, F : 2 * F] + squares[:, 2 * F : 3 * F] + squares[:, 3 * F :]
    if wide.shape[0] < R:
        squares = jnp.concatenate([squares, jnp.zeros((R - wide.shape[0], F), F32)], axis=0)
    ones = jnp.ones((16, F), BF)
    high = squares.astype(BF)
    low = (squares - high.astype(F32)).astype(BF)
    return (dot_t(ones, high) + dot_t(ones, low))[:8]


def stats_total(own, got, gate):
    gate.wait()
    total = own
    for offset in range(1, NZ):
        total = total + got[offset]
    return jnp.concatenate([total, jnp.zeros((R - 8, R), F32)], axis=0).T


def body(
    x_hbm, len_hbm, state_hbm, gain1_hbm, wq, wk, wv, wo, write_hbm, forget_hbm, rate_hbm, head_gain_hbm, w_out,
    gain2_hbm, w_gate, w_up, w_down,
    out_ref, next_hbm,
    xbuf, w4, wr, rate_w, rw, p1, s1, r1, stats1, got1, pre, last1, cols, on_first, updates, decays, readings, mixed_own, wz, mz, obuf, orecv,
    hown, hb, stats2, got2, wg, wu, wd, p2, s2, r2, abuf, part, psend, precv, fsend, frecv,
    x_ref, len_ref, state_ref, gain1_ref, write_ref, forget_ref, rate_ref, head_gain_ref, gain2_ref,
    ruler, local, send, recv,
):
    links = Links(send, recv, ruler)
    links.phase()
    arrive = greet(links)
    z, x, y, c = links.z, links.x, links.y, links.c
    tp = y * NC + c

    locals_ = [pltpu.make_async_copy(w, w4.at[i], local.at[i]) for i, w in enumerate((wq, wk, wv, wo))]

    def window(at):
        return pl.ds(pl.multiple_of((at * 3 - at // (NX - 1)) * F, F), WIN)

    feats = pl.ds(pl.multiple_of(x * F, F), F)
    given = [
        pltpu.make_async_copy(far, near, local.at[11 + i])
        for i, (far, near) in enumerate(
            (
                (x_hbm, x_ref), (write_hbm, write_ref), (forget_hbm, forget_ref), (gain1_hbm, gain1_ref),
                (gain2_hbm, gain2_ref), (len_hbm, len_ref), (rate_hbm, rate_ref), (head_gain_hbm, head_gain_ref),
                (state_hbm, state_ref),
            )
        )
    ]
    for one in given:
        one.start()
    own_x = pltpu.make_async_copy(x_hbm, xbuf.at[x, rows_of(tp)], local.at[4])
    own_out = pltpu.make_async_copy(w_out, wz.at[x], local.at[5])
    own_late = [
        pltpu.make_async_copy(w_gate.at[:, window(x)], wg.at[feats], local.at[6]),
        pltpu.make_async_copy(w_up.at[:, window(x)], wu.at[feats], local.at[7]),
        pltpu.make_async_copy(w_down.at[window(x)], wd.at[x], local.at[8]),
    ]
    for one in locals_ + [own_x, own_out] + own_late:
        one.start()
    arrive()

    given[0].wait()
    finish = gather_x_first(links, x_ref, xbuf)
    for one in given[1:8]:
        one.wait()
    small = [write_ref[...].astype(F32), forget_ref[...].astype(F32), jnp.zeros((12, F), F32)]
    rate_w[...] = jnp.concatenate(small, axis=0).astype(BF)
    rw[x] = rate_w[...]
    for one in locals_:
        one.wait()
    own_w = pltpu.make_async_copy(w4.at[x], wr.at[feats], local.at[9])
    own_w.start()
    early, early_rates, late, outs = Gate(links), Gate(links), Gate(links), Gate(links)
    for dx in (1, 3, 2):
        to = lax.rem(x + dx, NX)
        links.copy(w4.at[to], wr.at[feats], dx=dx, gate=early)
        links.copy(rate_w, rw.at[x], dx=dx, gate=early_rates)
    links.phase()
    for dx in (1, 3, 2):
        links.copy(w_out, wz.at[x], dx=dx, gate=outs)
    for dx in (1, 3, 2):
        to = lax.rem(x + dx, NX)
        links.copy(w_gate.at[:, window(to)], wg.at[feats], dx=dx, gate=late)
        links.copy(w_up.at[:, window(to)], wu.at[feats], dx=dx, gate=late)
    links.phase()

    which = lax.broadcasted_iota(jnp.int32, (32, F), 0)

    def gain_of(ref):
        wide = ref[...].astype(F32)
        return jnp.concatenate(
            [jnp.sum(jnp.where(which == z * NX + k, wide, 0.0), axis=0, keepdims=True) for k in range(NX)], axis=1
        )

    gain1, gain2 = gain_of(gain1_ref), gain_of(gain2_ref)
    own_x.wait()
    own_w.wait()
    finish()
    early.wait()
    early_rates.wait()
    links.phase()

    sub = lax.broadcasted_iota(jnp.int32, (8, R), 0)
    stats_gate, ready = Gate(links), {}

    def projected(offset):
        if offset not in ready:
            ready[offset] = True
            at = rows_of(lax.rem(z + offset, NZ))
            wide = jnp.concatenate([xbuf[k, at, :] for k in range(NX)], axis=1).astype(F32)
            normed = (wide * gain1).astype(BF)
            p1[offset] = jnp.dot(normed, wr[...], preferred_element_type=F32)
            stat = jnp.where(sub == 4, square_rows(wide), 0.0)
            for k in range(NX):
                stat = stat + dot_t(rw[k], normed[:, k * F : (k + 1) * F])[:8]
            stats1[offset] = stat
            if offset:
                links.copy(stats1.at[offset], got1.at[offset], dz=offset, gate=stats_gate)
        return p1[offset]

    def part_of(at):
        return pl.ds(pl.multiple_of(at * 32, 32), 32)

    near = {}
    for way in (0, 1):
        side = pl.ds(way * F, F)
        s1[way, 0, :, way * F : (way + 1) * F] = projected(4)[:, way * F : (way + 1) * F].astype(BF)
        near[way, 0] = links.copy(s1.at[way, 0, :, side], r1.at[way, 0, :, side], dz=2 if way == 0 else NZ - 2)
    for way in (0, 1):
        s1[way, 1] = projected(3 if way == 0 else 5).astype(BF)
        near[way, 1] = links.copy(s1.at[way, 1], r1.at[way, 1], dz=1 if way == 0 else NZ - 1)
    pre_gate = Gate(links)

    def to_owners(slot, value, dz):
        last1[slot] = value.astype(BF)
        for dx in (2, 1, 3, 0):
            if dx or dz:
                links.copy(last1.at[slot, part_of(lax.rem(x + dx, NX))], pre.at[x, slot], dz=dz, dx=dx, gate=pre_gate)

    to_owners(1, projected(1), 1)
    to_owners(2, projected(7), NZ - 1)
    to_owners(0, projected(0), 0)
    for way in (0, 1):
        value = projected(2 if way == 0 else 6)
        near[way, 0].wait_recv()
        near[way, 1].wait_recv()
        half = value[:, way * F : (way + 1) * F] + r1[way, 0, :, way * F : (way + 1) * F].astype(F32)
        halves = [half, value[:, F:]] if way == 0 else [value[:, :F], half]
        to_owners(3 + way, jnp.concatenate(halves, axis=1) + r1[way, 1].astype(F32), 2 if way == 0 else NZ - 2)
    quarter = part_of(x)
    pre[x, 0] = last1[0, quarter, :]
    cols[...] = stats_total(stats1[0], got1, stats_gate)
    stat = cols[quarter, :]
    scale = lax.rsqrt(stat[:, 4:5] / D + EPS)
    lane = lax.broadcasted_iota(jnp.int32, (32, R), 1)
    row = lax.broadcasted_iota(jnp.int32, (32, R), 0)
    live = jnp.zeros((32, R), F32)
    for s in range(8):
        inside = (row // NEW == s) & (lax.rem(row, NEW) < len_ref[s])
        live = live + jnp.where(inside, 1.0, 0.0)
    rated = stat * scale
    beta = jax.nn.sigmoid(rated) * live
    rate = jnp.where(lane == 2, rate_ref[0], jnp.where(lane == 3, rate_ref[1], 0.0))
    softplus = jnp.maximum(rated, 0.0) + jnp.log1p(jnp.exp(-jnp.abs(rated)))
    keep = jnp.exp(-rate * softplus * live)
    pre_gate.wait()
    links.phase()

    def summed(i):
        return sum(pre[i, k].astype(F32) for k in range(5)) * scale

    given[8].wait()
    for dx in (1, 3, 2):
        to = lax.rem(x + dx, NX)
        links.copy(w_down.at[window(to)], wd.at[x], dx=dx, gate=late)
    query, key, value, gate = (silu(summed(i)) for i in range(4))

    def unit(a):
        return a * lax.rsqrt(jnp.sum(a * a, axis=1, keepdims=True) + EPS)

    stacked = []
    for h in range(2):
        at = slice(h * F, (h + 1) * F)
        stacked += [unit(query[:, at]) * F ** (-0.5), unit(key[:, at])]
    upper = lax.broadcasted_iota(jnp.int32, (8, F), 0) < NEW
    for pair in range(4):
        near8 = slice(pair * 8, pair * 8 + 8)
        for h in range(2):
            both = jnp.concatenate([stacked[2 * h][near8], stacked[2 * h + 1][near8]], axis=0)
            one, two = (
                jnp.dot(both, state_ref[2 * pair + i, h], precision=lax.Precision.HIGHEST, preferred_element_type=F32)
                for i in range(2)
            )
            for k in range(2):
                half = slice(k * 8, k * 8 + 8)
                on_first[k, near8, h * F : (h + 1) * F] = jnp.where(upper, one[half], two[half])
    position = lax.rem(row, NEW)

    def later_by(a, n):
        return jnp.concatenate([a[32 - n :], a[: 32 - n]], axis=0)

    def sooner_by(a, n):
        return jnp.concatenate([a[n:], a[:n]], axis=0)

    for h in range(2):
        at = slice(h * F, (h + 1) * F)
        q_now, k_now, v_now = stacked[2 * h], stacked[2 * h + 1], value[:, at]
        write = jnp.broadcast_to(beta[:, h : h + 1], (32, F))
        hold = jnp.broadcast_to(keep[:, 2 + h : 3 + h], (32, F))
        over1 = hold
        over2 = over1 * later_by(hold, 1)
        over3 = over2 * later_by(hold, 2)
        over4 = over3 * later_by(hold, 3)
        whole = jnp.where(position == 0, over1, jnp.where(position == 1, over2, jnp.where(position == 2, over3, over4)))
        alone = write * (v_now - whole * on_first[1, :, at])
        among_k, among_q = [], [jnp.sum(q_now * k_now, axis=1, keepdims=True)]
        for n, over_n in ((1, over1), (2, over2), (3, over3)):
            k_then = later_by(k_now, n)
            inside = jnp.where(position >= n, over_n, 0.0)
            among_k.append(write * inside * jnp.sum(k_now * k_then, axis=1, keepdims=True))
            among_q.append(inside * jnp.sum(q_now * k_then, axis=1, keepdims=True))
        update = alone
        for _ in range(NEW - 1):
            update = alone - sum(among_k[n - 1] * later_by(update, n) for n in (1, 2, 3))
        reading = whole * on_first[0, :, at] + among_q[0] * update
        for n in (1, 2, 3):
            reading = reading + among_q[n] * later_by(update, n)
        readings[:, at] = reading
        ahead1 = sooner_by(hold, 1)
        ahead2 = ahead1 * sooner_by(hold, 2)
        ahead3 = ahead2 * sooner_by(hold, 3)
        rest = jnp.where(position == 3, 1.0, jnp.where(position == 2, ahead1, jnp.where(position == 1, ahead2, ahead3)))
        updates[:, at] = rest * update
        decays[:, at] = whole
    for h in range(2):
        at = slice(h * F, (h + 1) * F)
        read = readings[:, at] * live
        normed = read * lax.rsqrt(jnp.mean(read * read, axis=1, keepdims=True) + EPS)
        mixed_own[:, at] = (normed * head_gain_ref[...] * gate[:, at]).astype(BF)

    mixed_gates = [Gate(links), Gate(links)]
    for h in range(2):
        mz[h, z] = mixed_own[h * 16 : h * 16 + 16, :]
        for dz in (4, 3, 5, 2, 6, 1, 7):
            links.copy(mixed_own.at[pl.ds(h * 16, 16)], mz.at[h, z], dz=dz, gate=mixed_gates[h])
    turned = jnp.concatenate(stacked, axis=0).T
    for s in range(8):
        for h in range(2):
            at = slice(h * F, (h + 1) * F)
            state = decays[s * NEW + NEW - 1 : (s + 1) * NEW, at] * state_ref[s, h]
            for r in range(s * NEW, (s + 1) * NEW):
                state = state + turned[:, h * 64 + 32 + r : h * 64 + 33 + r] * updates[r : r + 1, at]
            state_ref[s, h] = state
    out_state = pltpu.make_async_copy(state_ref, next_hbm, local.at[10])
    out_state.start()
    own_out.wait()
    outs.wait()
    tp_gates = [Gate(links), Gate(links)]
    for h in range(2):
        mixed_gates[h].wait()
        heads = jnp.concatenate([mz[h, k] for k in range(NZ)], axis=0)
        for k in range(NX):
            terms = jnp.dot(heads, wz[k], preferred_element_type=F32).astype(BF)
            for b in range(NTP):
                obuf[h, b, :, k * F : (k + 1) * F] = terms[b * 16 : b * 16 + 16]
        for k in (4, 3, 5, 2, 6, 1, 7):
            to = lax.rem(tp + k, NTP)
            links.copy_to(obuf.at[h, to], orecv.at[h, k], (z, x, to // NC, lax.rem(to, NC)), tp_gates[h])

    finish = []
    for h in range(2):
        attended = obuf[h, tp].astype(F32)
        links.phase()
        tp_gates[h].wait()
        for k in range(1, NTP):
            attended = attended + orecv[h, k].astype(F32)
        at = pl.ds(pl.multiple_of(tp * R + x * 32 + h * 16, 16), 16)
        given = jnp.concatenate([xbuf[k, at, :] for k in range(NX)], axis=1).astype(F32)
        hown[h] = (given + attended).astype(BF)
        hb[h, tp, pl.ds(pl.multiple_of(x * 16, 16), 16), :] = hown[h]
        finish.append(gather_straight(links, hown.at[h], hb.at[h], 16))

    stats_gates, ready2 = (Gate(links), Gate(links)), ({}, {})

    def mixer(h):
        def block(offset):
            if offset not in ready2[h]:
                ready2[h][offset] = True
                wide = hb[h, lax.rem(z + offset, NZ)].astype(F32)
                normed = (wide * gain2).astype(BF)
                p2[h, offset, :, :WIN] = jnp.dot(normed, wg[...], preferred_element_type=F32)
                p2[h, offset, :, WIN:] = jnp.dot(normed, wu[...], preferred_element_type=F32)
                stats2[h, offset] = square_rows(wide)
                if offset:
                    links.copy(stats2.at[h, offset], got2.at[h, offset], dz=offset, gate=stats_gates[h])
            return p2[h, offset]

        return RingSum(links, block, s2.at[h], r2.at[h], 2 * WIN, STRAIGHT[h])

    sums = [mixer(h) for h in range(2)]
    gathers = [RingGather(links, abuf.at[h], 64) for h in range(2)]
    odd = lax.rem(z + c, 2)
    partner = (z, x, y, 1 - c)

    def activate(h):
        total = sums[h].total()
        scale2 = lax.rsqrt(stats_total(stats2[h, 0], got2.at[h], stats_gates[h])[:64, 0:1] / D + EPS)
        activated = silu(scale2 * total[:, :WIN]) * (scale2 * total[:, WIN:])
        again = (lax.broadcasted_iota(jnp.int32, (64, WIN), 1) < F) & (x == NX - 1)
        abuf[h, z] = jnp.where(again, 0.0, activated).astype(BF)
        gathers[h].step(0)
        down(h, 0)

    def down(h, offset):
        block = abuf[h, lax.rem(z + offset, NZ)]
        for k in range(NX):
            part[h, offset, :, k * F : (k + 1) * F] = jnp.dot(block, wd[k], preferred_element_type=F32)

    turns = (0, 6, 2, 4)
    over = {(h, base): links.fresh() for h in range(2) for base in turns}

    def give(h, base):
        at = base + 1 - odd
        psend[h, at] = part[h, at].astype(BF)
        over_made[h, base] = links.copy_to(psend.at[h, at], precv.at[h, at], partner, index=over[h, base])

    over_made = {}

    def gather_step(h, step):
        gathers[h].step(step) if step < 4 else gathers[h].finish()
        if step < 4:
            down(h, NZ - step)
            down(h, step)
        else:
            down(h, 4)
        give(h, turns[step - 1])

    last_gates = [Gate(links), Gate(links)]

    def spread(h, turn):
        at = turns[turn] + odd
        over_made[h, turns[turn]].wait_recv()
        both = (part[h, at] + precv[h, at].astype(F32)).astype(BF)
        for k in range(NX):
            fsend[h, turn, k] = both[:, k * F : (k + 1) * F]
        to = lax.rem(z + at, NZ) // NC
        for dx in (2, 1, 3):
            xd = lax.rem(x + dx, NX)
            links.copy_to(fsend.at[h, turn, xd], frecv.at[h, y * NX + x], (z, xd, to, c), last_gates[h])

        @pl.when(to != y)
        def _():
            links.copy_to(fsend.at[h, turn, x], frecv.at[h, y * NX + x], (z, x, to, c), last_gates[h])

        @pl.when(to == y)
        def _():
            frecv[h, y * NX + x] = fsend[h, turn, x]

        if turn == 3:
            links.sent[-1] -= 2 * 64 * F
            last_gates[h].size -= 2 * 64 * F

    def put(h):
        result = hb[h, tp, :, feats].astype(F32)
        last_gates[h].wait()
        for i in range(NX * NY):
            result = result + frecv[h, i].astype(F32)
        result = result.astype(BF)
        for k in range(NX):
            out_ref[k * 32 + h * 16 : k * 32 + h * 16 + 16, :] = result[k * 16 : (k + 1) * 16]

    finish[0]()
    for one in own_late:
        one.wait()
    late.wait()
    links.phase()
    sums[0].farthest()
    sums[0].three()
    finish[1]()
    sums[1].farthest()
    sums[0].later(0)
    sums[1].three()
    sums[1].later(0)
    sums[0].later(1)
    sums[1].later(1)
    sums[0].later(2)
    sums[1].later(2)
    links.phase()
    activate(0)
    activate(1)
    links.phase()
    gather_step(0, 1)
    gather_step(1, 1)
    gather_step(0, 2)
    spread(0, 0)
    gather_step(1, 2)
    spread(1, 0)
    gather_step(0, 3)
    spread(0, 1)
    gather_step(1, 3)
    spread(1, 1)
    gather_step(0, 4)
    spread(0, 2)
    gather_step(1, 4)
    spread(1, 2)
    spread(0, 3)
    spread(1, 3)
    put(0)
    put(1)
    out_state.wait()
    links.drain()


def hand_over(out_tmp, state_tmp, out_ref, state_out, held_out, held_state, came, went):
    pieces = [(out_tmp, held_out, out_ref)]
    pieces += [(state_tmp.at[i], held_state.at[i], state_out.at[i]) for i in range(8)]
    coming = [pltpu.make_async_copy(a, b, came.at[i]) for i, (a, b, _) in enumerate(pieces)]
    going = [pltpu.make_async_copy(b, c, went.at[i]) for i, (_, b, c) in enumerate(pieces)]
    for one in coming:
        one.start()
    for one, two in zip(coming, going):
        one.wait()
        two.start()
    for two in going:
        two.wait()


def local(
    layer_input, seq_lengths, delta_state, attn_gain, w_query, w_key, w_value, w_outgate, w_write, w_forget,
    forget_rate, head_gain, w_out, mixer_gain, w_gate, w_up, w_down,
):
    vmem = pl.BlockSpec(memory_space=pltpu.VMEM)
    hbm = pl.BlockSpec(memory_space=pltpu.HBM)
    scratch = [
        ((NX, NTP * R, F), BF),
        ((4, F, 256), BF),
        ((NX * F, 256), BF),
        ((16, F), BF),
        ((NX, 16, F), BF),
        ((NZ, R, 256), F32),
        ((2, 2, R, 256), BF),
        ((2, 2, R, 256), BF),
        ((NZ, 8, R), F32),
        ((NZ, 8, R), F32),
        ((NX, 5, 32, 256), BF),
        ((5, R, 256), BF),
        ((R, R), F32),
        ((2, 32, 256), F32),
        ((32, 256), F32),
        ((32, 256), F32),
        ((32, 256), F32),
        ((32, 256), BF),
        ((NX, 256, F), BF),
        ((2, NZ, 16, 256), BF),
        ((2, NTP, 16, NX * F), BF),
        ((2, NTP, 16, NX * F), BF),
        ((2, 16, NX * F), BF),
        ((2, NTP, 64, NX * F), BF),
        ((2, NZ, 8, R), F32),
        ((2, NZ, 8, R), F32),
        ((NX * F, WIN), BF),
        ((NX * F, WIN), BF),
        ((NX, WIN, F), BF),
        ((2, NZ, 64, 2 * WIN), F32),
        ((2, 2, 4, 64, 2 * WIN), BF),
        ((2, 2, 4, 64, 2 * WIN), BF),
        ((2, NZ, 64, WIN), BF),
        ((2, NZ, 64, NX * F), F32),
        ((2, NZ, 64, NX * F), BF),
        ((2, NZ, 64, NX * F), BF),
        ((2, NY, NX, 64, F), BF),
        ((2, NX * NY, 64, F), BF),
    ]
    held = [
        pltpu.VMEM((R, F), BF),
        pltpu.SMEM((8,), jnp.int32),
        pltpu.VMEM(delta_state.shape, F32),
        pltpu.VMEM((32, F), BF),
        pltpu.VMEM((2, F), BF),
        pltpu.VMEM((2, F), BF),
        pltpu.SMEM((2,), F32),
        pltpu.VMEM((1, F), F32),
        pltpu.VMEM((32, F), BF),
    ]
    out_tmp, state_tmp = pl.pallas_call(
        body,
        out_shape=(
            jax.ShapeDtypeStruct((R, F), BF),
            jax.ShapeDtypeStruct(delta_state.shape, F32),
        ),
        in_specs=[
            hbm, hbm, hbm, hbm, hbm, hbm, hbm, hbm, hbm, hbm, hbm, hbm, hbm, hbm, hbm, hbm, hbm,
        ],
        out_specs=(vmem, hbm),
        scratch_shapes=[pltpu.VMEM(shape, dtype) for shape, dtype in scratch]
        + held
        + [
            pltpu.VMEM((16384, F), BF),
            pltpu.SemaphoreType.DMA((20,)),
            pltpu.SemaphoreType.DMA((NSEND,)),
            pltpu.SemaphoreType.DMA((NRECV,)),
        ],
        compiler_params=pltpu.CompilerParams(
            collective_id=0, has_side_effects=True, vmem_limit_bytes=VMEM_LIMIT
        ),
    )(
        layer_input, seq_lengths, delta_state, attn_gain.reshape(32, F), w_query, w_key, w_value, w_outgate,
        w_write.T, w_forget.T, forget_rate, head_gain.reshape(1, F), w_out, mixer_gain.reshape(32, F), w_gate, w_up,
        w_down,
    )
    return pl.pallas_call(
        hand_over,
        out_shape=(
            jax.ShapeDtypeStruct((R, F), BF),
            jax.ShapeDtypeStruct(delta_state.shape, F32),
        ),
        in_specs=[hbm, hbm],
        out_specs=(hbm, hbm),
        scratch_shapes=[
            pltpu.VMEM((R, F), BF),
            pltpu.VMEM(delta_state.shape, F32),
            pltpu.SemaphoreType.DMA((9,)),
            pltpu.SemaphoreType.DMA((9,)),
        ],
        compiler_params=pltpu.CompilerParams(vmem_limit_bytes=VMEM_LIMIT),
    )(out_tmp, state_tmp)


def solution(mesh):
    split = Mesh(mesh.devices.reshape(NZ, NX, NY, NC), ("z", "x", "y", "c"))
    kv, tp = ("z", "x"), ("y", "c")
    in_specs = (
        P(tp, kv), P(kv), P(kv, tp, None, None), P(), P(kv, tp), P(kv, tp), P(kv, tp), P(kv, tp), P(kv, tp),
        P(kv, tp), P(tp), P(), P(tp, kv), P(), P(kv, tp), P(kv, tp), P(tp, kv),
    )
    out_specs = (P(tp, kv), P(kv, tp, None, None))
    return jax.shard_map(local, mesh=split, in_specs=in_specs, out_specs=out_specs, check_vma=False)
```

```python
import math

import jax
import jax.numpy as jnp
from jax import lax
from jax.experimental import pallas as pl
from jax.experimental.pallas import tpu as pltpu
from jax.sharding import Mesh
from jax.sharding import PartitionSpec as P

D = 4096
NEW = 4
EPS = 1e-06
NZ, NX, NY, NC = 8, 4, 4, 2
NTP = NY * NC
R = 128
F = 128
WIN = 384
MESH = pl.DeviceIdType.MESH
BF = jnp.bfloat16
F32 = jnp.float32


def hops_of(d):
    return min(d[0], NX - d[0]) + min(d[1], NY - d[1])


PLANE = sorted(((dx, dy) for dx in range(NX) for dy in range(NY) if dx or dy), key=hops_of)
STRAIGHT = (False, False)
NRECV = 88 - 2 * sum(STRAIGHT)
NSEND = 10
VMEM_LIMIT = 58 * 1024 * 1024


def silu(a):
    return a * jax.nn.sigmoid(a)


def rows_of(k):
    return pl.ds(pl.multiple_of(k * R, R), R)


def dot_t(a, b):
    return lax.dot_general(a, b, (((1,), (1,)), ((), ())), preferred_element_type=F32)


class Gate:
    def __init__(self, links):
        self.links, self.index, self.size = links, links.fresh(), 0

    def wait(self):
        self.links.wait_bytes(self.links.recv.at[self.index], self.size)


class Links:
    def __init__(self, send, recv, ruler):
        self.send, self.recv, self.ruler, self.n, self.sent = send, recv, ruler, 0, []
        self.z, self.x = lax.axis_index("z"), lax.axis_index("x")
        self.y, self.c = lax.axis_index("y"), lax.axis_index("c")

    def fresh(self):
        self.n += 1
        return self.n - 1

    def phase(self):
        self.sent.append(0)

    def copy(self, src, dst, dz=0, dx=0, dy=0, dc=0, gate=None):
        to = (
            lax.rem(self.z + dz, NZ),
            lax.rem(self.x + dx, NX),
            lax.rem(self.y + dy, NY),
            lax.rem(self.c + dc, NC),
        )
        return self.copy_to(src, dst, to, gate)

    def copy_to(self, src, dst, to, gate=None, index=None):
        size = math.prod(src.shape) * jnp.dtype(src.dtype).itemsize
        self.sent[-1] += size
        if gate is not None:
            gate.size += size
            index = gate.index
        elif index is None:
            index = self.fresh()
        made = pltpu.make_async_remote_copy(
            src_ref=src,
            dst_ref=dst,
            send_sem=self.send.at[len(self.sent) - 1],
            recv_sem=self.recv.at[index],
            device_id=to,
            device_id_type=MESH,
        )
        made.start()
        return made

    def wait_bytes(self, sem, size):
        part = self.ruler.at[pl.ds(0, size // (2 * F))]
        pltpu.make_async_copy(part, part, sem).wait()

    def drain(self):
        for i, size in enumerate(self.sent):
            self.wait_bytes(self.send.at[i], size)
        assert self.n == NRECV and len(self.sent) == NSEND, (self.n, len(self.sent))


def greet(links):
    z, x, y, c = links.z, links.x, links.y, links.c
    barrier = pltpu.get_barrier_semaphore()
    to = [(dz, 0, 0, 0) for dz in (4, 3, 5)]
    to += [(dz, dx, 0, 0) for dz in (2, NZ - 2, 1, NZ - 1, 0) for dx in range(NX) if dz or dx]
    to += [(0, dx, dy, 0) for dx in range(NX) for dy in range(1, NY)]
    to += [(0, 0, dy, 1) for dy in range(NY)]
    for dz, dx, dy, dc in to:
        pl.semaphore_signal(
            barrier,
            inc=1,
            device_id=(lax.rem(z + dz, NZ), lax.rem(x + dx, NX), lax.rem(y + dy, NY), lax.rem(c + dc, NC)),
            device_id_type=MESH,
        )
    return lambda: pl.semaphore_wait(barrier, len(to))


def gather_x_first(links, src, buf):
    z, x, y, c = links.z, links.x, links.y, links.c
    along_x = {dx: links.copy(src, buf.at[x, rows_of(y * NC + c)], dx=dx) for dx in (1, 3, 2)}
    along_y = {}
    for dy in (1, 3, 2):
        along_y[0, dy] = links.copy(src, buf.at[x, rows_of(y * NC + c)], dy=dy)
    forward = Gate(links)
    links.copy(src, buf.at[x, rows_of(y * NC + c)], dc=1, gate=forward)

    def finish():
        def block(dx, dy):
            return buf.at[lax.rem(x - dx + NX, NX), rows_of(lax.rem(y - dy + NY, NY) * NC + c)]

        for dx in (1, 3, 2):
            along_x[dx].wait_recv()
            for dy in (1, 3, 2):
                along_y[dx, dy] = links.copy(block(dx, 0), block(dx, 0), dy=dy)
            links.copy(block(dx, 0), block(dx, 0), dc=1, gate=forward)
        for dx in (0, 1, 3, 2):
            for dy in (1, 3, 2):
                along_y[dx, dy].wait_recv()
                links.copy(block(dx, dy), block(dx, dy), dc=1, gate=forward)
        forward.wait()

    return finish


def gather_straight(links, src, buf, rows):
    x, y, c = links.x, links.y, links.c

    def block(xs, ys):
        return buf.at[ys * NC + c, pl.ds(pl.multiple_of(xs * rows, rows), rows)]

    straight = {hops: Gate(links) for hops in range(1, 5)}
    for d in reversed(PLANE):
        links.copy(src, block(x, y), dx=d[0], dy=d[1], gate=straight[hops_of(d)])
    forward = Gate(links)
    links.copy(src, block(x, y), dc=1, gate=forward)

    def finish():
        for hops, gate in straight.items():
            gate.wait()
            for dx, dy in (d for d in PLANE if hops_of(d) == hops):
                came = block(lax.rem(x - dx + NX, NX), lax.rem(y - dy + NY, NY))
                links.copy(came, came, dc=1, gate=forward)
        forward.wait()

    return finish


FAR, THREE, TWO, ONE = range(4)


class RingSum:
    def __init__(self, links, block, sendbuf, recvbuf, width, straight):
        self.links, self.block, self.sendbuf, self.recvbuf = links, block, sendbuf, recvbuf
        self.half, self.made, self.straight = width // 2, {}, straight

    def lanes(self, side):
        return slice(None) if side is None else slice(side * self.half, (side + 1) * self.half)

    def add(self, value, way, kind, side, lanes):
        self.made[way, kind, side].wait_recv()
        return value + self.recvbuf[way, kind, :, lanes].astype(F32)

    def send(self, way, kind, side=None):
        lanes = self.lanes(side)
        value = self.block(4 - kind if way == 0 else 4 + kind)[:, lanes]
        if kind == THREE and side == way:
            value = self.add(value, way, FAR, side, lanes)
        elif kind == TWO and self.straight:
            parts = [value[:, : self.half], value[:, self.half :]]
            parts[way] = self.add(parts[way], way, FAR, way, self.lanes(way))
            value = self.add(jnp.concatenate(parts, axis=1), way, THREE, None, lanes)
        elif kind == TWO:
            self.made[way, THREE, 1 - way].wait_recv()
            value = self.add(value, way, THREE, way, lanes)
        elif kind == ONE:
            value = self.add(value, way, TWO, None, lanes)
        self.sendbuf[way, kind, :, lanes] = value.astype(BF)
        at = (way, kind) if side is None else (way, kind, slice(None), pl.ds(side * self.half, self.half))
        hops = 2 if kind == FAR and self.straight else 1
        self.made[way, kind, side] = self.links.copy(
            self.sendbuf.at[at], self.recvbuf.at[at], dz=hops if way == 0 else NZ - hops
        )

    def farthest(self):
        for way in (0, 1):
            self.send(way, FAR, way)

    def three(self):
        for way in (0, 1):
            self.send(way, THREE, None if self.straight else 1 - way)

    def later(self, number):
        if number or not self.straight:
            for way in (0, 1):
                self.send(way, *((THREE, way), (TWO, None), (ONE, None))[number])

    def total(self):
        value = self.block(0)
        for way in (0, 1):
            value = self.add(value, way, ONE, None, slice(None))
        return value


class RingGather:
    def __init__(self, links, buf, rows):
        self.links, self.buf, self.rows, self.going = links, buf, rows // 2, {}

    def step(self, step):
        for way in (0, 1):
            if step:
                self.going[way, step].wait_recv()
            at = lax.rem(self.links.z + (NZ - step if way == 0 else step), NZ)
            if step == 2:
                half = self.buf.at[at, pl.ds(way * self.rows, self.rows)]
                self.going[way, 4] = self.links.copy(half, half, dz=2 if way == 0 else NZ - 2)
            if step < 3:
                self.going[way, step + 1] = self.links.copy(
                    self.buf.at[at], self.buf.at[at], dz=1 if way == 0 else NZ - 1
                )

    def finish(self):
        for way in (0, 1):
            self.going[way, 4].wait_recv()


def square_rows(wide):
    squares = wide * wide
    squares = squares[:, :F] + squares[:, F : 2 * F] + squares[:, 2 * F : 3 * F] + squares[:, 3 * F :]
    if wide.shape[0] < R:
        squares = jnp.concatenate([squares, jnp.zeros((R - wide.shape[0], F), F32)], axis=0)
    ones = jnp.ones((16, F), BF)
    high = squares.astype(BF)
    low = (squares - high.astype(F32)).astype(BF)
    return (dot_t(ones, high) + dot_t(ones, low))[:8]


def stats_total(own, got, gate):
    gate.wait()
    total = own
    for offset in range(1, NZ):
        total = total + got[offset]
    return jnp.concatenate([total, jnp.zeros((R - 8, R), F32)], axis=0).T


def body(
    x_hbm, len_hbm, state_hbm, gain1_hbm, wq, wk, wv, wo, write_hbm, forget_hbm, rate_hbm, head_gain_hbm, w_out,
    gain2_hbm, w_gate, w_up, w_down,
    out_ref, next_hbm,
    xbuf, w4, wr, rate_w, rw, p1, s1, r1, stats1, got1, pre, last1, cols, on_first, updates, decays, readings, mixed_own, wz, mz, obuf, orecv,
    hown, hb, stats2, got2, wg, wu, wd, p2, s2, r2, abuf, part, psend, precv, fsend, frecv,
    x_ref, len_ref, state_ref, gain1_ref, write_ref, forget_ref, rate_ref, head_gain_ref, gain2_ref,
    ruler, local, send, recv,
):
    links = Links(send, recv, ruler)
    links.phase()
    arrive = greet(links)
    z, x, y, c = links.z, links.x, links.y, links.c
    tp = y * NC + c

    locals_ = [pltpu.make_async_copy(w, w4.at[i], local.at[i]) for i, w in enumerate((wq, wk, wv, wo))]

    def window(at):
        return pl.ds(pl.multiple_of((at * 3 - at // (NX - 1)) * F, F), WIN)

    feats = pl.ds(pl.multiple_of(x * F, F), F)
    given = [
        pltpu.make_async_copy(far, near, local.at[11 + i])
        for i, (far, near) in enumerate(
            (
                (x_hbm, x_ref), (write_hbm, write_ref), (forget_hbm, forget_ref), (gain1_hbm, gain1_ref),
                (gain2_hbm, gain2_ref), (len_hbm, len_ref), (rate_hbm, rate_ref), (head_gain_hbm, head_gain_ref),
                (state_hbm, state_ref),
            )
        )
    ]
    for one in given:
        one.start()
    own_x = pltpu.make_async_copy(x_hbm, xbuf.at[x, rows_of(tp)], local.at[4])
    own_out = pltpu.make_async_copy(w_out, wz.at[x], local.at[5])
    own_late = [
        pltpu.make_async_copy(w_gate.at[:, window(x)], wg.at[feats], local.at[6]),
        pltpu.make_async_copy(w_up.at[:, window(x)], wu.at[feats], local.at[7]),
        pltpu.make_async_copy(w_down.at[window(x)], wd.at[x], local.at[8]),
    ]
    for one in locals_ + [own_x, own_out] + own_late:
        one.start()
    arrive()

    given[0].wait()
    finish = gather_x_first(links, x_ref, xbuf)
    for one in given[1:8]:
        one.wait()
    small = [write_ref[...].astype(F32), forget_ref[...].astype(F32), jnp.zeros((12, F), F32)]
    rate_w[...] = jnp.concatenate(small, axis=0).astype(BF)
    rw[x] = rate_w[...]
    for one in locals_:
        one.wait()
    own_w = pltpu.make_async_copy(w4.at[x], wr.at[feats], local.at[9])
    own_w.start()
    early, early_rates, late, outs = Gate(links), Gate(links), Gate(links), Gate(links)
    for dx in (1, 3, 2):
        to = lax.rem(x + dx, NX)
        links.copy(w4.at[to], wr.at[feats], dx=dx, gate=early)
        links.copy(rate_w, rw.at[x], dx=dx, gate=early_rates)
    links.phase()
    for dx in (1, 3, 2):
        links.copy(w_out, wz.at[x], dx=dx, gate=outs)
    for dx in (1, 3, 2):
        to = lax.rem(x + dx, NX)
        links.copy(w_gate.at[:, window(to)], wg.at[feats], dx=dx, gate=late)
    links.phase()

    which = lax.broadcasted_iota(jnp.int32, (32, F), 0)

    def gain_of(ref):
        wide = ref[...].astype(F32)
        return jnp.concatenate(
            [jnp.sum(jnp.where(which == z * NX + k, wide, 0.0), axis=0, keepdims=True) for k in range(NX)], axis=1
        )

    gain1, gain2 = gain_of(gain1_ref), gain_of(gain2_ref)
    own_x.wait()
    own_w.wait()
    finish()
    early.wait()
    early_rates.wait()
    links.phase()

    sub = lax.broadcasted_iota(jnp.int32, (8, R), 0)
    stats_gate, ready = Gate(links), {}

    def projected(offset):
        if offset not in ready:
            ready[offset] = True
            at = rows_of(lax.rem(z + offset, NZ))
            wide = jnp.concatenate([xbuf[k, at, :] for k in range(NX)], axis=1).astype(F32)
            normed = (wide * gain1).astype(BF)
            p1[offset] = jnp.dot(normed, wr[...], preferred_element_type=F32)
            stat = jnp.where(sub == 4, square_rows(wide), 0.0)
            for k in range(NX):
                stat = stat + dot_t(rw[k], normed[:, k * F : (k + 1) * F])[:8]
            stats1[offset] = stat
            if offset:
                links.copy(stats1.at[offset], got1.at[offset], dz=offset, gate=stats_gate)
        return p1[offset]

    def part_of(at):
        return pl.ds(pl.multiple_of(at * 32, 32), 32)

    near = {}
    for way in (0, 1):
        side = pl.ds(way * F, F)
        s1[way, 0, :, way * F : (way + 1) * F] = projected(4)[:, way * F : (way + 1) * F].astype(BF)
        near[way, 0] = links.copy(s1.at[way, 0, :, side], r1.at[way, 0, :, side], dz=2 if way == 0 else NZ - 2)
    for way in (0, 1):
        s1[way, 1] = projected(3 if way == 0 else 5).astype(BF)
        near[way, 1] = links.copy(s1.at[way, 1], r1.at[way, 1], dz=1 if way == 0 else NZ - 1)
    pre_gate = Gate(links)

    def to_owners(slot, value, dz):
        last1[slot] = value.astype(BF)
        for dx in (2, 1, 3, 0):
            if dx or dz:
                links.copy(last1.at[slot, part_of(lax.rem(x + dx, NX))], pre.at[x, slot], dz=dz, dx=dx, gate=pre_gate)

    to_owners(1, projected(1), 1)
    to_owners(2, projected(7), NZ - 1)
    to_owners(0, projected(0), 0)
    for way in (0, 1):
        value = projected(2 if way == 0 else 6)
        near[way, 0].wait_recv()
        near[way, 1].wait_recv()
        half = value[:, way * F : (way + 1) * F] + r1[way, 0, :, way * F : (way + 1) * F].astype(F32)
        halves = [half, value[:, F:]] if way == 0 else [value[:, :F], half]
        to_owners(3 + way, jnp.concatenate(halves, axis=1) + r1[way, 1].astype(F32), 2 if way == 0 else NZ - 2)
    quarter = part_of(x)
    pre[x, 0] = last1[0, quarter, :]
    cols[...] = stats_total(stats1[0], got1, stats_gate)
    stat = cols[quarter, :]
    scale = lax.rsqrt(stat[:, 4:5] / D + EPS)
    lane = lax.broadcasted_iota(jnp.int32, (32, R), 1)
    row = lax.broadcasted_iota(jnp.int32, (32, R), 0)
    live = jnp.zeros((32, R), F32)
    for s in range(8):
        inside = (row // NEW == s) & (lax.rem(row, NEW) < len_ref[s])
        live = live + jnp.where(inside, 1.0, 0.0)
    rated = stat * scale
    beta = jax.nn.sigmoid(rated) * live
    rate = jnp.where(lane == 2, rate_ref[0], jnp.where(lane == 3, rate_ref[1], 0.0))
    softplus = jnp.maximum(rated, 0.0) + jnp.log1p(jnp.exp(-jnp.abs(rated)))
    keep = jnp.exp(-rate * softplus * live)
    pre_gate.wait()
    links.phase()

    def summed(i):
        return sum(pre[i, k].astype(F32) for k in range(5)) * scale

    given[8].wait()
    for dx in (1, 3, 2):
        to = lax.rem(x + dx, NX)
        links.copy(w_up.at[:, window(to)], wu.at[feats], dx=dx, gate=late)
        links.copy(w_down.at[window(to)], wd.at[x], dx=dx, gate=late)
    query, key, value, gate = (silu(summed(i)) for i in range(4))

    def unit(a):
        return a * lax.rsqrt(jnp.sum(a * a, axis=1, keepdims=True) + EPS)

    stacked = []
    for h in range(2):
        at = slice(h * F, (h + 1) * F)
        stacked += [unit(query[:, at]) * F ** (-0.5), unit(key[:, at])]
    upper = lax.broadcasted_iota(jnp.int32, (8, F), 0) < NEW
    for pair in range(4):
        near8 = slice(pair * 8, pair * 8 + 8)
        for h in range(2):
            both = jnp.concatenate([stacked[2 * h][near8], stacked[2 * h + 1][near8]], axis=0)
            one, two = (
                jnp.dot(both, state_ref[2 * pair + i, h], precision=lax.Precision.HIGHEST, preferred_element_type=F32)
                for i in range(2)
            )
            for k in range(2):
                half = slice(k * 8, k * 8 + 8)
                on_first[k, near8, h * F : (h + 1) * F] = jnp.where(upper, one[half], two[half])
    position = lax.rem(row, NEW)

    def later_by(a, n):
        return jnp.concatenate([a[32 - n :], a[: 32 - n]], axis=0)

    def sooner_by(a, n):
        return jnp.concatenate([a[n:], a[:n]], axis=0)

    for h in range(2):
        at = slice(h * F, (h + 1) * F)
        q_now, k_now, v_now = stacked[2 * h], stacked[2 * h + 1], value[:, at]
        write = jnp.broadcast_to(beta[:, h : h + 1], (32, F))
        hold = jnp.broadcast_to(keep[:, 2 + h : 3 + h], (32, F))
        over1 = hold
        over2 = over1 * later_by(hold, 1)
        over3 = over2 * later_by(hold, 2)
        over4 = over3 * later_by(hold, 3)
        whole = jnp.where(position == 0, over1, jnp.where(position == 1, over2, jnp.where(position == 2, over3, over4)))
        alone = write * (v_now - whole * on_first[1, :, at])
        among_k, among_q = [], [jnp.sum(q_now * k_now, axis=1, keepdims=True)]
        for n, over_n in ((1, over1), (2, over2), (3, over3)):
            k_then = later_by(k_now, n)
            inside = jnp.where(position >= n, over_n, 0.0)
            among_k.append(write * inside * jnp.sum(k_now * k_then, axis=1, keepdims=True))
            among_q.append(inside * jnp.sum(q_now * k_then, axis=1, keepdims=True))
        update = alone
        for _ in range(NEW - 1):
            update = alone - sum(among_k[n - 1] * later_by(update, n) for n in (1, 2, 3))
        reading = whole * on_first[0, :, at] + among_q[0] * update
        for n in (1, 2, 3):
            reading = reading + among_q[n] * later_by(update, n)
        readings[:, at] = reading
        ahead1 = sooner_by(hold, 1)
        ahead2 = ahead1 * sooner_by(hold, 2)
        ahead3 = ahead2 * sooner_by(hold, 3)
        rest = jnp.where(position == 3, 1.0, jnp.where(position == 2, ahead1, jnp.where(position == 1, ahead2, ahead3)))
        updates[:, at] = rest * update
        decays[:, at] = whole
    for h in range(2):
        at = slice(h * F, (h + 1) * F)
        read = readings[:, at] * live
        normed = read * lax.rsqrt(jnp.mean(read * read, axis=1, keepdims=True) + EPS)
        mixed_own[:, at] = (normed * head_gain_ref[...] * gate[:, at]).astype(BF)

    mixed_gates = [Gate(links), Gate(links)]
    for h in range(2):
        mz[h, z] = mixed_own[h * 16 : h * 16 + 16, :]
        for dz in (4, 3, 5, 2, 6, 1, 7):
            links.copy(mixed_own.at[pl.ds(h * 16, 16)], mz.at[h, z], dz=dz, gate=mixed_gates[h])
    turned = jnp.concatenate(stacked, axis=0).T
    for s in range(8):
        for h in range(2):
            at = slice(h * F, (h + 1) * F)
            state = decays[s * NEW + NEW - 1 : (s + 1) * NEW, at] * state_ref[s, h]
            for r in range(s * NEW, (s + 1) * NEW):
                state = state + turned[:, h * 64 + 32 + r : h * 64 + 33 + r] * updates[r : r + 1, at]
            state_ref[s, h] = state
    out_state = pltpu.make_async_copy(state_ref, next_hbm, local.at[10])
    out_state.start()
    own_out.wait()
    outs.wait()
    tp_gates = [Gate(links), Gate(links)]
    for h in range(2):
        mixed_gates[h].wait()
        heads = jnp.concatenate([mz[h, k] for k in range(NZ)], axis=0)
        for k in range(NX):
            terms = jnp.dot(heads, wz[k], preferred_element_type=F32).astype(BF)
            for b in range(NTP):
                obuf[h, b, :, k * F : (k + 1) * F] = terms[b * 16 : b * 16 + 16]
        for k in (4, 3, 5, 2, 6, 1, 7):
            to = lax.rem(tp + k, NTP)
            links.copy_to(obuf.at[h, to], orecv.at[h, k], (z, x, to // NC, lax.rem(to, NC)), tp_gates[h])

    finish = []
    for h in range(2):
        attended = obuf[h, tp].astype(F32)
        links.phase()
        tp_gates[h].wait()
        for k in range(1, NTP):
            attended = attended + orecv[h, k].astype(F32)
        at = pl.ds(pl.multiple_of(tp * R + x * 32 + h * 16, 16), 16)
        given = jnp.concatenate([xbuf[k, at, :] for k in range(NX)], axis=1).astype(F32)
        hown[h] = (given + attended).astype(BF)
        hb[h, tp, pl.ds(pl.multiple_of(x * 16, 16), 16), :] = hown[h]
        finish.append(gather_straight(links, hown.at[h], hb.at[h], 16))

    stats_gates, ready2 = (Gate(links), Gate(links)), ({}, {})

    def mixer(h):
        def block(offset):
            if offset not in ready2[h]:
                ready2[h][offset] = True
                wide = hb[h, lax.rem(z + offset, NZ)].astype(F32)
                normed = (wide * gain2).astype(BF)
                p2[h, offset, :, :WIN] = jnp.dot(normed, wg[...], preferred_element_type=F32)
                p2[h, offset, :, WIN:] = jnp.dot(normed, wu[...], preferred_element_type=F32)
                stats2[h, offset] = square_rows(wide)
                if offset:
                    links.copy(stats2.at[h, offset], got2.at[h, offset], dz=offset, gate=stats_gates[h])
            return p2[h, offset]

        return RingSum(links, block, s2.at[h], r2.at[h], 2 * WIN, STRAIGHT[h])

    sums = [mixer(h) for h in range(2)]
    gathers = [RingGather(links, abuf.at[h], 64) for h in range(2)]
    odd = lax.rem(z + c, 2)
    partner = (z, x, y, 1 - c)

    def activate(h):
        total = sums[h].total()
        scale2 = lax.rsqrt(stats_total(stats2[h, 0], got2.at[h], stats_gates[h])[:64, 0:1] / D + EPS)
        activated = silu(scale2 * total[:, :WIN]) * (scale2 * total[:, WIN:])
        again = (lax.broadcasted_iota(jnp.int32, (64, WIN), 1) < F) & (x == NX - 1)
        abuf[h, z] = jnp.where(again, 0.0, activated).astype(BF)
        gathers[h].step(0)
        down(h, 0)

    def down(h, offset):
        block = abuf[h, lax.rem(z + offset, NZ)]
        for k in range(NX):
            part[h, offset, :, k * F : (k + 1) * F] = jnp.dot(block, wd[k], preferred_element_type=F32)

    turns = (0, 6, 2, 4)
    over = {(h, base): links.fresh() for h in range(2) for base in turns}

    def give(h, base):
        at = base + 1 - odd
        psend[h, at] = part[h, at].astype(BF)
        over_made[h, base] = links.copy_to(psend.at[h, at], precv.at[h, at], partner, index=over[h, base])

    over_made = {}

    def gather_step(h, step):
        gathers[h].step(step) if step < 4 else gathers[h].finish()
        if step < 4:
            down(h, NZ - step)
            down(h, step)
        else:
            down(h, 4)
        give(h, turns[step - 1])

    last_gates = [Gate(links), Gate(links)]

    def spread(h, turn):
        at = turns[turn] + odd
        over_made[h, turns[turn]].wait_recv()
        both = (part[h, at] + precv[h, at].astype(F32)).astype(BF)
        for k in range(NX):
            fsend[h, turn, k] = both[:, k * F : (k + 1) * F]
        to = lax.rem(z + at, NZ) // NC
        for dx in (2, 1, 3):
            xd = lax.rem(x + dx, NX)
            links.copy_to(fsend.at[h, turn, xd], frecv.at[h, y * NX + x], (z, xd, to, c), last_gates[h])

        @pl.when(to != y)
        def _():
            links.copy_to(fsend.at[h, turn, x], frecv.at[h, y * NX + x], (z, x, to, c), last_gates[h])

        @pl.when(to == y)
        def _():
            frecv[h, y * NX + x] = fsend[h, turn, x]

        if turn == 3:
            links.sent[-1] -= 2 * 64 * F
            last_gates[h].size -= 2 * 64 * F

    def put(h):
        result = hb[h, tp, :, feats].astype(F32)
        last_gates[h].wait()
        for i in range(NX * NY):
            result = result + frecv[h, i].astype(F32)
        result = result.astype(BF)
        for k in range(NX):
            out_ref[k * 32 + h * 16 : k * 32 + h * 16 + 16, :] = result[k * 16 : (k + 1) * 16]

    finish[0]()
    for one in own_late:
        one.wait()
    late.wait()
    links.phase()
    sums[0].farthest()
    sums[0].three()
    finish[1]()
    sums[1].farthest()
    sums[0].later(0)
    sums[1].three()
    sums[1].later(0)
    sums[0].later(1)
    sums[1].later(1)
    sums[0].later(2)
    sums[1].later(2)
    links.phase()
    activate(0)
    activate(1)
    links.phase()
    gather_step(0, 1)
    gather_step(1, 1)
    gather_step(0, 2)
    spread(0, 0)
    gather_step(1, 2)
    spread(1, 0)
    gather_step(0, 3)
    spread(0, 1)
    gather_step(1, 3)
    spread(1, 1)
    gather_step(0, 4)
    spread(0, 2)
    gather_step(1, 4)
    spread(1, 2)
    spread(0, 3)
    spread(1, 3)
    put(0)
    put(1)
    out_state.wait()
    links.drain()


def hand_over(out_tmp, state_tmp, out_ref, state_out, held_out, held_state, came, went):
    pieces = [(out_tmp, held_out, out_ref)]
    pieces += [(state_tmp.at[i], held_state.at[i], state_out.at[i]) for i in range(8)]
    coming = [pltpu.make_async_copy(a, b, came.at[i]) for i, (a, b, _) in enumerate(pieces)]
    going = [pltpu.make_async_copy(b, c, went.at[i]) for i, (_, b, c) in enumerate(pieces)]
    for one in coming:
        one.start()
    for one, two in zip(coming, going):
        one.wait()
        two.start()
    for two in going:
        two.wait()


def local(
    layer_input, seq_lengths, delta_state, attn_gain, w_query, w_key, w_value, w_outgate, w_write, w_forget,
    forget_rate, head_gain, w_out, mixer_gain, w_gate, w_up, w_down,
):
    vmem = pl.BlockSpec(memory_space=pltpu.VMEM)
    hbm = pl.BlockSpec(memory_space=pltpu.HBM)
    scratch = [
        ((NX, NTP * R, F), BF),
        ((4, F, 256), BF),
        ((NX * F, 256), BF),
        ((16, F), BF),
        ((NX, 16, F), BF),
        ((NZ, R, 256), F32),
        ((2, 2, R, 256), BF),
        ((2, 2, R, 256), BF),
        ((NZ, 8, R), F32),
        ((NZ, 8, R), F32),
        ((NX, 5, 32, 256), BF),
        ((5, R, 256), BF),
        ((R, R), F32),
        ((2, 32, 256), F32),
        ((32, 256), F32),
        ((32, 256), F32),
        ((32, 256), F32),
        ((32, 256), BF),
        ((NX, 256, F), BF),
        ((2, NZ, 16, 256), BF),
        ((2, NTP, 16, NX * F), BF),
        ((2, NTP, 16, NX * F), BF),
        ((2, 16, NX * F), BF),
        ((2, NTP, 64, NX * F), BF),
        ((2, NZ, 8, R), F32),
        ((2, NZ, 8, R), F32),
        ((NX * F, WIN), BF),
        ((NX * F, WIN), BF),
        ((NX, WIN, F), BF),
        ((2, NZ, 64, 2 * WIN), F32),
        ((2, 2, 4, 64, 2 * WIN), BF),
        ((2, 2, 4, 64, 2 * WIN), BF),
        ((2, NZ, 64, WIN), BF),
        ((2, NZ, 64, NX * F), F32),
        ((2, NZ, 64, NX * F), BF),
        ((2, NZ, 64, NX * F), BF),
        ((2, NY, NX, 64, F), BF),
        ((2, NX * NY, 64, F), BF),
    ]
    held = [
        pltpu.VMEM((R, F), BF),
        pltpu.SMEM((8,), jnp.int32),
        pltpu.VMEM(delta_state.shape, F32),
        pltpu.VMEM((32, F), BF),
        pltpu.VMEM((2, F), BF),
        pltpu.VMEM((2, F), BF),
        pltpu.SMEM((2,), F32),
        pltpu.VMEM((1, F), F32),
        pltpu.VMEM((32, F), BF),
    ]
    out_tmp, state_tmp = pl.pallas_call(
        body,
        out_shape=(
            jax.ShapeDtypeStruct((R, F), BF),
            jax.ShapeDtypeStruct(delta_state.shape, F32),
        ),
        in_specs=[
            hbm, hbm, hbm, hbm, hbm, hbm, hbm, hbm, hbm, hbm, hbm, hbm, hbm, hbm, hbm, hbm, hbm,
        ],
        out_specs=(vmem, hbm),
        scratch_shapes=[pltpu.VMEM(shape, dtype) for shape, dtype in scratch]
        + held
        + [
            pltpu.VMEM((16384, F), BF),
            pltpu.SemaphoreType.DMA((20,)),
            pltpu.SemaphoreType.DMA((NSEND,)),
            pltpu.SemaphoreType.DMA((NRECV,)),
        ],
        compiler_params=pltpu.CompilerParams(
            collective_id=0, has_side_effects=True, vmem_limit_bytes=VMEM_LIMIT
        ),
    )(
        layer_input, seq_lengths, delta_state, attn_gain.reshape(32, F), w_query, w_key, w_value, w_outgate,
        w_write.T, w_forget.T, forget_rate, head_gain.reshape(1, F), w_out, mixer_gain.reshape(32, F), w_gate, w_up,
        w_down,
    )
    return pl.pallas_call(
        hand_over,
        out_shape=(
            jax.ShapeDtypeStruct((R, F), BF),
            jax.ShapeDtypeStruct(delta_state.shape, F32),
        ),
        in_specs=[hbm, hbm],
        out_specs=(hbm, hbm),
        scratch_shapes=[
            pltpu.VMEM((R, F), BF),
            pltpu.VMEM(delta_state.shape, F32),
            pltpu.SemaphoreType.DMA((9,)),
            pltpu.SemaphoreType.DMA((9,)),
        ],
        compiler_params=pltpu.CompilerParams(vmem_limit_bytes=VMEM_LIMIT),
    )(out_tmp, state_tmp)


def solution(mesh):
    split = Mesh(mesh.devices.reshape(NZ, NX, NY, NC), ("z", "x", "y", "c"))
    kv, tp = ("z", "x"), ("y", "c")
    in_specs = (
        P(tp, kv), P(kv), P(kv, tp, None, None), P(), P(kv, tp), P(kv, tp), P(kv, tp), P(kv, tp), P(kv, tp),
        P(kv, tp), P(tp), P(), P(tp, kv), P(), P(kv, tp), P(kv, tp), P(tp, kv),
    )
    out_specs = (P(tp, kv), P(kv, tp, None, None))
    return jax.shard_map(local, mesh=split, in_specs=in_specs, out_specs=out_specs, check_vma=False)
```
